512 devices in a mesh: sp: 16 (over z), fs: 4 (over y), tp: 8 (over x, core).
Axes of the slice: x: 4, y: 4, z: 16, core: 2. Of those that a mesh axis runs over, the one named last changes fastest.
Arguments:
- input_layer_rows: bfloat16 [4, 4096, 2048], P('fs', 'sp'), may hold values from -6 to 6
- input_norm_gain: float32 [2048], replicated, may hold values from 0.1 to 1.9
- query_weight_attention: bfloat16 [2048, 1024], P(('sp', 'fs'), 'tp'), may hold values from -0.125 to 0.125
- key_weight_attention: bfloat16 [2048, 1024], P(('sp', 'fs'), 'tp'), may hold values from -0.125 to 0.125
- value_weight_attention: bfloat16 [2048, 1024], P(('sp', 'fs'), 'tp'), may hold values from -0.125 to 0.125
- query_weight_recurrent: bfloat16 [2048, 1024], P(('sp', 'fs'), 'tp'), may hold values from -0.125 to 0.125
- forget_weight_recurrent: bfloat16 [2048, 1024], P(('sp', 'fs'), 'tp'), may hold values from -0.125 to 0.125
- value_weight_recurrent: bfloat16 [2048, 1024], P(('sp', 'fs'), 'tp'), may hold values from -0.125 to 0.125
- gate_weight_recurrent: bfloat16 [2048, 1024], P(('sp', 'fs'), 'tp'), may hold values from -0.125 to 0.125
- output_weight_attention: bfloat16 [2048, 1024], P(('sp', 'fs'), 'tp'), may hold values from -0.125 to 0.125
- emitted_projection_linear_scan: bfloat16 [2048, 1024], P(('sp', 'fs'), 'tp'), may hold values from -0.125 to 0.125
- score_offset: float32 [8], P('tp'), as said below
- attention_norm_gain: float32 [1024], P('tp'), may hold values from 0.1 to 1.9
- recurrence_norm_gain: float32 [1024], P('tp'), may hold values from 0.1 to 1.9
- forget_floor: float32 [1024], P('tp'), may hold values from 0.1 to 0.5
- forget_offset: float32 [1024], P('tp'), as said below
- extra_log_decay: float32 [4, 4096, 1024], P('fs', 'sp', 'tp')
Outputs:
- layer_out: bfloat16 [4, 4096, 2048], P('fs', ('sp', 'tp'))
- row_log_total: float32 [4, 8, 4096], P('fs', 'tp', 'sp')
The draws below stay inside these ranges and needn't reach their ends.
Inputs may be any that keep to these rules, and one draw needn't show every extreme that they name: `score_offset`: each head's offset lies between -ln(4096) - 2 and -ln(4096) + 0.5. `forget_offset`: each channel's offset lies between ln(256) - 3 and ln(4096) + 0.6.
All inputs are finite; a program needn't handle non-finite values.
Results may differ from the reference program's by a relative error of at most 0.015.
Values may be sent and summed in bfloat16 or wider, within the bound.
No kernel may reach another device: no remote copies, remote signals or barrier semaphores. Data moves between devices by JAX's collectives and lax.ppermute only.
A program may use at most 64 MiB of HBM per device.

```python
import math
import jax
import jax.numpy as jnp
from jax import lax

HEAD = 128
HEADS = 8
D_HALF = 1024
D = 2048
TOK_DEV = 256
BLOCK = 64
SEQ = 4096
BATCH = 4


def draw_score_offset(key, part):
    center = -math.log(SEQ)
    return jax.random.uniform(key, (HEADS,), jnp.float32, center - 2.0, center + 0.5)


def draw_forget_offset(key, part):
    width = HEADS * HEAD
    first, second, third = jax.random.split(key, 3)
    chooser = jax.random.uniform(first, (width,), jnp.float32)
    slow_value = math.log(SEQ) + jax.random.uniform(second, (width,), jnp.float32, -0.4, 0.6)
    fast_value = math.log(TOK_DEV) - 2.5 + jax.random.uniform(third, (width,), jnp.float32, -0.5, 0.5)
    share = 0.5
    return jnp.where(chooser < share, fast_value, slow_value)


def draw_extra_log_decay(key, part):
    width = HEADS * HEAD
    first, second, third = jax.random.split(key, 3)
    blocks = SEQ // TOK_DEV
    lowest, highest_score = (0.05, 0.4)
    rates = jnp.exp(jax.random.uniform(first, (BATCH, blocks, 1, width), jnp.float32, math.log(lowest), math.log(highest_score))) / SEQ
    constant_component = jnp.broadcast_to(rates, (BATCH, blocks, TOK_DEV, width)).reshape(BATCH, SEQ, width)
    spots = jax.random.randint(second, (BATCH, 3), 0, SEQ)
    stratum_level = jnp.log(jax.random.uniform(third, (BATCH, 3, width), jnp.float32, 0.6, 0.85))
    equality_indicators = (jnp.arange(SEQ)[None, :, None] == spots[:, None, :]).astype(jnp.float32)
    fading_spikes = jnp.einsum('tsk,tkx->tsx', equality_indicators, stratum_level, precision=jax.lax.Precision.HIGHEST)
    return fading_spikes - constant_component


def level_of(rng, extent, shards, smallest, high):
    level, own = 1.0, jax.random.fold_in(rng, 6)
    for axis_at, shards_of in shards:
        heights = jnp.exp(jax.random.uniform(jax.random.fold_in(own, axis_at), (shards_of,), jnp.float32, smallest / len(shards), high / len(shards)))
        level = level * jnp.repeat(heights, extent[axis_at] // shards_of).reshape([-1 if axis == axis_at else 1 for axis in range(len(extent))])
    return level


def normal_values(key, dims, spread, reach, pieces=(), held_as=jnp.bfloat16):
    level = level_of(key, dims, pieces, -0.22, 0.18) if pieces else 1.0
    result = jax.random.normal(key, dims, jnp.float32) * spread * level
    return jnp.minimum(jnp.maximum(result, -reach), reach).astype(held_as)


def setup_inputs(seed: int = 0) -> dict:
    key_of = jax.random.split(jax.random.key(seed), 18)
    input_layer_rows = normal_values(key_of[0], (BATCH, SEQ, D), 1.0, 6.0, ((0, 4), (1, 16)))
    input_norm_gain = jnp.clip(1.0 + 0.18 * jax.random.normal(key_of[1], (D,), jnp.float32), 0.1, 1.9)
    query_weight_attention = normal_values(key_of[2], (D, D_HALF), D ** -0.5, 0.125, ((0, 64), (1, 8)))
    key_weight_attention = normal_values(key_of[3], (D, D_HALF), D ** -0.5, 0.125, ((0, 64), (1, 8)))
    value_weight_attention = normal_values(key_of[4], (D, D_HALF), D ** -0.5, 0.125, ((0, 64), (1, 8)))
    query_weight_recurrent = normal_values(key_of[5], (D, D_HALF), D ** -0.5, 0.125, ((0, 64), (1, 8)))
    forget_weight_recurrent = normal_values(key_of[6], (D, D_HALF), D ** -0.5, 0.125, ((0, 64), (1, 8)))
    value_weight_recurrent = normal_values(key_of[7], (D, D_HALF), D ** -0.5, 0.125, ((0, 64), (1, 8)))
    gate_weight_recurrent = normal_values(key_of[8], (D, D_HALF), D ** -0.5, 0.125, ((0, 64), (1, 8)))
    output_weight_attention = normal_values(key_of[9], (D, D_HALF), D ** -0.5, 0.125, ((0, 64), (1, 8)))
    emitted_projection_linear_scan = normal_values(key_of[10], (D, D_HALF), D ** -0.5, 0.125, ((0, 64), (1, 8)))
    score_offset = draw_score_offset(jax.random.fold_in(key_of[17], 71), 0)
    attention_norm_gain = jnp.clip(1.0 + 0.18 * jax.random.normal(key_of[12], (D_HALF,), jnp.float32), 0.1, 1.9)
    recurrence_norm_gain = jnp.clip(1.0 + 0.18 * jax.random.normal(key_of[13], (D_HALF,), jnp.float32), 0.1, 1.9)
    forget_floor = jnp.clip(0.1 + 0.4 * jax.random.uniform(key_of[14], (D_HALF,), jnp.float32) ** level_of(key_of[14], (D_HALF,), ((0, 8),), -0.2, 0.2), 0.1, 0.5)
    forget_offset = draw_forget_offset(jax.random.fold_in(key_of[17], 71), 0)
    extra_log_decay = draw_extra_log_decay(jax.random.fold_in(key_of[17], 71), 0)
    return {"input_layer_rows": input_layer_rows, "input_norm_gain": input_norm_gain, "query_weight_attention": query_weight_attention, "key_weight_attention": key_weight_attention, "value_weight_attention": value_weight_attention, "query_weight_recurrent": query_weight_recurrent, "forget_weight_recurrent": forget_weight_recurrent, "value_weight_recurrent": value_weight_recurrent, "gate_weight_recurrent": gate_weight_recurrent, "output_weight_attention": output_weight_attention, "emitted_projection_linear_scan": emitted_projection_linear_scan, "score_offset": score_offset, "attention_norm_gain": attention_norm_gain, "recurrence_norm_gain": recurrence_norm_gain, "forget_floor": forget_floor, "forget_offset": forget_offset, "extra_log_decay": extra_log_decay}


epsilon = 1e-06
log_floor = 0.05

def normalize_rows(inputs, gain):
    values = inputs.astype(jnp.float32)
    square_mean = lax.optimization_barrier(jnp.mean(values * values, axis=-1, keepdims=True))
    return values * lax.rsqrt(square_mean + epsilon) * gain

def head_norm(values, gain):
    square_mean = lax.optimization_barrier(jnp.mean(values * values, axis=-1, keepdims=True))
    return values * lax.rsqrt(square_mean + epsilon) * gain

def project(normed, weight):
    return jnp.dot(normed, weight, preferred_element_type=jnp.float32).astype(jnp.bfloat16)

def recurrence_block(memory_matrix, inputs):
    query_slice, decay_part, key_slice, value_slice = inputs
    highest_score = lax.Precision.HIGHEST
    length = decay_part.shape[0]
    running_total = jnp.cumsum(decay_part, axis=0)
    causal = (lax.broadcasted_iota(jnp.int32, (length, length), 0) >= lax.broadcasted_iota(jnp.int32, (length, length), 1))[:, :, None, None]
    relative = jnp.where(causal, running_total[:, None] - running_total[None, :], -jnp.inf)
    pairwise = lax.optimization_barrier(jnp.sum(query_slice[:, None] * key_slice[None, :] * jnp.exp(relative), axis=-1))
    inner_part = jnp.einsum('tsh,shv->thv', pairwise, value_slice, precision=highest_score)
    carried_state = jnp.einsum('fby,bym->fbm', query_slice * jnp.exp(running_total), memory_matrix, precision=highest_score)
    final_total = running_total[-1]
    updated_state = jnp.exp(final_total)[:, :, None] * memory_matrix + jnp.einsum('rxc,rxa->xca', key_slice * jnp.exp(final_total[None] - running_total), value_slice, precision=highest_score)
    return (updated_state, inner_part + carried_state)

def recurrence(query_rows_input, forget_log_value, key_in, value_in):
    seq_len = query_rows_input.shape[0]

    def to_blocks(array_in):
        return array_in.reshape(seq_len // BLOCK, BLOCK, HEADS, HEAD)
    initial = jnp.zeros((HEADS, HEAD, HEAD), jnp.float32)
    unused, outputs = lax.scan(recurrence_block, initial, (to_blocks(query_rows_input), to_blocks(forget_log_value), to_blocks(key_in), to_blocks(value_in)))
    return outputs.reshape(seq_len, HEADS, HEAD)

def stick_attention(queries, keys_all, values_all, shifts):
    outputs = []
    totals = []
    for block_index in range(SEQ // TOK_DEV):
        first = block_index * TOK_DEV
        final = first + TOK_DEV
        scores = jnp.einsum('thd,shd->hts', queries[first:final].astype(jnp.float32), keys_all[:final].astype(jnp.float32)) * HEAD ** (-0.5) + shifts[:, None, None]
        strict = first + lax.broadcasted_iota(jnp.int32, (TOK_DEV, final), 0) > lax.broadcasted_iota(jnp.int32, (TOK_DEV, final), 1)
        logarithmic_retention = jnp.where(strict, jax.nn.log_sigmoid(-scores), 0.0)
        suffix = lax.cumsum(logarithmic_retention, axis=2, reverse=True) - logarithmic_retention
        log_weight = jnp.where(strict, jax.nn.log_sigmoid(scores) + suffix, -jnp.inf)
        weights = jnp.exp(log_weight).astype(jnp.bfloat16)
        outputs.append(jnp.einsum('hts,shd->thd', weights.astype(jnp.float32), values_all[:final].astype(jnp.float32)))
        totals.append(lax.optimization_barrier(jnp.sum(logarithmic_retention, axis=2)))
    return (jnp.concatenate(outputs, axis=0), jnp.concatenate(totals, axis=1))

def reference(input_layer_rows, input_norm_gain, query_weight_attention, key_weight_attention, value_weight_attention, query_weight_recurrent, forget_weight_recurrent, value_weight_recurrent, gate_weight_recurrent, output_weight_attention, emitted_projection_linear_scan, score_offset, attention_norm_gain, recurrence_norm_gain, forget_floor, forget_offset, extra_log_decay):
    layer_rows = []
    log_rows = []
    for batch_position in range(BATCH):
        normed = normalize_rows(input_layer_rows[batch_position], input_norm_gain).astype(jnp.bfloat16)
        query_a = project(normed, query_weight_attention).reshape(SEQ, HEADS, HEAD)
        key_a = project(normed, key_weight_attention).reshape(SEQ, HEADS, HEAD)
        value_a = project(normed, value_weight_attention).reshape(SEQ, HEADS, HEAD)
        query_b = project(normed, query_weight_recurrent)
        forget_b = project(normed, forget_weight_recurrent)
        input_b = project(normed, value_weight_recurrent)
        gate_b = project(normed, gate_weight_recurrent)
        attended, keep_total = stick_attention(query_a, key_a, value_a, score_offset)
        log_rows.append(jnp.log(jnp.maximum(-jnp.expm1(keep_total), log_floor)))
        mixed_a = head_norm(attended, attention_norm_gain.reshape(HEADS, HEAD)).reshape(SEQ, D_HALF).astype(jnp.bfloat16)
        forget_logits = forget_b.astype(jnp.float32) + forget_offset
        forget_log_value = jnp.logaddexp(jnp.log(forget_floor), jnp.log1p(-forget_floor) + jax.nn.log_sigmoid(forget_logits)) + extra_log_decay[batch_position]
        key_in = (1.0 - forget_floor) * jax.nn.sigmoid(-forget_logits)
        query_rows_input = jax.nn.silu(query_b.astype(jnp.float32))
        value_in = input_b.astype(jnp.float32)
        recurrent = recurrence(query_rows_input.reshape(SEQ, HEADS, HEAD), forget_log_value.reshape(SEQ, HEADS, HEAD), key_in.reshape(SEQ, HEADS, HEAD), value_in.reshape(SEQ, HEADS, HEAD))
        gated_out = head_norm(recurrent, recurrence_norm_gain.reshape(HEADS, HEAD)) * jax.nn.silu(gate_b.astype(jnp.float32).reshape(SEQ, HEADS, HEAD))
        mixed_b = gated_out.reshape(SEQ, D_HALF).astype(jnp.bfloat16)
        summed = jnp.dot(mixed_a, output_weight_attention.T, preferred_element_type=jnp.float32) + jnp.dot(mixed_b, emitted_projection_linear_scan.T, preferred_element_type=jnp.float32)
        layer_rows.append(summed.astype(jnp.bfloat16))
    return (jnp.stack(layer_rows), jnp.stack(log_rows))
```

```python
import jax
import jax.numpy as jnp
from jax import lax
from jax.experimental import pallas as pl
from jax.experimental.pallas import tpu as pltpu
from jax.sharding import PartitionSpec as P

HEAD = 128
ROWS = 32
TILE = 16

epsilon = 1e-06
log_floor = 0.05
F32 = jnp.float32
BF16 = jnp.bfloat16
INTERPRET = False


def vmem_call(kernel, outs, n_in, smem=()):
    specs = [
        pl.BlockSpec(memory_space=pltpu.SMEM if k in smem else pltpu.VMEM) for k in range(n_in)
    ]
    return pl.pallas_call(
        kernel,
        out_shape=outs,
        in_specs=specs,
        out_specs=jax.tree.map(lambda _: pl.BlockSpec(memory_space=pltpu.VMEM), outs),
        interpret=INTERPRET,
    )


def dot(a, b, dims=((1,), (0,))):
    return lax.dot_general(a, b, (dims, ((), ())), preferred_element_type=F32)


def parts(a):
    high = a.astype(BF16)
    return high, (a - high.astype(F32)).astype(BF16)


def dot_left(a, b, dims=((1,), (0,))):
    high, low = parts(a)
    return dot(high, b, dims) + dot(low, b, dims)


def dot_both(a, b, dims):
    a_high, a_low = parts(a)
    b_high, b_low = parts(b)
    return dot(a_high, b_high, dims) + (dot(a_high, b_low, dims) + dot(a_low, b_high, dims))


def times_weight(normed, weight_ref):
    fs, sp, rows, cols = weight_ref.shape
    step = 2 if sp % 2 == 0 else 1
    total = None
    for s in range(0, sp, step):
        piece = jnp.concatenate(
            [weight_ref[:, s + k].reshape(fs * rows, cols) for k in range(step)], axis=0
        )
        width = step * fs * rows
        term = dot(normed[:, s * fs * rows : s * fs * rows + width], piece)
        total = term if total is None else total + term
    return total


def norm_project_kernel(x_ref, gain_ref, weight_ref, normed_ref, out_ref):
    values = x_ref[...].astype(F32)
    square_mean = jnp.mean(values * values, axis=-1, keepdims=True)
    normed = (values * lax.rsqrt(square_mean + epsilon) * gain_ref[...]).astype(BF16)
    normed_ref[...] = normed
    out_ref[...] = times_weight(normed_ref, weight_ref).astype(BF16)


def local_recurrence_kernel(
    normed_ref,
    weight_ref,
    floor_ref,
    offset_ref,
    extra_ref,
    query_a_ref,
    inner_ref,
    query_decayed_ref,
    gate_ref,
    state_ref,
):
    projected = times_weight(normed_ref, weight_ref).astype(BF16)
    columns = [projected[:, k * HEAD : (k + 1) * HEAD] for k in range(5)]
    query_a_ref[...] = columns[0]
    query_b = columns[1].astype(F32)
    query = query_b / (1.0 + jnp.exp(-query_b))
    value = columns[3]
    gate_b = columns[4].astype(F32)
    gate_ref[...] = gate_b / (1.0 + jnp.exp(-gate_b))
    u = columns[2].astype(F32) + offset_ref[...]
    key = (1.0 - floor_ref[...]) / (1.0 + jnp.exp(u))
    log_forget = jnp.log(1.0 - key) + extra_ref[...]
    length = log_forget.shape[0]
    row = lax.broadcasted_iota(jnp.int32, (length, length), 0)
    col = lax.broadcasted_iota(jnp.int32, (length, length), 1)
    lower = (row >= col).astype(BF16)
    high = log_forget.astype(BF16)
    rest = log_forget - high.astype(F32)
    middle = rest.astype(BF16)
    low = (rest - middle.astype(F32)).astype(BF16)
    running = dot(lower, high) + (dot(lower, middle) + dot(lower, low))
    position = lax.broadcasted_iota(jnp.int32, (length, 1), 0)
    pairwise = jnp.where(row == col, dot_both(query, key, ((1,), (1,))), 0.0)
    half = 1
    while half < length:
        block = 2 * half
        if block >= 8:
            boundary = running.reshape(length // block, block, HEAD)[:, half - 1 : half]
            boundary = jnp.broadcast_to(boundary, (length // block, block, HEAD)).reshape(
                length, HEAD
            )
        else:
            tiles = running.reshape(length // 8, 8, HEAD)
            inside = lax.broadcasted_iota(jnp.int32, (1, 8, 1), 1) // block
            boundary = jnp.zeros_like(tiles)
            for k in range(8 // block):
                at = k * block + half - 1
                boundary = jnp.where(inside == k, tiles[:, at : at + 1], boundary)
            boundary = boundary.reshape(length, HEAD)
        second = (position // half) % 2 == 1
        after = jnp.where(second, query * jnp.exp(running - boundary), 0.0)
        before = jnp.where(second, 0.0, key * jnp.exp(boundary - running))
        chosen = (row // block == col // block) & (row // half != col // half) & (row > col)
        pairwise = jnp.where(chosen, dot_both(after, before, ((1,), (1,))), pairwise)
        half = block
    inner_ref[...] = dot_left(pairwise, value)
    final = running[length - 1 : length]
    query_decayed_ref[...] = query * jnp.exp(running)
    key_high, key_low = parts(key * jnp.exp(final - running))
    state = dot(value, key_high, ((0,), (0,))) + dot(value, key_low, ((0,), (0,)))
    state_ref[0:HEAD] = state.astype(BF16)
    state_ref[HEAD : HEAD + TILE] = jnp.broadcast_to(jnp.exp(final), (TILE, HEAD)).astype(BF16)


def mixed_b_kernel(
    rank_ref, message_ref, inner_ref, query_decayed_ref, gate_ref, gain_ref, out_ref
):
    def chain(k, state):
        decay = message_ref[k, HEAD : HEAD + TILE].astype(F32)[0:1]
        return decay * state + message_ref[k, 0:HEAD].astype(F32)

    state = lax.fori_loop(0, rank_ref[0], chain, jnp.zeros((HEAD, HEAD), F32))
    recurrent = inner_ref[...] + dot_both(query_decayed_ref[...], state, ((1,), (1,)))
    square_mean = jnp.mean(recurrent * recurrent, axis=-1, keepdims=True)
    mixed = recurrent * lax.rsqrt(square_mean + epsilon) * gain_ref[...] * gate_ref[...]
    out_ref[...] = mixed.astype(BF16)


def attention_kernel(
    rank_ref,
    shift_ref,
    query_ref,
    key_value_ref,
    gain_ref,
    mixed_b_ref,
    weight_ref,
    out_ref,
    total_ref,
):
    rank = rank_ref[0]
    shift = shift_ref[0]
    query = query_ref[...]
    length = query.shape[0]
    row = lax.broadcasted_iota(jnp.int32, (length, length), 0)
    col = lax.broadcasted_iota(jnp.int32, (length, length), 1)
    strict = row > col
    suffix = (row >= col).astype(BF16)

    def piece(source, total, is_own):
        start = pl.multiple_of(source * length, length)
        key = key_value_ref[pl.ds(start, length), 0:HEAD]
        value = key_value_ref[pl.ds(start, length), HEAD : 2 * HEAD]
        scores = dot(query, key, ((1,), (1,))) * HEAD ** (-0.5) + shift
        softplus = jnp.maximum(scores, 0.0) + jnp.log(1.0 + jnp.exp(-jnp.abs(scores)))
        if is_own:
            softplus = jnp.where(strict, softplus, 0.0)
        spent = dot_left(softplus, suffix) + total
        weights = jnp.exp(scores - spent)
        if is_own:
            weights = jnp.where(strict, weights, 0.0)
        return dot(weights.astype(BF16), value), spent[:, 0:1]

    carry = piece(rank, 0.0, True)

    def earlier(k, carry):
        weighted, total = carry
        more, total = piece(rank - 1 - k, total, False)
        return weighted + more, total

    weighted, total = lax.fori_loop(0, rank, earlier, carry)
    total_row = jnp.transpose(jnp.broadcast_to(total, (length, HEAD)))[0:1]
    total_ref[...] = jnp.log(jnp.maximum(1.0 - jnp.exp(-total_row), log_floor))
    square_mean = jnp.mean(weighted * weighted, axis=-1, keepdims=True)
    mixed_a = (weighted * lax.rsqrt(square_mean + epsilon) * gain_ref[...]).astype(BF16)
    mixed = jnp.concatenate([mixed_a, mixed_b_ref[...]], axis=1)
    fs, sp = weight_ref.shape[:2]
    width = fs * ROWS
    for s in range(sp):
        both = jnp.concatenate(
            [weight_ref[:, s, k].reshape(width, HEAD) for k in range(2)], axis=1
        )
        out_ref[:, s * width : (s + 1) * width] = dot(mixed, both, ((1,), (1,))).astype(BF16)


def over_fs(shard):
    size = lax.axis_size("fs")
    copies = jnp.broadcast_to(shard[None], (size, *shard.shape))
    return lax.all_to_all(copies, "fs", 0, 0, tiled=True)


def on_device(
    input_layer_rows,
    input_norm_gain,
    query_weight_attention,
    key_weight_attention,
    value_weight_attention,
    query_weight_recurrent,
    forget_weight_recurrent,
    value_weight_recurrent,
    gate_weight_recurrent,
    output_weight_attention,
    emitted_projection_linear_scan,
    score_offset,
    attention_norm_gain,
    recurrence_norm_gain,
    forget_floor,
    forget_offset,
    extra_log_decay,
):
    x = input_layer_rows[0]
    tokens, width = x.shape
    sp, fs, tp = (lax.axis_size(name) for name in ("sp", "fs", "tp"))
    rank = lax.axis_index("sp").astype(jnp.int32).reshape(1)
    local = jnp.concatenate(
        (
            key_weight_attention,
            value_weight_attention,
            query_weight_attention,
            query_weight_recurrent,
            forget_weight_recurrent,
            value_weight_recurrent,
            gate_weight_recurrent,
        ),
        axis=1,
    )
    column = lax.all_gather(local, "sp")
    first = over_fs(column[:, :, : 2 * HEAD])
    normed, key_value = vmem_call(
        norm_project_kernel,
        (
            jax.ShapeDtypeStruct((tokens, width), BF16),
            jax.ShapeDtypeStruct((tokens, 2 * HEAD), BF16),
        ),
        3,
    )(x, input_norm_gain.reshape(1, width), first)
    everything = lax.all_gather(key_value, "sp", axis=0, tiled=True)
    column, key_value = lax.optimization_barrier((column, key_value))
    second = over_fs(column[:, :, 2 * HEAD :])
    small = jax.ShapeDtypeStruct((tokens, HEAD), F32)
    query_a, inner, query_decayed, gate, state = vmem_call(
        local_recurrence_kernel,
        (
            jax.ShapeDtypeStruct((tokens, HEAD), BF16),
            small,
            small,
            small,
            jax.ShapeDtypeStruct((HEAD + TILE, HEAD), BF16),
        ),
        5,
    )(
        normed,
        second,
        forget_floor.reshape(1, HEAD),
        forget_offset.reshape(1, HEAD),
        extra_log_decay[0],
    )
    message = lax.all_gather(
        jnp.concatenate((state, output_weight_attention, emitted_projection_linear_scan), axis=0),
        "sp",
    )
    out_weights = over_fs(message[:, HEAD + TILE :].reshape(sp, 2, ROWS, HEAD))
    mixed_b = vmem_call(mixed_b_kernel, jax.ShapeDtypeStruct((tokens, HEAD), BF16), 6, (0,))(
        rank, message, inner, query_decayed, gate, recurrence_norm_gain.reshape(1, HEAD)
    )
    projected, row_log_total = vmem_call(
        attention_kernel,
        (
            jax.ShapeDtypeStruct((tokens, width), BF16),
            jax.ShapeDtypeStruct((1, tokens), F32),
        ),
        7,
        (0, 1),
    )(
        rank,
        score_offset,
        query_a,
        everything,
        attention_norm_gain.reshape(1, HEAD),
        mixed_b,
        out_weights,
    )
    tiles = lax.all_to_all(projected.reshape(tp, tokens // tp, width), "tp", 0, 0, tiled=True)
    layer_out = jnp.sum(tiles.astype(F32), axis=0).astype(BF16)
    return (layer_out[None], row_log_total[None])


def solution(mesh):
    weight = P(("sp", "fs"), "tp")
    return jax.shard_map(
        on_device,
        mesh=mesh,
        in_specs=(
            P("fs", "sp", None),
            P(),
            *(weight for _ in range(9)),
            *(P("tp") for _ in range(5)),
            P("fs", "sp", "tp"),
        ),
        out_specs=(P("fs", ("sp", "tp"), None), P("fs", "tp", "sp")),
        check_vma=False,
    )
```

```python
import jax
import jax.numpy as jnp
from jax import lax
from jax.experimental import pallas as pl
from jax.experimental.pallas import tpu as pltpu
from jax.sharding import PartitionSpec as P

HEAD = 128
ROWS = 32
TILE = 16
FIRST = 64

epsilon = 1e-06
log_floor = 0.05
F32 = jnp.float32
BF16 = jnp.bfloat16
INTERPRET = False


def vmem_call(kernel, outs, n_in, smem=(), mib=16):
    specs = [
        pl.BlockSpec(memory_space=pltpu.SMEM if k in smem else pltpu.VMEM) for k in range(n_in)
    ]
    return pl.pallas_call(
        kernel,
        out_shape=outs,
        in_specs=specs,
        out_specs=jax.tree.map(lambda _: pl.BlockSpec(memory_space=pltpu.VMEM), outs),
        compiler_params=pltpu.CompilerParams(vmem_limit_bytes=mib << 20),
        interpret=INTERPRET,
    )


def dot(a, b, dims=((1,), (0,))):
    return lax.dot_general(a, b, (dims, ((), ())), preferred_element_type=F32)


def parts(a):
    high = a.astype(BF16)
    return high, (a - high.astype(F32)).astype(BF16)


def dot_left(a, b, dims=((1,), (0,))):
    high, low = parts(a)
    return dot(high, b, dims) + dot(low, b, dims)


def dot_both(a, b, dims):
    a_high, a_low = parts(a)
    b_high, b_low = parts(b)
    return dot(a_high, b_high, dims) + (dot(a_high, b_low, dims) + dot(a_low, b_high, dims))


def norm_kernel(fs_ref, x_ref, gain_ref, *out_refs):
    values = x_ref[...].astype(F32)
    square_mean = jnp.mean(values * values, axis=-1, keepdims=True)
    normed = (values * lax.rsqrt(square_mean + epsilon) * gain_ref[...]).astype(BF16)
    count = len(out_refs)
    wide = count * HEAD
    target = lax.broadcasted_iota(jnp.int32, (wide, wide), 1)
    source = lax.broadcasted_iota(jnp.int32, (wide, wide), 0)
    owner = (target // HEAD + fs_ref[0]) % count
    inside = target % HEAD
    wanted = (inside // ROWS) * (count * ROWS) + owner * ROWS + inside % ROWS
    pick = (source == wanted).astype(BF16)
    for b in range(x_ref.shape[1] // wide):
        moved = dot(normed[:, b * wide : (b + 1) * wide], pick).astype(BF16)
        for k in range(count):
            out_refs[k][:, b * HEAD : (b + 1) * HEAD] = moved[:, k * HEAD : (k + 1) * HEAD]


def partial_kernel(*refs):
    count = (len(refs) - 1) // 3
    rows = refs[:count]
    weight = refs[count][...]
    first_refs = refs[count + 1 : 2 * count + 1]
    second_refs = refs[2 * count + 1 :]
    cut = first_refs[0].shape[1]
    for k in range(count):
        product = dot(rows[k][...], weight)
        first_refs[k][...] = product[:, :cut].astype(first_refs[k].dtype)
        second_refs[k][...] = product[:, cut:].astype(second_refs[k].dtype)


def sum_of(refs):
    total = refs[0][...]
    for ref in refs[1:]:
        total = total + ref[...].astype(F32)
    return total.astype(BF16)


def attention_inputs_kernel(*refs):
    message_ref, rest_ref, query_ref = refs[-3:]
    total = sum_of(refs[:-3])
    length = total.shape[0]
    message_ref[0:length] = total[:, 0:HEAD]
    message_ref[length : length + FIRST] = total[:FIRST, HEAD : 2 * HEAD]
    rest_ref[...] = total[FIRST:, HEAD : 2 * HEAD]
    query_ref[...] = total[:, 2 * HEAD :]


def local_recurrence_kernel(*refs):
    sums = refs[:-10]
    floor_ref, offset_ref, extra_ref, rest_ref, low_ref, high_ref = refs[-10:-4]
    message_ref, inner_ref, query_decayed_ref, gate_ref = refs[-4:]
    projected = sum_of(sums)
    columns = [projected[:, k * HEAD : (k + 1) * HEAD] for k in range(4)]
    query_b = columns[0].astype(F32)
    query = query_b / (1.0 + jnp.exp(-query_b))
    value = columns[2]
    gate_b = columns[3].astype(F32)
    gate_ref[...] = gate_b / (1.0 + jnp.exp(-gate_b))
    u = columns[1].astype(F32) + offset_ref[...]
    key = (1.0 - floor_ref[...]) / (1.0 + jnp.exp(u))
    log_forget = jnp.log(1.0 - key) + extra_ref[...]
    length = log_forget.shape[0]
    row = lax.broadcasted_iota(jnp.int32, (length, length), 0)
    col = lax.broadcasted_iota(jnp.int32, (length, length), 1)
    lower = (row >= col).astype(BF16)
    high = log_forget.astype(BF16)
    rest = log_forget - high.astype(F32)
    middle = rest.astype(BF16)
    low = (rest - middle.astype(F32)).astype(BF16)
    running = dot(lower, high) + (dot(lower, middle) + dot(lower, low))
    position = lax.broadcasted_iota(jnp.int32, (length, 1), 0)
    pairwise = jnp.where(row == col, dot_both(query, key, ((1,), (1,))), 0.0)
    half = 1
    while half < length:
        block = 2 * half
        if block >= 8:
            boundary = running.reshape(length // block, block, HEAD)[:, half - 1 : half]
            boundary = jnp.broadcast_to(boundary, (length // block, block, HEAD)).reshape(
                length, HEAD
            )
        else:
            tiles = running.reshape(length // 8, 8, HEAD)
            inside = lax.broadcasted_iota(jnp.int32, (1, 8, 1), 1) // block
            boundary = jnp.zeros_like(tiles)
            for k in range(8 // block):
                at = k * block + half - 1
                boundary = jnp.where(inside == k, tiles[:, at : at + 1], boundary)
            boundary = boundary.reshape(length, HEAD)
        second = (position // half) % 2 == 1
        after = jnp.where(second, query * jnp.exp(running - boundary), 0.0)
        before = jnp.where(second, 0.0, key * jnp.exp(boundary - running))
        chosen = (row // block == col // block) & (row // half != col // half) & (row > col)
        pairwise = jnp.where(chosen, dot_both(after, before, ((1,), (1,))), pairwise)
        half = block
    inner_ref[...] = dot_left(pairwise, value)
    final = running[length - 1 : length]
    query_decayed_ref[...] = query * jnp.exp(running)
    key_high, key_low = parts(key * jnp.exp(final - running))
    state = dot(value, key_high, ((0,), (0,))) + dot(value, key_low, ((0,), (0,)))
    at = 0
    vector = jnp.broadcast_to(jnp.exp(final), (TILE, HEAD)).astype(BF16)
    for piece in (rest_ref[...], state.astype(BF16), vector, low_ref[...], high_ref[...]):
        message_ref[at : at + piece.shape[0]] = piece
        at += piece.shape[0]


def chain(message_ref, start):
    def step(k, carry):
        decay_all, state = carry
        decay = message_ref[k, start + HEAD : start + HEAD + TILE].astype(F32)[0:1]
        return decay * decay_all, decay * state + message_ref[k, start : start + HEAD].astype(F32)

    return step, (jnp.ones((1, HEAD), F32), jnp.zeros((HEAD, HEAD), F32))


def attend(query, first_ref, second_ref, shift, k, total, is_own):
    length = query.shape[0]
    row = lax.broadcasted_iota(jnp.int32, (length, length), 0)
    col = lax.broadcasted_iota(jnp.int32, (length, length), 1)
    key = first_ref[k, 0:length]
    value = jnp.concatenate(
        [first_ref[k, length : length + FIRST], second_ref[k, 0 : length - FIRST]], axis=0
    )
    scores = dot(query, key, ((1,), (1,))) * HEAD ** (-0.5) + shift
    softplus = jnp.maximum(scores, 0.0) + jnp.log(1.0 + jnp.exp(-jnp.abs(scores)))
    if is_own:
        softplus = jnp.where(row > col, softplus, 0.0)
    spent = dot_left(softplus, (row >= col).astype(BF16)) + total
    weights = jnp.exp(scores - spent)
    if is_own:
        weights = jnp.where(row > col, weights, 0.0)
    return dot(weights.astype(BF16), value), spent[:, 0:1]


def as_row(total):
    return jnp.transpose(jnp.broadcast_to(total, (total.shape[0], HEAD)))[0:1]


def far_kernel(count_ref, shift_ref, query_ref, first_ref, second_ref, out_ref):
    shift = shift_ref[0]
    query = query_ref[...]
    length = query.shape[0]
    count = count_ref[0]

    def earlier(k, carry):
        weighted, total = carry
        more, total = attend(
            query, first_ref, second_ref, shift, count - 1 - k, total, False
        )
        return weighted + more, total

    weighted, total = lax.fori_loop(
        0, count, earlier, (jnp.zeros((length, HEAD), F32), jnp.zeros((length, 1), F32))
    )
    out_ref[0:length] = weighted.astype(BF16)
    row = as_row(total)
    high, low = parts(row)
    index = lax.broadcasted_iota(jnp.int32, (TILE, HEAD), 0)
    vector = jnp.zeros((TILE, HEAD), F32)
    pieces = [piece[:, k * HEAD : (k + 1) * HEAD] for piece in (high, low) for k in range(2)]
    for k, piece in enumerate(pieces):
        vector = jnp.where(index == k, piece.astype(F32), vector)
    out_ref[length : length + TILE] = vector.astype(BF16)
    step, start = chain(second_ref, length - FIRST)
    decay, state = lax.fori_loop(0, count, step, start)
    at = length + TILE
    out_ref[at : at + HEAD] = state.astype(BF16)


def final_kernel(
    place_ref,
    shift_ref,
    query_ref,
    first_ref,
    second_ref,
    far_ref,
    inner_ref,
    query_decayed_ref,
    gate_ref,
    gain_a_ref,
    gain_b_ref,
    weight_ref,
    out_ref,
    total_ref,
):
    place = place_ref[0]
    shift = shift_ref[0]
    query = query_ref[...]
    length = query.shape[0]
    at = length + TILE
    step, start = chain(second_ref, length - FIRST)
    decay, state = lax.fori_loop(0, place, step, start)
    state = state + decay * far_ref[at : at + HEAD].astype(F32)
    recurrent = inner_ref[...] + dot_both(query_decayed_ref[...], state, ((1,), (1,)))
    square_mean = jnp.mean(recurrent * recurrent, axis=-1, keepdims=True)
    mixed_b = (
        recurrent * lax.rsqrt(square_mean + epsilon) * gain_b_ref[...] * gate_ref[...]
    ).astype(BF16)
    carry = attend(query, first_ref, second_ref, shift, place, 0.0, True)

    def earlier(k, carry):
        weighted, total = carry
        more, total = attend(
            query, first_ref, second_ref, shift, place - 1 - k, total, False
        )
        return weighted + more, total

    weighted, total = lax.fori_loop(0, place, earlier, carry)
    weighted = weighted + jnp.exp(-total) * far_ref[0:length].astype(F32)
    vector = far_ref[length : length + TILE].astype(F32)
    far_row = jnp.concatenate(
        [vector[k : k + 1] + vector[k + 2 : k + 3] for k in range(2)], axis=1
    )
    total_row = as_row(total) + far_row
    total_ref[...] = jnp.log(jnp.maximum(1.0 - jnp.exp(-total_row), log_floor))
    square_mean = jnp.mean(weighted * weighted, axis=-1, keepdims=True)
    mixed_a = (weighted * lax.rsqrt(square_mean + epsilon) * gain_a_ref[...]).astype(BF16)
    mixed = jnp.concatenate([mixed_a, mixed_b], axis=1)
    fs, near = weight_ref.shape[:2]
    width = fs * ROWS
    for far in range(2):
        for s in range(near):
            both = jnp.concatenate(
                [weight_ref[:, s, far, k].reshape(width, HEAD) for k in range(2)], axis=1
            )
            at = (far * near + s) * width
            out_ref[:, at : at + width] = dot(mixed, both, ((1,), (1,))).astype(BF16)


def over_fs(shard):
    size = lax.axis_size("fs")
    copies = jnp.broadcast_to(shard[None], (size, *shard.shape))
    return lax.all_to_all(copies, "fs", 0, 0, tiled=True)


def turned(array, axis, places):
    size = lax.axis_size(axis)
    return lax.ppermute(array, axis, [(k, (k + places) % size) for k in range(size)])


def on_device(
    input_layer_rows,
    input_norm_gain,
    query_weight_attention,
    key_weight_attention,
    value_weight_attention,
    query_weight_recurrent,
    forget_weight_recurrent,
    value_weight_recurrent,
    gate_weight_recurrent,
    output_weight_attention,
    emitted_projection_linear_scan,
    score_offset,
    attention_norm_gain,
    recurrence_norm_gain,
    forget_floor,
    forget_offset,
    extra_log_decay,
):
    x = input_layer_rows[0]
    tokens, width = x.shape
    sp, fs, tp = (lax.axis_size(name) for name in ("sp", "fs", "tp"))
    half = sp // 2
    rank = lax.axis_index("sp").astype(jnp.int32)
    upper = rank >= half
    groups = [list(range(half)), list(range(half, sp))]
    shape = jax.ShapeDtypeStruct

    out_own = jnp.concatenate((output_weight_attention, emitted_projection_linear_scan), axis=0)
    out_other = turned(out_own, "sp", half)
    out_low = jnp.where(upper, out_other, out_own)
    out_high = jnp.where(upper, out_own, out_other)

    ahead = vmem_call(
        norm_kernel,
        tuple(shape((tokens, width // fs), BF16) for _ in range(fs)),
        3,
        (0,),
    )(
        lax.axis_index("fs").astype(jnp.int32).reshape(1),
        x,
        input_norm_gain.reshape(1, width),
    )
    rows = [ahead[0]] + [turned(ahead[k], "fs", k) for k in range(1, fs)]
    column = lax.all_gather(
        jnp.concatenate(
            (
                key_weight_attention,
                value_weight_attention,
                query_weight_attention,
                query_weight_recurrent,
                forget_weight_recurrent,
                value_weight_recurrent,
                gate_weight_recurrent,
            ),
            axis=1,
        ),
        "sp",
        axis=0,
        tiled=True,
    )
    products = vmem_call(
        partial_kernel,
        tuple(
            shape((tokens, columns * HEAD), F32 if k == 0 else BF16)
            for columns in (3, 4)
            for k in range(fs)
        ),
        fs + 1,
    )(*rows, column)
    first = [products[0]] + [turned(products[k], "fs", -k) for k in range(1, fs)]
    second = [products[fs]] + [turned(products[fs + k], "fs", -k) for k in range(1, fs)]

    message, rest, query = vmem_call(
        attention_inputs_kernel,
        (
            shape((tokens + FIRST, HEAD), BF16),
            shape((tokens - FIRST, HEAD), BF16),
            shape((tokens, HEAD), BF16),
        ),
        fs,
    )(*first)
    query_far = lax.ppermute(query, "sp", [(half + k, k) for k in range(half)])
    gathered_first = lax.all_gather(message, "sp", axis_index_groups=groups)
    small = shape((tokens, HEAD), F32)
    length = tokens - FIRST + HEAD + TILE + 4 * ROWS
    message, inner, query_decayed, gate = vmem_call(
        local_recurrence_kernel, (shape((length, HEAD), BF16), small, small, small), fs + 6
    )(
        *second,
        forget_floor.reshape(1, HEAD),
        forget_offset.reshape(1, HEAD),
        extra_log_decay[0],
        rest,
        out_low,
        out_high,
    )
    gathered_second = lax.all_gather(message, "sp", axis_index_groups=groups)
    far = vmem_call(far_kernel, shape((tokens + TILE + HEAD, HEAD), BF16), 5, (0, 1))(
        jnp.where(upper, 0, half).astype(jnp.int32).reshape(1),
        score_offset,
        query_far,
        gathered_first,
        gathered_second,
    )
    far = lax.ppermute(far, "sp", [(k, half + k) for k in range(half)])
    out_weights = over_fs(
        gathered_second[:, length - 4 * ROWS :].reshape(half, 2, 2, ROWS, HEAD)
    )
    projected, row_log_total = vmem_call(
        final_kernel,
        (shape((tokens, width), BF16), shape((1, tokens), F32)),
        12,
        (0, 1),
    )(
        (rank % half).reshape(1),
        score_offset,
        query,
        gathered_first,
        gathered_second,
        far,
        inner,
        query_decayed,
        gate,
        attention_norm_gain.reshape(1, HEAD),
        recurrence_norm_gain.reshape(1, HEAD),
        out_weights,
    )
    tiles = lax.all_to_all(projected.reshape(tp, tokens // tp, width), "tp", 0, 0, tiled=True)
    layer_out = jnp.sum(tiles.astype(F32), axis=0).astype(BF16)
    return (layer_out[None], row_log_total[None])


def solution(mesh):
    weight = P(("sp", "fs"), "tp")
    return jax.shard_map(
        on_device,
        mesh=mesh,
        in_specs=(
            P("fs", "sp", None),
            P(),
            *(weight for _ in range(9)),
            *(P("tp") for _ in range(5)),
            P("fs", "sp", "tp"),
        ),
        out_specs=(P("fs", ("sp", "tp"), None), P("fs", "tp", "sp")),
        check_vma=False,
    )
```

```python
import jax
import jax.numpy as jnp
from jax import lax
from jax.experimental import pallas as pl
from jax.experimental.pallas import tpu as pltpu
from jax.sharding import PartitionSpec as P

HEAD = 128
ROWS = 32
TILE = 16
NEAR = 4

epsilon = 1e-06
log_floor = 0.05
F32 = jnp.float32
BF16 = jnp.bfloat16
INTERPRET = False


def vmem_call(kernel, outs, n_in, smem=(), mib=16):
    specs = [
        pl.BlockSpec(memory_space=pltpu.SMEM if k in smem else pltpu.VMEM) for k in range(n_in)
    ]
    return pl.pallas_call(
        kernel,
        out_shape=outs,
        in_specs=specs,
        out_specs=jax.tree.map(lambda _: pl.BlockSpec(memory_space=pltpu.VMEM), outs),
        compiler_params=pltpu.CompilerParams(vmem_limit_bytes=mib << 20),
        interpret=INTERPRET,
    )


def dot(a, b, dims=((1,), (0,))):
    return lax.dot_general(a, b, (dims, ((), ())), preferred_element_type=F32)


def parts(a):
    high = a.astype(BF16)
    return high, (a - high.astype(F32)).astype(BF16)


def dot_left(a, b, dims=((1,), (0,))):
    high, low = parts(a)
    return dot(high, b, dims) + dot(low, b, dims)


def dot_both(a, b, dims):
    a_high, a_low = parts(a)
    b_high, b_low = parts(b)
    return dot(a_high, b_high, dims) + (dot(a_high, b_low, dims) + dot(a_low, b_high, dims))


def start_kernel(fs_ref, x_ref, gain_ref, *refs):
    weights, out_refs = refs[:9], refs[9:-2]
    packed_ref, own_ref = refs[-2:]
    for k in range(7):
        packed_ref[:, k * HEAD : (k + 1) * HEAD] = weights[k][...]
    for k in range(2):
        own_ref[k * ROWS : (k + 1) * ROWS] = weights[7 + k][...]
    values = x_ref[...].astype(F32)
    square_mean = jnp.mean(values * values, axis=-1, keepdims=True)
    normed = (values * lax.rsqrt(square_mean + epsilon) * gain_ref[...]).astype(BF16)
    count = len(out_refs)
    wide = count * HEAD
    target = lax.broadcasted_iota(jnp.int32, (wide, wide), 1)
    source = lax.broadcasted_iota(jnp.int32, (wide, wide), 0)
    owner = (target // HEAD + fs_ref[0]) % count
    inside = target % HEAD
    wanted = (inside // ROWS) * (count * ROWS) + owner * ROWS + inside % ROWS
    pick = (source == wanted).astype(BF16)
    for b in range(x_ref.shape[1] // wide):
        moved = dot(normed[:, b * wide : (b + 1) * wide], pick).astype(BF16)
        for k in range(count):
            out_refs[k][:, b * HEAD : (b + 1) * HEAD] = moved[:, k * HEAD : (k + 1) * HEAD]


def partial_kernel(fs_ref, *refs):
    rows, weight_ref, out_ref = refs[:-2], refs[-2], refs[-1]
    count = len(rows)
    weight = weight_ref[...]
    for k in range(count):
        out_ref[(fs_ref[0] + count - k) % count] = dot(rows[k][...], weight).astype(BF16)


def local_recurrence_kernel(*refs):
    group_ref, products_ref, floor_ref, offset_ref, extra_ref = refs[:5]
    own = refs[5:-5]
    message_ref, query_ref, inner_ref, query_decayed_ref, gate_ref = refs[-5:]
    total = products_ref[0].astype(F32)
    for k in range(1, products_ref.shape[0]):
        total = total + products_ref[k].astype(F32)
    total = total.astype(BF16)
    columns = [total[:, k * HEAD : (k + 1) * HEAD] for k in range(7)]
    query_ref[...] = columns[2]
    query_b = columns[3].astype(F32)
    query = query_b / (1.0 + jnp.exp(-query_b))
    value = columns[5]
    gate_b = columns[6].astype(F32)
    gate_ref[...] = gate_b / (1.0 + jnp.exp(-gate_b))
    u = columns[4].astype(F32) + offset_ref[...]
    key = (1.0 - floor_ref[...]) / (1.0 + jnp.exp(u))
    log_forget = jnp.log(1.0 - key) + extra_ref[...]
    length = log_forget.shape[0]
    row = lax.broadcasted_iota(jnp.int32, (length, length), 0)
    col = lax.broadcasted_iota(jnp.int32, (length, length), 1)
    lower = (row >= col).astype(BF16)
    high = log_forget.astype(BF16)
    rest = log_forget - high.astype(F32)
    middle = rest.astype(BF16)
    low = (rest - middle.astype(F32)).astype(BF16)
    running = dot(lower, high) + (dot(lower, middle) + dot(lower, low))
    position = lax.broadcasted_iota(jnp.int32, (length, 1), 0)
    pairwise = jnp.where(row == col, dot_both(query, key, ((1,), (1,))), 0.0)
    half = 1
    while half < length:
        block = 2 * half
        if block >= 8:
            boundary = running.reshape(length // block, block, HEAD)[:, half - 1 : half]
            boundary = jnp.broadcast_to(boundary, (length // block, block, HEAD)).reshape(
                length, HEAD
            )
        else:
            tiles = running.reshape(length // 8, 8, HEAD)
            inside = lax.broadcasted_iota(jnp.int32, (1, 8, 1), 1) // block
            boundary = jnp.zeros_like(tiles)
            for k in range(8 // block):
                at = k * block + half - 1
                boundary = jnp.where(inside == k, tiles[:, at : at + 1], boundary)
            boundary = boundary.reshape(length, HEAD)
        second = (position // half) % 2 == 1
        after = jnp.where(second, query * jnp.exp(running - boundary), 0.0)
        before = jnp.where(second, 0.0, key * jnp.exp(boundary - running))
        chosen = (row // block == col // block) & (row // half != col // half) & (row > col)
        pairwise = jnp.where(chosen, dot_both(after, before, ((1,), (1,))), pairwise)
        half = block
    inner_ref[...] = dot_left(pairwise, value)
    final = running[length - 1 : length]
    query_decayed_ref[...] = query * jnp.exp(running)
    key_high, key_low = parts(key * jnp.exp(final - running))
    state = dot(value, key_high, ((0,), (0,))) + dot(value, key_low, ((0,), (0,)))
    at = 0
    vector = jnp.broadcast_to(jnp.exp(final), (TILE, HEAD)).astype(BF16)
    for piece in (columns[0], columns[1], state.astype(BF16), vector):
        message_ref[at : at + piece.shape[0]] = piece
        at += piece.shape[0]
    groups = len(own)
    for k in range(groups):
        slot = (group_ref[0] + groups - k) % groups
        start = pl.multiple_of(at + slot * 2 * ROWS, TILE)
        message_ref[pl.ds(start, 2 * ROWS)] = own[k][...]


def chain(message_ref, start, count):
    def step(k, carry):
        decay_all, state = carry
        decay = message_ref[k, start + HEAD : start + HEAD + TILE].astype(F32)[0:1]
        return decay * decay_all, decay * state + message_ref[k, start : start + HEAD].astype(F32)

    return lax.fori_loop(
        0, count, step, (jnp.ones((1, HEAD), F32), jnp.zeros((HEAD, HEAD), F32))
    )


def attend(query, message_ref, shift, k, total, is_own):
    length = query.shape[0]
    row = lax.broadcasted_iota(jnp.int32, (length, length), 0)
    col = lax.broadcasted_iota(jnp.int32, (length, length), 1)
    key = message_ref[k, 0:length]
    value = message_ref[k, length : 2 * length]
    scores = dot(query, key, ((1,), (1,))) * HEAD ** (-0.5) + shift
    softplus = jnp.maximum(scores, 0.0) + jnp.log(1.0 + jnp.exp(-jnp.abs(scores)))
    if is_own:
        softplus = jnp.where(row > col, softplus, 0.0)
    spent = dot_left(softplus, (row >= col).astype(BF16)) + total
    weights = jnp.exp(scores - spent)
    if is_own:
        weights = jnp.where(row > col, weights, 0.0)
    return dot(weights.astype(BF16), value), spent[:, 0:1]


def attend_down(query, message_ref, shift, count, carry):
    def earlier(k, carry):
        weighted, total = carry
        more, total = attend(query, message_ref, shift, count - 1 - k, total, False)
        return weighted + more, total

    return lax.fori_loop(0, count, earlier, carry)


def as_row(total):
    return jnp.transpose(jnp.broadcast_to(total, (total.shape[0], HEAD)))[0:1]


def as_column(row):
    pieces = [
        jnp.transpose(jnp.broadcast_to(row[:, k : k + HEAD], (HEAD, HEAD)))[:, 0:1]
        for k in range(0, row.shape[1], HEAD)
    ]
    return jnp.concatenate(pieces, axis=0)


def far_kernel(group_ref, shift_ref, message_ref, *refs):
    count = len(refs) // 2
    shift = shift_ref[0]
    index = lax.broadcasted_iota(jnp.int32, (TILE, HEAD), 0)
    near = message_ref.shape[0]
    for j in range(count):
        query = refs[j][...]
        out_ref = refs[count + j]
        length = query.shape[0]
        wanted = jnp.where(group_ref[0] + j < count, near, 0)
        start = (jnp.zeros((length, HEAD), F32), jnp.zeros((length, 1), F32))
        weighted, total = attend_down(query, message_ref, shift, wanted, start)
        out_ref[0:length] = weighted.astype(BF16)
        if j == 0:
            decay, state = chain(message_ref, 2 * length, near)
            state = state.astype(BF16)
        high, low = parts(as_row(total))
        pieces = [piece[:, k * HEAD : (k + 1) * HEAD] for piece in (high, low) for k in range(2)]
        vector = jnp.zeros((TILE, HEAD), F32)
        for k, piece in enumerate(pieces + [decay]):
            vector = jnp.where(index == k, piece.astype(F32), vector)
        out_ref[length : length + TILE] = vector.astype(BF16)
        out_ref[length + TILE : length + TILE + HEAD] = state


def final_kernel(
    place_ref,
    shift_ref,
    query_ref,
    message_ref,
    inner_ref,
    query_decayed_ref,
    gate_ref,
    gain_a_ref,
    gain_b_ref,
    weight_ref,
    *refs,
):
    far_refs, out_ref, total_ref = refs[:-2], refs[-2], refs[-1]
    place = place_ref[0]
    shift = shift_ref[0]
    query = query_ref[...]
    length = query.shape[0]
    incoming = jnp.zeros((HEAD, HEAD), F32)
    outside = jnp.zeros((length, HEAD), F32)
    outside_row = jnp.zeros((1, length), F32)
    for ref in reversed(far_refs):
        vector = ref[length : length + TILE].astype(F32)
        row = jnp.concatenate(
            [vector[k : k + 1] + vector[k + 2 : k + 3] for k in range(2)], axis=1
        )
        incoming = vector[4:5] * incoming + ref[
            length + TILE : length + TILE + HEAD
        ].astype(F32)
        outside = ref[0:length].astype(F32) + jnp.exp(-as_column(row)) * outside
        outside_row = outside_row + row
    decay, state = chain(message_ref, 2 * length, place)
    state = state + decay * incoming
    recurrent = inner_ref[...] + dot_both(query_decayed_ref[...], state, ((1,), (1,)))
    square_mean = jnp.mean(recurrent * recurrent, axis=-1, keepdims=True)
    mixed_b = (
        recurrent * lax.rsqrt(square_mean + epsilon) * gain_b_ref[...] * gate_ref[...]
    ).astype(BF16)
    carry = attend(query, message_ref, shift, place, 0.0, True)
    weighted, total = attend_down(query, message_ref, shift, place, carry)
    weighted = weighted + jnp.exp(-total) * outside
    total_row = as_row(total) + outside_row
    total_ref[...] = jnp.log(jnp.maximum(1.0 - jnp.exp(-total_row), log_floor))
    square_mean = jnp.mean(weighted * weighted, axis=-1, keepdims=True)
    mixed_a = (weighted * lax.rsqrt(square_mean + epsilon) * gain_a_ref[...]).astype(BF16)
    mixed = jnp.concatenate([mixed_a, mixed_b], axis=1)
    fs, near, groups = weight_ref.shape[:3]
    width = fs * ROWS
    for group in range(groups):
        for s in range(near):
            both = jnp.concatenate(
                [weight_ref[:, s, group, k].reshape(width, HEAD) for k in range(2)], axis=1
            )
            at = (group * near + s) * width
            out_ref[:, at : at + width] = dot(mixed, both, ((1,), (1,))).astype(BF16)


def over_fs(shard):
    size = lax.axis_size("fs")
    copies = jnp.broadcast_to(shard[None], (size, *shard.shape))
    return lax.all_to_all(copies, "fs", 0, 0, tiled=True)


def turned(array, axis, places):
    size = lax.axis_size(axis)
    return lax.ppermute(array, axis, [(k, (k + places) % size) for k in range(size)])


def on_device(
    input_layer_rows,
    input_norm_gain,
    query_weight_attention,
    key_weight_attention,
    value_weight_attention,
    query_weight_recurrent,
    forget_weight_recurrent,
    value_weight_recurrent,
    gate_weight_recurrent,
    output_weight_attention,
    emitted_projection_linear_scan,
    score_offset,
    attention_norm_gain,
    recurrence_norm_gain,
    forget_floor,
    forget_offset,
    extra_log_decay,
):
    x = input_layer_rows[0]
    tokens, width = x.shape
    sp, fs, tp = (lax.axis_size(name) for name in ("sp", "fs", "tp"))
    count = sp // NEAR
    rank = lax.axis_index("sp").astype(jnp.int32)
    group = (rank // NEAR).reshape(1)
    fs_index = lax.axis_index("fs").astype(jnp.int32).reshape(1)
    shape = jax.ShapeDtypeStruct

    *ahead, packed, out_own = vmem_call(
        start_kernel,
        (
            *(shape((tokens, width // fs), BF16) for _ in range(fs)),
            shape((ROWS, 7 * HEAD), BF16),
            shape((2 * ROWS, HEAD), BF16),
        ),
        12,
        (0,),
    )(
        fs_index,
        x,
        input_norm_gain.reshape(1, width),
        key_weight_attention,
        value_weight_attention,
        query_weight_attention,
        query_weight_recurrent,
        forget_weight_recurrent,
        value_weight_recurrent,
        gate_weight_recurrent,
        output_weight_attention,
        emitted_projection_linear_scan,
    )
    rows = [ahead[0]] + [turned(ahead[k], "fs", k) for k in range(1, fs)]
    out_slots = [out_own] + [turned(out_own, "sp", NEAR * k) for k in range(1, count)]
    column = lax.all_gather(packed, "sp", axis=0, tiled=True)
    products = vmem_call(
        partial_kernel, shape((fs, tokens, 7 * HEAD), BF16), fs + 2, (0,)
    )(fs_index, *rows, column)
    products = lax.all_to_all(products, "fs", 0, 0, tiled=True)

    small = shape((tokens, HEAD), F32)
    start = 2 * tokens + HEAD + TILE
    message, query, inner, query_decayed, gate = vmem_call(
        local_recurrence_kernel,
        (
            shape((start + count * 2 * ROWS, HEAD), BF16),
            shape((tokens, HEAD), BF16),
            small,
            small,
            small,
        ),
        5 + count,
        (0,),
    )(
        group,
        products,
        forget_floor.reshape(1, HEAD),
        forget_offset.reshape(1, HEAD),
        extra_log_decay[0],
        *out_slots,
    )
    queries = [
        lax.ppermute(query, "sp", [(k, k - NEAR * j) for k in range(NEAR * j, sp)])
        for j in range(1, count)
    ]
    groups = [list(range(NEAR * k, NEAR * (k + 1))) for k in range(count)]
    gathered = lax.all_gather(message, "sp", axis_index_groups=groups)
    far = vmem_call(
        far_kernel,
        tuple(shape((tokens + TILE + HEAD, HEAD), BF16) for _ in queries),
        2 + count,
        (0, 1),
    )(group, score_offset, gathered, *queries)
    far = [
        lax.ppermute(far[j - 1], "sp", [(k, k + NEAR * j) for k in range(sp - NEAR * j)])
        for j in range(1, count)
    ]
    out_weights = over_fs(gathered[:, start:].reshape(NEAR, count, 2, ROWS, HEAD))
    projected, row_log_total = vmem_call(
        final_kernel,
        (shape((tokens, width), BF16), shape((1, tokens), F32)),
        9 + count,
        (0, 1),
    )(
        (rank % NEAR).reshape(1),
        score_offset,
        query,
        gathered,
        inner,
        query_decayed,
        gate,
        attention_norm_gain.reshape(1, HEAD),
        recurrence_norm_gain.reshape(1, HEAD),
        out_weights,
        *far,
    )
    tiles = lax.all_to_all(projected.reshape(tp, tokens // tp, width), "tp", 0, 0, tiled=True)
    layer_out = jnp.sum(tiles.astype(F32), axis=0).astype(BF16)
    return (layer_out[None], row_log_total[None])


def solution(mesh):
    weight = P(("sp", "fs"), "tp")
    return jax.shard_map(
        on_device,
        mesh=mesh,
        in_specs=(
            P("fs", "sp", None),
            P(),
            *(weight for _ in range(9)),
            *(P("tp") for _ in range(5)),
            P("fs", "sp", "tp"),
        ),
        out_specs=(P("fs", ("sp", "tp"), None), P("fs", "tp", "sp")),
        check_vma=False,
    )
```

```python
import jax
import jax.numpy as jnp
from jax import lax
from jax.experimental import pallas as pl
from jax.experimental.pallas import tpu as pltpu
from jax.sharding import PartitionSpec as P


HEAD = 128
ROWS = 32
TILE = 16
NEAR = 4

epsilon = 1e-06
log_floor = 0.05
F32 = jnp.float32
BF16 = jnp.bfloat16
INTERPRET = False


def vmem_call(kernel, outs, n_in, smem=(), hbm=(), scratch=(), mib=16):
    def space(k):
        return pltpu.SMEM if k in smem else pltpu.HBM if k in hbm else pltpu.VMEM

    return pl.pallas_call(
        kernel,
        out_shape=outs,
        in_specs=[pl.BlockSpec(memory_space=space(k)) for k in range(n_in)],
        out_specs=jax.tree.map(lambda _: pl.BlockSpec(memory_space=pltpu.VMEM), outs),
        scratch_shapes=list(scratch),
        compiler_params=pltpu.CompilerParams(vmem_limit_bytes=mib << 20),
        interpret=INTERPRET,
    )


def dot(a, b, dims=((1,), (0,))):
    return lax.dot_general(a, b, (dims, ((), ())), preferred_element_type=F32)


def parts(a):
    high = a.astype(BF16)
    return high, (a - high.astype(F32)).astype(BF16)


def dot_left(a, b, dims=((1,), (0,))):
    high, low = parts(a)
    return dot(high, b, dims) + dot(low, b, dims)


def dot_both(a, b, dims):
    a_high, a_low = parts(a)
    b_high, b_low = parts(b)
    return dot(a_high, b_high, dims) + (dot(a_high, b_low, dims) + dot(a_low, b_high, dims))


def start_kernel(x_hbm, gain_hbm, *refs):
    weights = refs[:9]
    slices_ref, packed_ref, own_ref, x_ref, gain_ref, arrived = refs[9:]
    copies = [
        pltpu.make_async_copy(x_hbm, x_ref, arrived.at[0]),
        pltpu.make_async_copy(gain_hbm, gain_ref, arrived.at[1]),
    ]
    for k in range(7):
        place = packed_ref.at[:, k * HEAD : (k + 1) * HEAD]
        copies.append(pltpu.make_async_copy(weights[k], place, arrived.at[2 + k]))
    for k in range(2):
        place = own_ref.at[k * ROWS : (k + 1) * ROWS]
        copies.append(pltpu.make_async_copy(weights[7 + k], place, arrived.at[9 + k]))
    for copy in copies:
        copy.start()
    for copy in copies:
        copy.wait()
    values = x_ref[...].astype(F32)
    square_mean = jnp.mean(values * values, axis=-1, keepdims=True)
    normed = (values * lax.rsqrt(square_mean + epsilon) * gain_ref[...]).astype(BF16)
    count = slices_ref.shape[0]
    wide = count * HEAD
    target = lax.broadcasted_iota(jnp.int32, (wide, wide), 1)
    source = lax.broadcasted_iota(jnp.int32, (wide, wide), 0)
    inside = target % HEAD
    wanted = (inside // ROWS) * (count * ROWS) + (target // HEAD) * ROWS + inside % ROWS
    pick = (source == wanted).astype(BF16)
    for b in range(x_ref.shape[1] // wide):
        moved = dot(normed[:, b * wide : (b + 1) * wide], pick).astype(BF16)
        for k in range(count):
            slices_ref[k, :, b * HEAD : (b + 1) * HEAD] = moved[:, k * HEAD : (k + 1) * HEAD]


def partial_kernel(rows_ref, weight_ref, out_ref):
    weight = weight_ref[...]
    for k in range(rows_ref.shape[0]):
        out_ref[k] = dot(rows_ref[k], weight).astype(BF16)


def local_recurrence_kernel(*refs):
    group_ref, products_ref, floor_ref, offset_ref, extra_hbm = refs[:5]
    own = refs[5:-7]
    message_ref, query_ref, inner_ref, query_decayed_ref, gate_ref, extra_ref, arrived = refs[-7:]
    copy = pltpu.make_async_copy(extra_hbm, extra_ref, arrived)
    copy.start()
    total = products_ref[0].astype(F32)
    for k in range(1, products_ref.shape[0]):
        total = total + products_ref[k].astype(F32)
    total = total.astype(BF16)
    columns = [total[:, k * HEAD : (k + 1) * HEAD] for k in range(7)]
    query_ref[...] = columns[2]
    query_b = columns[3].astype(F32)
    query = query_b / (1.0 + jnp.exp(-query_b))
    value = columns[5]
    gate_b = columns[6].astype(F32)
    gate_ref[...] = gate_b / (1.0 + jnp.exp(-gate_b))
    u = columns[4].astype(F32) + offset_ref[...]
    key = (1.0 - floor_ref[...]) / (1.0 + jnp.exp(u))
    copy.wait()
    log_forget = jnp.log(1.0 - key) + extra_ref[...]
    length = log_forget.shape[0]
    row = lax.broadcasted_iota(jnp.int32, (length, length), 0)
    col = lax.broadcasted_iota(jnp.int32, (length, length), 1)
    lower = (row >= col).astype(BF16)
    high = log_forget.astype(BF16)
    rest = log_forget - high.astype(F32)
    middle = rest.astype(BF16)
    low = (rest - middle.astype(F32)).astype(BF16)
    running = dot(lower, high) + (dot(lower, middle) + dot(lower, low))
    position = lax.broadcasted_iota(jnp.int32, (length, 1), 0)
    pairwise = jnp.where(row == col, dot_both(query, key, ((1,), (1,))), 0.0)
    half = 1
    while half < length:
        block = 2 * half
        if block >= 8:
            boundary = running.reshape(length // block, block, HEAD)[:, half - 1 : half]
            boundary = jnp.broadcast_to(boundary, (length // block, block, HEAD)).reshape(
                length, HEAD
            )
        else:
            tiles = running.reshape(length // 8, 8, HEAD)
            inside = lax.broadcasted_iota(jnp.int32, (1, 8, 1), 1) // block
            boundary = jnp.zeros_like(tiles)
            for k in range(8 // block):
                at = k * block + half - 1
                boundary = jnp.where(inside == k, tiles[:, at : at + 1], boundary)
            boundary = boundary.reshape(length, HEAD)
        second = (position // half) % 2 == 1
        after = jnp.where(second, query * jnp.exp(running - boundary), 0.0)
        before = jnp.where(second, 0.0, key * jnp.exp(boundary - running))
        chosen = (row // block == col // block) & (row // half != col // half) & (row > col)
        pairwise = jnp.where(chosen, dot_both(after, before, ((1,), (1,))), pairwise)
        half = block
    inner_ref[...] = dot_left(pairwise, value)
    final = running[length - 1 : length]
    query_decayed_ref[...] = query * jnp.exp(running)
    key_high, key_low = parts(key * jnp.exp(final - running))
    state = dot(value, key_high, ((0,), (0,))) + dot(value, key_low, ((0,), (0,)))
    at = 0
    vector = jnp.broadcast_to(jnp.exp(final), (TILE, HEAD)).astype(BF16)
    for piece in (columns[0], columns[1], state.astype(BF16), vector):
        message_ref[at : at + piece.shape[0]] = piece
        at += piece.shape[0]
    groups = len(own)
    for k in range(groups):
        slot = (group_ref[0] + groups - k) % groups
        start = pl.multiple_of(at + slot * 2 * ROWS, TILE)
        message_ref[pl.ds(start, 2 * ROWS)] = own[k][...]


def chain(message_ref, start, count):
    def step(k, carry):
        decay_all, state = carry
        decay = message_ref[k, start + HEAD : start + HEAD + TILE].astype(F32)[0:1]
        return decay * decay_all, decay * state + message_ref[k, start : start + HEAD].astype(F32)

    return lax.fori_loop(
        0, count, step, (jnp.ones((1, HEAD), F32), jnp.zeros((HEAD, HEAD), F32))
    )


def attend(query, message_ref, shift, k, ahead=None):
    length = query.shape[0]
    row = lax.broadcasted_iota(jnp.int32, (length, length), 0)
    col = lax.broadcasted_iota(jnp.int32, (length, length), 1)
    key = message_ref[k, 0:length]
    value = message_ref[k, length : 2 * length]
    scores = dot(query, key, ((1,), (1,))) * HEAD ** (-0.5) + shift
    softplus = jnp.maximum(scores, 0.0) + jnp.log(1.0 + jnp.exp(-jnp.abs(scores)))
    if ahead is not None:
        seen = row + ahead * length > col
        softplus = jnp.where(seen, softplus, 0.0)
    spent = dot_left(softplus, (row >= col).astype(BF16))
    weights = jnp.exp(scores - spent)
    if ahead is not None:
        weights = jnp.where(seen, weights, 0.0)
    return dot(weights.astype(BF16), value), spent[:, 0:1]


def attend_near(query, message_ref, shift, place=None):
    weighted, total = None, None
    for k in reversed(range(message_ref.shape[0])):
        ahead = None if place is None else place - k
        more, spent = attend(query, message_ref, shift, k, ahead)
        weighted = more if weighted is None else weighted + jnp.exp(-total) * more
        total = spent if total is None else total + spent
    return weighted, total


def as_row(total):
    return jnp.transpose(jnp.broadcast_to(total, (total.shape[0], HEAD)))[0:1]


def as_column(row):
    pieces = [
        jnp.transpose(jnp.broadcast_to(row[:, k : k + HEAD], (HEAD, HEAD)))[:, 0:1]
        for k in range(0, row.shape[1], HEAD)
    ]
    return jnp.concatenate(pieces, axis=0)


def far_kernel(group_ref, shift_ref, message_ref, *refs):
    count = len(refs) // 2
    shift = shift_ref[0]
    near = message_ref.shape[0]
    length = refs[0].shape[0]
    for j in range(count):
        out_ref = refs[count + j]
        wanted = group_ref[0] + j < count

        @pl.when(wanted)
        def _(query_ref=refs[j], out_ref=out_ref):
            weighted, total = attend_near(query_ref[...], message_ref, shift)
            out_ref[0:length] = weighted.astype(BF16)
            decay, state = chain(message_ref, 2 * length, near)
            high, low = parts(as_row(total))
            pieces = [
                piece[:, k * HEAD : (k + 1) * HEAD] for piece in (high, low) for k in range(2)
            ]
            index = lax.broadcasted_iota(jnp.int32, (TILE, HEAD), 0)
            vector = jnp.zeros((TILE, HEAD), F32)
            for k, piece in enumerate(pieces + [decay]):
                vector = jnp.where(index == k, piece.astype(F32), vector)
            out_ref[length : length + TILE] = vector.astype(BF16)
            out_ref[length + TILE : length + TILE + HEAD] = state.astype(BF16)

        @pl.when(jnp.logical_not(wanted))
        def _(out_ref=out_ref):
            out_ref[...] = jnp.zeros(out_ref.shape, BF16)


def final_kernel(
    place_ref,
    shift_ref,
    query_ref,
    message_ref,
    inner_ref,
    query_decayed_ref,
    gate_ref,
    gain_a_ref,
    gain_b_ref,
    weight_ref,
    *refs,
):
    far_refs, out_ref, total_ref = refs[:-2], refs[-2], refs[-1]
    place = place_ref[0]
    shift = shift_ref[0]
    query = query_ref[...]
    length = query.shape[0]
    incoming = jnp.zeros((HEAD, HEAD), F32)
    outside = jnp.zeros((length, HEAD), F32)
    outside_row = jnp.zeros((1, length), F32)
    for ref in reversed(far_refs):
        vector = ref[length : length + TILE].astype(F32)
        row = jnp.concatenate(
            [vector[k : k + 1] + vector[k + 2 : k + 3] for k in range(2)], axis=1
        )
        incoming = vector[4:5] * incoming + ref[
            length + TILE : length + TILE + HEAD
        ].astype(F32)
        outside = ref[0:length].astype(F32) + jnp.exp(-as_column(row)) * outside
        outside_row = outside_row + row
    decay, state = chain(message_ref, 2 * length, place)
    state = state + decay * incoming
    recurrent = inner_ref[...] + dot_both(query_decayed_ref[...], state, ((1,), (1,)))
    square_mean = jnp.mean(recurrent * recurrent, axis=-1, keepdims=True)
    mixed_b = (
        recurrent * lax.rsqrt(square_mean + epsilon) * gain_b_ref[...] * gate_ref[...]
    ).astype(BF16)
    weighted, total = attend_near(query, message_ref, shift, place)
    weighted = weighted + jnp.exp(-total) * outside
    total_row = as_row(total) + outside_row
    total_ref[...] = jnp.log(jnp.maximum(1.0 - jnp.exp(-total_row), log_floor))
    square_mean = jnp.mean(weighted * weighted, axis=-1, keepdims=True)
    mixed_a = (weighted * lax.rsqrt(square_mean + epsilon) * gain_a_ref[...]).astype(BF16)
    mixed = jnp.concatenate([mixed_a, mixed_b], axis=1)
    fs, near, groups = weight_ref.shape[:3]
    width = fs * ROWS
    for group in range(groups):
        for s in range(near):
            both = jnp.concatenate(
                [weight_ref[:, s, group, k].reshape(width, HEAD) for k in range(2)], axis=1
            )
            at = (group * near + s) * width
            out_ref[:, at : at + width] = dot(mixed, both, ((1,), (1,))).astype(BF16)


def over_fs(shard):
    size = lax.axis_size("fs")
    copies = jnp.broadcast_to(shard[None], (size, *shard.shape))
    return lax.all_to_all(copies, "fs", 0, 0, tiled=True)


def turned(array, axis, places):
    size = lax.axis_size(axis)
    return lax.ppermute(array, axis, [(k, (k + places) % size) for k in range(size)])


def on_device(
    input_layer_rows,
    input_norm_gain,
    query_weight_attention,
    key_weight_attention,
    value_weight_attention,
    query_weight_recurrent,
    forget_weight_recurrent,
    value_weight_recurrent,
    gate_weight_recurrent,
    output_weight_attention,
    emitted_projection_linear_scan,
    score_offset,
    attention_norm_gain,
    recurrence_norm_gain,
    forget_floor,
    forget_offset,
    extra_log_decay,
):
    x = input_layer_rows[0]
    tokens, width = x.shape
    sp, fs, tp = (lax.axis_size(name) for name in ("sp", "fs", "tp"))
    count = sp // NEAR
    rank = lax.axis_index("sp").astype(jnp.int32)
    group = (rank // NEAR).reshape(1)
    shape = jax.ShapeDtypeStruct

    slices, packed, out_own = vmem_call(
        start_kernel,
        (
            shape((fs, tokens, width // fs), BF16),
            shape((ROWS, 7 * HEAD), BF16),
            shape((2 * ROWS, HEAD), BF16),
        ),
        11,
        hbm=range(11),
        scratch=(
            pltpu.VMEM((tokens, width), BF16),
            pltpu.VMEM((1, width), F32),
            pltpu.SemaphoreType.DMA((11,)),
        ),
        mib=58,
    )(
        x,
        input_norm_gain.reshape(1, width),
        key_weight_attention,
        value_weight_attention,
        query_weight_attention,
        query_weight_recurrent,
        forget_weight_recurrent,
        value_weight_recurrent,
        gate_weight_recurrent,
        output_weight_attention,
        emitted_projection_linear_scan,
    )
    rows = lax.all_to_all(slices, "fs", 0, 0, tiled=True)
    out_slots = [out_own] + [turned(out_own, "sp", NEAR * k) for k in range(1, count)]
    column = lax.all_gather(packed, "sp", axis=0, tiled=True)
    products = vmem_call(partial_kernel, shape((fs, tokens, 7 * HEAD), BF16), 2)(rows, column)
    products = lax.all_to_all(products, "fs", 0, 0, tiled=True)

    small = shape((tokens, HEAD), F32)
    start = 2 * tokens + HEAD + TILE
    message, query, inner, query_decayed, gate = vmem_call(
        local_recurrence_kernel,
        (
            shape((start + count * 2 * ROWS, HEAD), BF16),
            shape((tokens, HEAD), BF16),
            small,
            small,
            small,
        ),
        5 + count,
        (0,),
        (4,),
        (pltpu.VMEM((tokens, HEAD), F32), pltpu.SemaphoreType.DMA(())),
    )(
        group,
        products,
        forget_floor.reshape(1, HEAD),
        forget_offset.reshape(1, HEAD),
        extra_log_decay[0],
        *out_slots,
    )
    queries = []
    for j in range(1, count):
        places = [(k, k - NEAR * j) for k in range(NEAR * j, sp)]
        queries.append(lax.ppermute(query, "sp", places))
    groups = [list(range(NEAR * k, NEAR * (k + 1))) for k in range(count)]
    gathered = lax.all_gather(message, "sp", axis_index_groups=groups)
    far = vmem_call(
        far_kernel,
        tuple(shape((tokens + TILE + HEAD, HEAD), BF16) for _ in queries),
        2 + count,
        (0, 1),
    )(group, score_offset, gathered, *queries)
    far = [
        lax.ppermute(far[j - 1], "sp", [(k, k + NEAR * j) for k in range(sp - NEAR * j)])
        for j in range(1, count)
    ]
    out_weights = over_fs(gathered[:, start:].reshape(NEAR, count, 2, ROWS, HEAD))
    projected, row_log_total = vmem_call(
        final_kernel,
        (shape((tokens, width), BF16), shape((1, tokens), F32)),
        9 + count,
        (0, 1),
    )(
        (rank % NEAR).reshape(1),
        score_offset,
        query,
        gathered,
        inner,
        query_decayed,
        gate,
        attention_norm_gain.reshape(1, HEAD),
        recurrence_norm_gain.reshape(1, HEAD),
        out_weights,
        *far,
    )
    tiles = lax.all_to_all(projected.reshape(tp, tokens // tp, width), "tp", 0, 0, tiled=True)
    layer_out = jnp.sum(tiles.astype(F32), axis=0).astype(BF16)
    return (layer_out[None], row_log_total[None])


def solution(mesh):
    weight = P(("sp", "fs"), "tp")
    return jax.shard_map(
        on_device,
        mesh=mesh,
        in_specs=(
            P("fs", "sp", None),
            P(),
            *(weight for _ in range(9)),
            *(P("tp") for _ in range(5)),
            P("fs", "sp", "tp"),
        ),
        out_specs=(P("fs", ("sp", "tp"), None), P("fs", "tp", "sp")),
        check_vma=False,
    )
```

```python
import jax
import jax.numpy as jnp
from jax import lax
from jax.experimental import pallas as pl
from jax.experimental.pallas import tpu as pltpu
from jax.sharding import PartitionSpec as P


HEAD = 128
ROWS = 32
TILE = 16
NEAR = 4

epsilon = 1e-06
log_floor = 0.05
F32 = jnp.float32
BF16 = jnp.bfloat16
INTERPRET = False


def vmem_call(kernel, outs, n_in, smem=(), hbm=(), scratch=(), mib=16):
    def space(k):
        return pltpu.SMEM if k in smem else pltpu.HBM if k in hbm else pltpu.VMEM

    return pl.pallas_call(
        kernel,
        out_shape=outs,
        in_specs=[pl.BlockSpec(memory_space=space(k)) for k in range(n_in)],
        out_specs=jax.tree.map(lambda _: pl.BlockSpec(memory_space=pltpu.VMEM), outs),
        scratch_shapes=list(scratch),
        compiler_params=pltpu.CompilerParams(vmem_limit_bytes=mib << 20),
        interpret=INTERPRET,
    )


def dot(a, b, dims=((1,), (0,))):
    return lax.dot_general(a, b, (dims, ((), ())), preferred_element_type=F32)


def parts(a):
    high = a.astype(BF16)
    return high, (a - high.astype(F32)).astype(BF16)


def dot_left(a, b, dims=((1,), (0,))):
    high, low = parts(a)
    return dot(high, b, dims) + dot(low, b, dims)


def dot_both(a, b, dims):
    a_high, a_low = parts(a)
    b_high, b_low = parts(b)
    return dot(a_high, b_high, dims) + (dot(a_high, b_low, dims) + dot(a_low, b_high, dims))


def start_kernel(x_hbm, gain_hbm, *refs):
    weights = refs[:9]
    slices_ref, packed_ref, own_ref, x_ref, gain_ref, arrived = refs[9:]
    copies = [
        pltpu.make_async_copy(x_hbm, x_ref, arrived.at[0]),
        pltpu.make_async_copy(gain_hbm, gain_ref, arrived.at[1]),
    ]
    for k in range(7):
        place = packed_ref.at[:, k * HEAD : (k + 1) * HEAD]
        copies.append(pltpu.make_async_copy(weights[k], place, arrived.at[2 + k]))
    for k in range(2):
        place = own_ref.at[k * ROWS : (k + 1) * ROWS]
        copies.append(pltpu.make_async_copy(weights[7 + k], place, arrived.at[9 + k]))
    for copy in copies:
        copy.start()
    for copy in copies:
        copy.wait()
    values = x_ref[...].astype(F32)
    square_mean = jnp.mean(values * values, axis=-1, keepdims=True)
    normed = (values * lax.rsqrt(square_mean + epsilon) * gain_ref[...]).astype(BF16)
    count = slices_ref.shape[0]
    wide = count * HEAD
    target = lax.broadcasted_iota(jnp.int32, (wide, wide), 1)
    source = lax.broadcasted_iota(jnp.int32, (wide, wide), 0)
    inside = target % HEAD
    wanted = (inside // ROWS) * (count * ROWS) + (target // HEAD) * ROWS + inside % ROWS
    pick = (source == wanted).astype(BF16)
    for b in range(x_ref.shape[1] // wide):
        moved = dot(normed[:, b * wide : (b + 1) * wide], pick).astype(BF16)
        for k in range(count):
            slices_ref[k, :, b * HEAD : (b + 1) * HEAD] = moved[:, k * HEAD : (k + 1) * HEAD]


def partial_kernel(rows_ref, weight_ref, first_ref, second_ref):
    cut = first_ref.shape[2]
    weight = weight_ref[...]
    for k in range(rows_ref.shape[0]):
        first_ref[k] = dot(rows_ref[k], weight[:, :cut]).astype(BF16)
    for k in range(rows_ref.shape[0]):
        second_ref[k] = dot(rows_ref[k], weight[:, cut:]).astype(BF16)


def sum_of(products_ref):
    total = products_ref[0].astype(F32)
    for k in range(1, products_ref.shape[0]):
        total = total + products_ref[k].astype(F32)
    return total.astype(BF16)


def attention_inputs_kernel(products_ref, own_ref, far_ref, key_value_ref):
    total = sum_of(products_ref)
    length = total.shape[0]
    key_value_ref[0:length] = total[:, 0:HEAD]
    key_value_ref[length : 2 * length] = total[:, HEAD : 2 * HEAD]
    far_ref[0:length] = total[:, 2 * HEAD :]
    far_ref[length : length + 2 * ROWS] = own_ref[...]


def local_recurrence_kernel(*refs):
    products_ref, floor_ref, offset_ref, extra_hbm, key_value_ref, slots_ref = refs[:6]
    message_ref, inner_ref, query_decayed_ref, gate_ref, extra_ref, arrived = refs[6:]
    copy = pltpu.make_async_copy(extra_hbm, extra_ref, arrived)
    copy.start()
    total = sum_of(products_ref)
    columns = [total[:, k * HEAD : (k + 1) * HEAD] for k in range(4)]
    query_b = columns[0].astype(F32)
    query = query_b / (1.0 + jnp.exp(-query_b))
    value = columns[2]
    gate_b = columns[3].astype(F32)
    gate_ref[...] = gate_b / (1.0 + jnp.exp(-gate_b))
    u = columns[1].astype(F32) + offset_ref[...]
    key = (1.0 - floor_ref[...]) / (1.0 + jnp.exp(u))
    copy.wait()
    log_forget = jnp.log(1.0 - key) + extra_ref[...]
    length = log_forget.shape[0]
    row = lax.broadcasted_iota(jnp.int32, (length, length), 0)
    col = lax.broadcasted_iota(jnp.int32, (length, length), 1)
    lower = (row >= col).astype(BF16)
    high = log_forget.astype(BF16)
    rest = log_forget - high.astype(F32)
    middle = rest.astype(BF16)
    low = (rest - middle.astype(F32)).astype(BF16)
    running = dot(lower, high) + (dot(lower, middle) + dot(lower, low))
    position = lax.broadcasted_iota(jnp.int32, (length, 1), 0)
    pairwise = jnp.where(row == col, dot_both(query, key, ((1,), (1,))), 0.0)
    half = 1
    while half < length:
        block = 2 * half
        if block >= 8:
            boundary = running.reshape(length // block, block, HEAD)[:, half - 1 : half]
            boundary = jnp.broadcast_to(boundary, (length // block, block, HEAD)).reshape(
                length, HEAD
            )
        else:
            tiles = running.reshape(length // 8, 8, HEAD)
            inside = lax.broadcasted_iota(jnp.int32, (1, 8, 1), 1) // block
            boundary = jnp.zeros_like(tiles)
            for k in range(8 // block):
                at = k * block + half - 1
                boundary = jnp.where(inside == k, tiles[:, at : at + 1], boundary)
            boundary = boundary.reshape(length, HEAD)
        second = (position // half) % 2 == 1
        after = jnp.where(second, query * jnp.exp(running - boundary), 0.0)
        before = jnp.where(second, 0.0, key * jnp.exp(boundary - running))
        chosen = (row // block == col // block) & (row // half != col // half) & (row > col)
        pairwise = jnp.where(chosen, dot_both(after, before, ((1,), (1,))), pairwise)
        half = block
    inner_ref[...] = dot_left(pairwise, value)
    final = running[length - 1 : length]
    query_decayed_ref[...] = query * jnp.exp(running)
    key_high, key_low = parts(key * jnp.exp(final - running))
    state = dot(value, key_high, ((0,), (0,))) + dot(value, key_low, ((0,), (0,)))
    at = 0
    vector = jnp.broadcast_to(jnp.exp(final), (TILE, HEAD)).astype(BF16)
    for piece in (key_value_ref[...], state.astype(BF16), vector):
        message_ref[at : at + piece.shape[0]] = piece
        at += piece.shape[0]
    for k in range(slots_ref.shape[0]):
        message_ref[at : at + 2 * ROWS] = slots_ref[k, slots_ref.shape[1] - 2 * ROWS :]
        at += 2 * ROWS


def chain(message_ref, start, count):
    def step(k, carry):
        decay_all, state = carry
        decay = message_ref[k, start + HEAD : start + HEAD + TILE].astype(F32)[0:1]
        return decay * decay_all, decay * state + message_ref[k, start : start + HEAD].astype(F32)

    return lax.fori_loop(
        0, count, step, (jnp.ones((1, HEAD), F32), jnp.zeros((HEAD, HEAD), F32))
    )


def attend(query, message_ref, shift, k, ahead=None):
    length = query.shape[0]
    row = lax.broadcasted_iota(jnp.int32, (length, length), 0)
    col = lax.broadcasted_iota(jnp.int32, (length, length), 1)
    key = message_ref[k, 0:length]
    value = message_ref[k, length : 2 * length]
    scores = dot(query, key, ((1,), (1,))) * HEAD ** (-0.5) + shift
    softplus = jnp.maximum(scores, 0.0) + jnp.log(1.0 + jnp.exp(-jnp.abs(scores)))
    if ahead is not None:
        seen = row + ahead * length > col
        softplus = jnp.where(seen, softplus, 0.0)
    spent = dot_left(softplus, (row >= col).astype(BF16))
    weights = jnp.exp(scores - spent)
    if ahead is not None:
        weights = jnp.where(seen, weights, 0.0)
    return dot(weights.astype(BF16), value), spent[:, 0:1]


def attend_near(query, message_ref, shift, place=None):
    weighted, total = None, None
    for k in reversed(range(message_ref.shape[0])):
        ahead = None if place is None else place - k
        more, spent = attend(query, message_ref, shift, k, ahead)
        weighted = more if weighted is None else weighted + jnp.exp(-total) * more
        total = spent if total is None else total + spent
    return weighted, total


def as_row(total):
    return jnp.transpose(jnp.broadcast_to(total, (total.shape[0], HEAD)))[0:1]


def as_column(row):
    pieces = [
        jnp.transpose(jnp.broadcast_to(row[:, k : k + HEAD], (HEAD, HEAD)))[:, 0:1]
        for k in range(0, row.shape[1], HEAD)
    ]
    return jnp.concatenate(pieces, axis=0)


def far_kernel(group_ref, shift_ref, message_ref, query_ref, *out_refs):
    count = query_ref.shape[0]
    length = message_ref.shape[1] - count * 2 * ROWS - HEAD - TILE
    length = length // 2
    shift = shift_ref[0]
    near = message_ref.shape[0]
    index = lax.broadcasted_iota(jnp.int32, (TILE, HEAD), 0)
    for j, out_ref in enumerate(out_refs):
        wanted = group_ref[0] + j + 1 < count

        @pl.when(wanted)
        def _(j=j, out_ref=out_ref):
            query = query_ref[group_ref[0] + j + 1, 0:length]
            weighted, total = attend_near(query, message_ref, shift)
            out_ref[0:length] = weighted.astype(BF16)
            decay, state = chain(message_ref, 2 * length, near)
            high, low = parts(as_row(total))
            pieces = [
                piece[:, k * HEAD : (k + 1) * HEAD] for piece in (high, low) for k in range(2)
            ]
            vector = jnp.zeros((TILE, HEAD), F32)
            for k, piece in enumerate(pieces + [decay]):
                vector = jnp.where(index == k, piece.astype(F32), vector)
            out_ref[length : length + TILE] = vector.astype(BF16)
            out_ref[length + TILE : length + TILE + HEAD] = state.astype(BF16)

        @pl.when(jnp.logical_not(wanted))
        def _(out_ref=out_ref):
            out_ref[...] = jnp.zeros(out_ref.shape, BF16)


def near_kernel(place_ref, shift_ref, query_ref, message_ref, weighted_ref, total_ref):
    place = place_ref[0]
    length = weighted_ref.shape[0]
    weighted, total = attend_near(query_ref[0:length], message_ref, shift_ref[0], place)
    weighted_ref[...] = weighted
    total_ref[...] = jnp.broadcast_to(total, total_ref.shape)


def final_kernel(
    place_ref,
    message_ref,
    weighted_ref,
    spent_ref,
    inner_ref,
    query_decayed_ref,
    gate_ref,
    gain_a_ref,
    gain_b_ref,
    weight_ref,
    *refs,
):
    far_refs, out_ref, total_ref = refs[:-2], refs[-2], refs[-1]
    length = weighted_ref.shape[0]
    incoming = jnp.zeros((HEAD, HEAD), F32)
    outside = jnp.zeros((length, HEAD), F32)
    outside_row = jnp.zeros((1, length), F32)
    for ref in reversed(far_refs):
        vector = ref[length : length + TILE].astype(F32)
        row = jnp.concatenate(
            [vector[k : k + 1] + vector[k + 2 : k + 3] for k in range(2)], axis=1
        )
        incoming = vector[4:5] * incoming + ref[
            length + TILE : length + TILE + HEAD
        ].astype(F32)
        outside = ref[0:length].astype(F32) + jnp.exp(-as_column(row)) * outside
        outside_row = outside_row + row
    decay, state = chain(message_ref, 2 * length, place_ref[0])
    state = state + decay * incoming
    recurrent = inner_ref[...] + dot_both(query_decayed_ref[...], state, ((1,), (1,)))
    square_mean = jnp.mean(recurrent * recurrent, axis=-1, keepdims=True)
    mixed_b = (
        recurrent * lax.rsqrt(square_mean + epsilon) * gain_b_ref[...] * gate_ref[...]
    ).astype(BF16)
    total = spent_ref[...]
    weighted = weighted_ref[...] + jnp.exp(-total) * outside
    total_row = jnp.transpose(total)[0:1] + outside_row
    total_ref[...] = jnp.log(jnp.maximum(1.0 - jnp.exp(-total_row), log_floor))
    square_mean = jnp.mean(weighted * weighted, axis=-1, keepdims=True)
    mixed_a = (weighted * lax.rsqrt(square_mean + epsilon) * gain_a_ref[...]).astype(BF16)
    mixed = jnp.concatenate([mixed_a, mixed_b], axis=1)
    fs, near, groups = weight_ref.shape[:3]
    width = fs * ROWS
    for group in range(groups):
        for s in range(near):
            both = jnp.concatenate(
                [weight_ref[:, s, group, k].reshape(width, HEAD) for k in range(2)], axis=1
            )
            at = (group * near + s) * width
            out_ref[:, at : at + width] = dot(mixed, both, ((1,), (1,))).astype(BF16)


def copies(array, size):
    return jnp.broadcast_to(array[None], (size, *array.shape))


def on_device(
    input_layer_rows,
    input_norm_gain,
    query_weight_attention,
    key_weight_attention,
    value_weight_attention,
    query_weight_recurrent,
    forget_weight_recurrent,
    value_weight_recurrent,
    gate_weight_recurrent,
    output_weight_attention,
    emitted_projection_linear_scan,
    score_offset,
    attention_norm_gain,
    recurrence_norm_gain,
    forget_floor,
    forget_offset,
    extra_log_decay,
):
    x = input_layer_rows[0]
    tokens, width = x.shape
    sp, fs, tp = (lax.axis_size(name) for name in ("sp", "fs", "tp"))
    count = sp // NEAR
    rank = lax.axis_index("sp").astype(jnp.int32)
    group = (rank // NEAR).reshape(1)
    shape = jax.ShapeDtypeStruct

    slices, packed, out_own = vmem_call(
        start_kernel,
        (
            shape((fs, tokens, width // fs), BF16),
            shape((ROWS, 7 * HEAD), BF16),
            shape((2 * ROWS, HEAD), BF16),
        ),
        11,
        hbm=range(11),
        scratch=(
            pltpu.VMEM((tokens, width), BF16),
            pltpu.VMEM((1, width), F32),
            pltpu.SemaphoreType.DMA((11,)),
        ),
        mib=58,
    )(
        x,
        input_norm_gain.reshape(1, width),
        key_weight_attention,
        value_weight_attention,
        query_weight_attention,
        query_weight_recurrent,
        forget_weight_recurrent,
        value_weight_recurrent,
        gate_weight_recurrent,
        output_weight_attention,
        emitted_projection_linear_scan,
    )
    rows = lax.all_to_all(slices, "fs", 0, 0, tiled=True)
    column = lax.all_gather(packed, "sp", axis=0, tiled=True)
    first, second = vmem_call(
        partial_kernel,
        tuple(shape((fs, tokens, columns * HEAD), BF16) for columns in (3, 4)),
        2,
    )(rows, column)
    first = lax.all_to_all(first, "fs", 0, 0, tiled=True)
    own, key_value = vmem_call(
        attention_inputs_kernel,
        (shape((tokens + 2 * ROWS, HEAD), BF16), shape((2 * tokens, HEAD), BF16)),
        2,
    )(first, out_own)
    second, _ = lax.optimization_barrier((second, own))
    second = lax.all_to_all(second, "fs", 0, 0, tiled=True)
    strided = [list(range(k, sp, NEAR)) for k in range(NEAR)]
    across = lax.all_gather(own, "sp", axis_index_groups=strided)

    small = shape((tokens, HEAD), F32)
    start = 2 * tokens + HEAD + TILE
    message, inner, query_decayed, gate = vmem_call(
        local_recurrence_kernel,
        (shape((start + count * 2 * ROWS, HEAD), BF16), small, small, small),
        6,
        (),
        (3,),
        (pltpu.VMEM((tokens, HEAD), F32), pltpu.SemaphoreType.DMA(())),
    )(
        second,
        forget_floor.reshape(1, HEAD),
        forget_offset.reshape(1, HEAD),
        extra_log_decay[0],
        key_value,
        across,
    )
    groups = [list(range(NEAR * k, NEAR * (k + 1))) for k in range(count)]
    gathered = lax.all_gather(message, "sp", axis_index_groups=groups)
    out_weights = lax.all_to_all(
        copies(gathered[:, start:].reshape(NEAR, count, 2, ROWS, HEAD), fs),
        "fs",
        0,
        0,
        tiled=True,
    )
    far = vmem_call(
        far_kernel,
        tuple(shape((tokens + TILE + HEAD, HEAD), BF16) for _ in range(count - 1)),
        4,
        (0, 1),
    )(group, score_offset, gathered, across)
    outside = []
    for j in range(1, count):
        places = [(k, k + NEAR * j) for k in range(sp - NEAR * j)]
        outside.append(lax.ppermute(far[j - 1], "sp", places))
    place = (rank % NEAR).reshape(1)
    weighted, spent = vmem_call(near_kernel, (small, small), 4, (0, 1))(
        place, score_offset, own, gathered
    )
    projected, row_log_total = vmem_call(
        final_kernel,
        (shape((tokens, width), BF16), shape((1, tokens), F32)),
        9 + count,
        (0,),
    )(
        place,
        gathered,
        weighted,
        spent,
        inner,
        query_decayed,
        gate,
        attention_norm_gain.reshape(1, HEAD),
        recurrence_norm_gain.reshape(1, HEAD),
        out_weights,
        *outside,
    )
    tiles = lax.all_to_all(projected.reshape(tp, tokens // tp, width), "tp", 0, 0, tiled=True)
    layer_out = jnp.sum(tiles.astype(F32), axis=0).astype(BF16)
    return (layer_out[None], row_log_total[None])


def solution(mesh):
    weight = P(("sp", "fs"), "tp")
    return jax.shard_map(
        on_device,
        mesh=mesh,
        in_specs=(
            P("fs", "sp", None),
            P(),
            *(weight for _ in range(9)),
            *(P("tp") for _ in range(5)),
            P("fs", "sp", "tp"),
        ),
        out_specs=(P("fs", ("sp", "tp"), None), P("fs", "tp", "sp")),
        check_vma=False,
    )
```

```python
import functools

import jax
import jax.numpy as jnp
from jax import lax
from jax.experimental import pallas as pl
from jax.experimental.pallas import tpu as pltpu
from jax.sharding import PartitionSpec as P


HEAD = 128
ROWS = 32
TILE = 16
NEAR = 4

epsilon = 1e-06
log_floor = 0.05
F32 = jnp.float32
BF16 = jnp.bfloat16
INTERPRET = False


def vmem_call(kernel, outs, n_in, smem=(), hbm=(), scratch=(), mib=16):
    def space(k):
        return pltpu.SMEM if k in smem else pltpu.HBM if k in hbm else pltpu.VMEM

    return pl.pallas_call(
        kernel,
        out_shape=outs,
        in_specs=[pl.BlockSpec(memory_space=space(k)) for k in range(n_in)],
        out_specs=jax.tree.map(lambda _: pl.BlockSpec(memory_space=pltpu.VMEM), outs),
        scratch_shapes=list(scratch),
        compiler_params=pltpu.CompilerParams(vmem_limit_bytes=mib << 20),
        interpret=INTERPRET,
    )


def dot(a, b, dims=((1,), (0,))):
    return lax.dot_general(a, b, (dims, ((), ())), preferred_element_type=F32)


def parts(a):
    high = a.astype(BF16)
    return high, (a - high.astype(F32)).astype(BF16)


def dot_left(a, b, dims=((1,), (0,))):
    high, low = parts(a)
    return dot(high, b, dims) + dot(low, b, dims)


def dot_both(a, b, dims):
    a_high, a_low = parts(a)
    b_high, b_low = parts(b)
    return dot(a_high, b_high, dims) + (dot(a_high, b_low, dims) + dot(a_low, b_high, dims))


def start_kernel(x_hbm, gain_hbm, *refs):
    weights = refs[:9]
    slices_ref, packed_ref, own_ref, x_ref, gain_ref, arrived = refs[9:]
    copies = [
        pltpu.make_async_copy(x_hbm, x_ref, arrived.at[0]),
        pltpu.make_async_copy(gain_hbm, gain_ref, arrived.at[1]),
    ]
    for k in range(7):
        place = packed_ref.at[k * ROWS : (k + 1) * ROWS]
        copies.append(pltpu.make_async_copy(weights[k], place, arrived.at[2 + k]))
    for k in range(2):
        place = own_ref.at[k * ROWS : (k + 1) * ROWS]
        copies.append(pltpu.make_async_copy(weights[7 + k], place, arrived.at[9 + k]))
    for copy in copies:
        copy.start()
    for copy in copies:
        copy.wait()
    values = x_ref[...].astype(F32)
    square_mean = jnp.mean(values * values, axis=-1, keepdims=True)
    normed = (values * lax.rsqrt(square_mean + epsilon) * gain_ref[...]).astype(BF16)
    count = slices_ref.shape[0]
    wide = count * HEAD
    target = lax.broadcasted_iota(jnp.int32, (wide, wide), 1)
    source = lax.broadcasted_iota(jnp.int32, (wide, wide), 0)
    inside = target % HEAD
    wanted = (inside // ROWS) * (count * ROWS) + (target // HEAD) * ROWS + inside % ROWS
    pick = (source == wanted).astype(BF16)
    for b in range(x_ref.shape[1] // wide):
        moved = dot(normed[:, b * wide : (b + 1) * wide], pick).astype(BF16)
        for k in range(count):
            slices_ref[k, :, b * HEAD : (b + 1) * HEAD] = moved[:, k * HEAD : (k + 1) * HEAD]


def partial_kernel(first, rows_ref, weight_ref, out_ref):
    sp = weight_ref.shape[0]
    pieces = [
        weight_ref[:, k * ROWS : (k + 1) * ROWS].reshape(sp * ROWS, HEAD)
        for k in range(first, first + out_ref.shape[2] // HEAD)
    ]
    weight = jnp.concatenate(pieces, axis=1)
    for k in range(rows_ref.shape[0]):
        out_ref[k] = dot(rows_ref[k], weight).astype(BF16)


def sum_of(products_ref):
    total = products_ref[0].astype(F32)
    for k in range(1, products_ref.shape[0]):
        total = total + products_ref[k].astype(F32)
    return total.astype(BF16)


def attention_inputs_kernel(products_ref, own_ref, far_ref, key_value_ref):
    total = sum_of(products_ref)
    length = total.shape[0]
    key_value_ref[0:length] = total[:, 0:HEAD]
    key_value_ref[length : 2 * length] = total[:, HEAD : 2 * HEAD]
    far_ref[0:length] = total[:, 2 * HEAD :]
    far_ref[length : length + 2 * ROWS] = own_ref[...]


def local_recurrence_kernel(*refs):
    products_ref, floor_ref, offset_ref, extra_hbm, key_value_ref, slots_ref = refs[:6]
    message_ref, inner_ref, query_decayed_ref, gate_ref, extra_ref, arrived = refs[6:]
    copy = pltpu.make_async_copy(extra_hbm, extra_ref, arrived)
    copy.start()
    total = sum_of(products_ref)
    columns = [total[:, k * HEAD : (k + 1) * HEAD] for k in range(4)]
    query_b = columns[0].astype(F32)
    query = query_b / (1.0 + jnp.exp(-query_b))
    value = columns[2]
    gate_b = columns[3].astype(F32)
    gate_ref[...] = gate_b / (1.0 + jnp.exp(-gate_b))
    u = columns[1].astype(F32) + offset_ref[...]
    key = (1.0 - floor_ref[...]) / (1.0 + jnp.exp(u))
    copy.wait()
    log_forget = jnp.log(1.0 - key) + extra_ref[...]
    length = log_forget.shape[0]
    row = lax.broadcasted_iota(jnp.int32, (length, length), 0)
    col = lax.broadcasted_iota(jnp.int32, (length, length), 1)
    lower = (row >= col).astype(BF16)
    high = log_forget.astype(BF16)
    rest = log_forget - high.astype(F32)
    middle = rest.astype(BF16)
    low = (rest - middle.astype(F32)).astype(BF16)
    running = dot(lower, high) + (dot(lower, middle) + dot(lower, low))
    position = lax.broadcasted_iota(jnp.int32, (length, 1), 0)
    pairwise = jnp.where(row == col, dot_both(query, key, ((1,), (1,))), 0.0)
    half = 1
    while half < length:
        block = 2 * half
        if block >= 8:
            boundary = running.reshape(length // block, block, HEAD)[:, half - 1 : half]
            boundary = jnp.broadcast_to(boundary, (length // block, block, HEAD)).reshape(
                length, HEAD
            )
        else:
            tiles = running.reshape(length // 8, 8, HEAD)
            inside = lax.broadcasted_iota(jnp.int32, (1, 8, 1), 1) // block
            boundary = jnp.zeros_like(tiles)
            for k in range(8 // block):
                at = k * block + half - 1
                boundary = jnp.where(inside == k, tiles[:, at : at + 1], boundary)
            boundary = boundary.reshape(length, HEAD)
        second = (position // half) % 2 == 1
        after = jnp.where(second, query * jnp.exp(running - boundary), 0.0)
        before = jnp.where(second, 0.0, key * jnp.exp(boundary - running))
        chosen = (row // block == col // block) & (row // half != col // half) & (row > col)
        pairwise = jnp.where(chosen, dot_both(after, before, ((1,), (1,))), pairwise)
        half = block
    inner_ref[...] = dot_left(pairwise, value)
    final = running[length - 1 : length]
    query_decayed_ref[...] = query * jnp.exp(running)
    key_high, key_low = parts(key * jnp.exp(final - running))
    state = dot(value, key_high, ((0,), (0,))) + dot(value, key_low, ((0,), (0,)))
    at = 0
    vector = jnp.broadcast_to(jnp.exp(final), (TILE, HEAD)).astype(BF16)
    for piece in (key_value_ref[...], state.astype(BF16), vector):
        message_ref[at : at + piece.shape[0]] = piece
        at += piece.shape[0]
    for k in range(slots_ref.shape[0]):
        message_ref[at : at + 2 * ROWS] = slots_ref[k, slots_ref.shape[1] - 2 * ROWS :]
        at += 2 * ROWS


def chain(message_ref, start, count):
    def step(k, carry):
        decay_all, state = carry
        decay = message_ref[k, start + HEAD : start + HEAD + TILE].astype(F32)[0:1]
        return decay * decay_all, decay * state + message_ref[k, start : start + HEAD].astype(F32)

    return lax.fori_loop(
        0, count, step, (jnp.ones((1, HEAD), F32), jnp.zeros((HEAD, HEAD), F32))
    )


def attend(query, message_ref, shift, k, ahead=None):
    length = query.shape[0]
    row = lax.broadcasted_iota(jnp.int32, (length, length), 0)
    col = lax.broadcasted_iota(jnp.int32, (length, length), 1)
    key = message_ref[k, 0:length]
    value = message_ref[k, length : 2 * length]
    scores = dot(query, key, ((1,), (1,))) * HEAD ** (-0.5) + shift
    softplus = jnp.maximum(scores, 0.0) + jnp.log(1.0 + jnp.exp(-jnp.abs(scores)))
    if ahead is not None:
        seen = row + ahead * length > col
        softplus = jnp.where(seen, softplus, 0.0)
    spent = dot_left(softplus, (row >= col).astype(BF16))
    weights = jnp.exp(scores - spent)
    if ahead is not None:
        weights = jnp.where(seen, weights, 0.0)
    return dot(weights.astype(BF16), value), spent[:, 0:1]


def attend_near(query, message_ref, shift, place=None):
    weighted, total = None, None
    for k in reversed(range(message_ref.shape[0])):
        ahead = None if place is None else place - k
        more, spent = attend(query, message_ref, shift, k, ahead)
        weighted = more if weighted is None else weighted + jnp.exp(-total) * more
        total = spent if total is None else total + spent
    return weighted, total


def as_row(total):
    return jnp.transpose(jnp.broadcast_to(total, (total.shape[0], HEAD)))[0:1]


def as_column(row):
    pieces = [
        jnp.transpose(jnp.broadcast_to(row[:, k : k + HEAD], (HEAD, HEAD)))[:, 0:1]
        for k in range(0, row.shape[1], HEAD)
    ]
    return jnp.concatenate(pieces, axis=0)


def far_kernel(places, group_ref, shift_ref, message_ref, query_ref, out_ref):
    count = query_ref.shape[0]
    near = message_ref.shape[0]
    length = out_ref.shape[0] - TILE - HEAD
    wanted = group_ref[0] + places < count

    @pl.when(wanted)
    def _():
        query = query_ref[group_ref[0] + places, 0:length]
        weighted, total = attend_near(query, message_ref, shift_ref[0])
        out_ref[0:length] = weighted.astype(BF16)
        decay, state = chain(message_ref, 2 * length, near)
        high, low = parts(as_row(total))
        pieces = [piece[:, k * HEAD : (k + 1) * HEAD] for piece in (high, low) for k in range(2)]
        index = lax.broadcasted_iota(jnp.int32, (TILE, HEAD), 0)
        vector = jnp.zeros((TILE, HEAD), F32)
        for k, piece in enumerate(pieces + [decay]):
            vector = jnp.where(index == k, piece.astype(F32), vector)
        out_ref[length : length + TILE] = vector.astype(BF16)
        out_ref[length + TILE : length + TILE + HEAD] = state.astype(BF16)

    @pl.when(jnp.logical_not(wanted))
    def _():
        out_ref[...] = jnp.zeros(out_ref.shape, BF16)


def near_kernel(place_ref, shift_ref, query_ref, message_ref, weighted_ref, total_ref):
    place = place_ref[0]
    length = weighted_ref.shape[0]
    weighted, total = attend_near(query_ref[0:length], message_ref, shift_ref[0], place)
    weighted_ref[...] = weighted
    total_ref[...] = jnp.broadcast_to(total, total_ref.shape)


def final_kernel(
    place_ref,
    message_ref,
    weighted_ref,
    spent_ref,
    inner_ref,
    query_decayed_ref,
    gate_ref,
    gain_a_ref,
    gain_b_ref,
    weight_ref,
    *refs,
):
    far_refs, out_ref, total_ref = refs[:-2], refs[-2], refs[-1]
    length = weighted_ref.shape[0]
    incoming = jnp.zeros((HEAD, HEAD), F32)
    outside = jnp.zeros((length, HEAD), F32)
    outside_row = jnp.zeros((1, length), F32)
    for ref in reversed(far_refs):
        vector = ref[length : length + TILE].astype(F32)
        row = jnp.concatenate(
            [vector[k : k + 1] + vector[k + 2 : k + 3] for k in range(2)], axis=1
        )
        incoming = vector[4:5] * incoming + ref[
            length + TILE : length + TILE + HEAD
        ].astype(F32)
        outside = ref[0:length].astype(F32) + jnp.exp(-as_column(row)) * outside
        outside_row = outside_row + row
    decay, state = chain(message_ref, 2 * length, place_ref[0])
    state = state + decay * incoming
    recurrent = inner_ref[...] + dot_both(query_decayed_ref[...], state, ((1,), (1,)))
    square_mean = jnp.mean(recurrent * recurrent, axis=-1, keepdims=True)
    mixed_b = (
        recurrent * lax.rsqrt(square_mean + epsilon) * gain_b_ref[...] * gate_ref[...]
    ).astype(BF16)
    total = spent_ref[...]
    weighted = weighted_ref[...] + jnp.exp(-total) * outside
    total_row = jnp.transpose(total)[0:1] + outside_row
    total_ref[...] = jnp.log(jnp.maximum(1.0 - jnp.exp(-total_row), log_floor))
    square_mean = jnp.mean(weighted * weighted, axis=-1, keepdims=True)
    mixed_a = (weighted * lax.rsqrt(square_mean + epsilon) * gain_a_ref[...]).astype(BF16)
    mixed = jnp.concatenate([mixed_a, mixed_b], axis=1)
    fs, near, groups = weight_ref.shape[:3]
    width = fs * ROWS
    for group in range(groups):
        for s in range(near):
            both = jnp.concatenate(
                [weight_ref[:, s, group, k].reshape(width, HEAD) for k in range(2)], axis=1
            )
            at = (group * near + s) * width
            out_ref[:, at : at + width] = dot(mixed, both, ((1,), (1,))).astype(BF16)


def copies(array, size):
    return jnp.broadcast_to(array[None], (size, *array.shape))


def on_device(
    input_layer_rows,
    input_norm_gain,
    query_weight_attention,
    key_weight_attention,
    value_weight_attention,
    query_weight_recurrent,
    forget_weight_recurrent,
    value_weight_recurrent,
    gate_weight_recurrent,
    output_weight_attention,
    emitted_projection_linear_scan,
    score_offset,
    attention_norm_gain,
    recurrence_norm_gain,
    forget_floor,
    forget_offset,
    extra_log_decay,
):
    x = input_layer_rows[0]
    tokens, width = x.shape
    sp, fs, tp = (lax.axis_size(name) for name in ("sp", "fs", "tp"))
    count = sp // NEAR
    rank = lax.axis_index("sp").astype(jnp.int32)
    group = (rank // NEAR).reshape(1)
    shape = jax.ShapeDtypeStruct

    slices, packed, out_own = vmem_call(
        start_kernel,
        (
            shape((fs, tokens, width // fs), BF16),
            shape((7 * ROWS, HEAD), BF16),
            shape((2 * ROWS, HEAD), BF16),
        ),
        11,
        hbm=range(11),
        scratch=(
            pltpu.VMEM((tokens, width), BF16),
            pltpu.VMEM((1, width), F32),
            pltpu.SemaphoreType.DMA((11,)),
        ),
        mib=58,
    )(
        x,
        input_norm_gain.reshape(1, width),
        key_weight_attention,
        value_weight_attention,
        query_weight_attention,
        query_weight_recurrent,
        forget_weight_recurrent,
        value_weight_recurrent,
        gate_weight_recurrent,
        output_weight_attention,
        emitted_projection_linear_scan,
    )
    rows = lax.all_to_all(slices, "fs", 0, 0, tiled=True)
    column = lax.all_gather(packed, "sp")
    first = vmem_call(
        functools.partial(partial_kernel, 0), shape((fs, tokens, 3 * HEAD), BF16), 2
    )(rows, column)
    second = vmem_call(
        functools.partial(partial_kernel, 3), shape((fs, tokens, 4 * HEAD), BF16), 2
    )(rows, column)
    first = lax.all_to_all(first, "fs", 0, 0, tiled=True)
    own, key_value = vmem_call(
        attention_inputs_kernel,
        (shape((tokens + 2 * ROWS, HEAD), BF16), shape((2 * tokens, HEAD), BF16)),
        2,
    )(first, out_own)
    second, _ = lax.optimization_barrier((second, own))
    second = lax.all_to_all(second, "fs", 0, 0, tiled=True)
    strided = [list(range(k, sp, NEAR)) for k in range(NEAR)]
    across = lax.all_gather(own, "sp", axis_index_groups=strided)

    small = shape((tokens, HEAD), F32)
    start = 2 * tokens + HEAD + TILE
    message, inner, query_decayed, gate = vmem_call(
        local_recurrence_kernel,
        (shape((start + count * 2 * ROWS, HEAD), BF16), small, small, small),
        6,
        (),
        (3,),
        (pltpu.VMEM((tokens, HEAD), F32), pltpu.SemaphoreType.DMA(())),
    )(
        second,
        forget_floor.reshape(1, HEAD),
        forget_offset.reshape(1, HEAD),
        extra_log_decay[0],
        key_value,
        across,
    )
    groups = [list(range(NEAR * k, NEAR * (k + 1))) for k in range(count)]
    gathered = lax.all_gather(message, "sp", axis_index_groups=groups)
    out_weights = lax.all_to_all(
        copies(gathered[:, start:].reshape(NEAR, count, 2, ROWS, HEAD), fs),
        "fs",
        0,
        0,
        tiled=True,
    )
    outside = []
    for j in range(1, count):
        far = vmem_call(
            functools.partial(far_kernel, j),
            shape((tokens + TILE + HEAD, HEAD), BF16),
            4,
            (0, 1),
        )(group, score_offset, gathered, across)
        places = [(k, k + NEAR * j) for k in range(sp - NEAR * j)]
        outside.append(lax.ppermute(far, "sp", places))
    place = (rank % NEAR).reshape(1)
    weighted, spent = vmem_call(near_kernel, (small, small), 4, (0, 1))(
        place, score_offset, own, gathered
    )
    projected, row_log_total = vmem_call(
        final_kernel,
        (shape((tokens, width), BF16), shape((1, tokens), F32)),
        9 + count,
        (0,),
    )(
        place,
        gathered,
        weighted,
        spent,
        inner,
        query_decayed,
        gate,
        attention_norm_gain.reshape(1, HEAD),
        recurrence_norm_gain.reshape(1, HEAD),
        out_weights,
        *outside,
    )
    tiles = lax.all_to_all(projected.reshape(tp, tokens // tp, width), "tp", 0, 0, tiled=True)
    layer_out = jnp.sum(tiles.astype(F32), axis=0).astype(BF16)
    return (layer_out[None], row_log_total[None])


def solution(mesh):
    weight = P(("sp", "fs"), "tp")
    return jax.shard_map(
        on_device,
        mesh=mesh,
        in_specs=(
            P("fs", "sp", None),
            P(),
            *(weight for _ in range(9)),
            *(P("tp") for _ in range(5)),
            P("fs", "sp", "tp"),
        ),
        out_specs=(P("fs", ("sp", "tp"), None), P("fs", "tp", "sp")),
        check_vma=False,
    )
```

```python
import functools

import jax
import jax.numpy as jnp
from jax import lax
from jax.experimental import pallas as pl
from jax.experimental.pallas import tpu as pltpu
from jax.sharding import PartitionSpec as P


HEAD = 128
ROWS = 32
TILE = 16
NEAR = 4

epsilon = 1e-06
log_floor = 0.05
F32 = jnp.float32
BF16 = jnp.bfloat16
INTERPRET = False


def vmem_call(kernel, outs, n_in, smem=(), hbm=(), scratch=(), mib=16):
    def space(k):
        return pltpu.SMEM if k in smem else pltpu.HBM if k in hbm else pltpu.VMEM

    return pl.pallas_call(
        kernel,
        out_shape=outs,
        in_specs=[pl.BlockSpec(memory_space=space(k)) for k in range(n_in)],
        out_specs=jax.tree.map(lambda _: pl.BlockSpec(memory_space=pltpu.VMEM), outs),
        scratch_shapes=list(scratch),
        compiler_params=pltpu.CompilerParams(vmem_limit_bytes=mib << 20),
        interpret=INTERPRET,
    )


def dot(a, b, dims=((1,), (0,))):
    return lax.dot_general(a, b, (dims, ((), ())), preferred_element_type=F32)


def parts(a):
    high = a.astype(BF16)
    return high, (a - high.astype(F32)).astype(BF16)


def dot_left(a, b, dims=((1,), (0,))):
    high, low = parts(a)
    return dot(high, b, dims) + dot(low, b, dims)


def dot_both(a, b, dims):
    a_high, a_low = parts(a)
    b_high, b_low = parts(b)
    return dot(a_high, b_high, dims) + (dot(a_high, b_low, dims) + dot(a_low, b_high, dims))


def start_kernel(x_hbm, gain_hbm, *refs):
    weights = refs[:9]
    slices_ref, packed_ref, own_ref, x_ref, gain_ref, arrived = refs[9:]
    copies = [
        pltpu.make_async_copy(x_hbm, x_ref, arrived.at[0]),
        pltpu.make_async_copy(gain_hbm, gain_ref, arrived.at[1]),
    ]
    for k in range(7):
        place = packed_ref.at[k * ROWS : (k + 1) * ROWS]
        copies.append(pltpu.make_async_copy(weights[k], place, arrived.at[2 + k]))
    for k in range(2):
        place = own_ref.at[k * ROWS : (k + 1) * ROWS]
        copies.append(pltpu.make_async_copy(weights[7 + k], place, arrived.at[9 + k]))
    for copy in copies:
        copy.start()
    for copy in copies:
        copy.wait()
    values = x_ref[...].astype(F32)
    square_mean = jnp.mean(values * values, axis=-1, keepdims=True)
    normed = (values * lax.rsqrt(square_mean + epsilon) * gain_ref[...]).astype(BF16)
    count = slices_ref.shape[0]
    wide = count * HEAD
    target = lax.broadcasted_iota(jnp.int32, (wide, wide), 1)
    source = lax.broadcasted_iota(jnp.int32, (wide, wide), 0)
    inside = target % HEAD
    wanted = (inside // ROWS) * (count * ROWS) + (target // HEAD) * ROWS + inside % ROWS
    pick = (source == wanted).astype(BF16)
    for b in range(x_ref.shape[1] // wide):
        moved = dot(normed[:, b * wide : (b + 1) * wide], pick).astype(BF16)
        for k in range(count):
            slices_ref[k, :, b * HEAD : (b + 1) * HEAD] = moved[:, k * HEAD : (k + 1) * HEAD]


def partial_kernel(first, rows_ref, weight_ref, *refs):
    vectors = refs[: (len(refs) - 1) // 2]
    out_ref = refs[len(vectors)]
    for k, ref in enumerate(refs[len(vectors) + 1 :]):
        ref[...] = vectors[k][...]
    sp = weight_ref.shape[0]
    pieces = [
        weight_ref[:, k * ROWS : (k + 1) * ROWS].reshape(sp * ROWS, HEAD)
        for k in range(first, first + out_ref.shape[2] // HEAD)
    ]
    weight = jnp.concatenate(pieces, axis=1)
    for k in range(rows_ref.shape[0]):
        out_ref[k] = dot(rows_ref[k], weight).astype(BF16)


def sum_of(products_ref):
    total = products_ref[0].astype(F32)
    for k in range(1, products_ref.shape[0]):
        total = total + products_ref[k].astype(F32)
    return total.astype(BF16)


def attention_inputs_kernel(products_ref, own_ref, far_ref):
    length = products_ref.shape[1]
    far_ref[0:length] = sum_of(products_ref)
    far_ref[length : length + 2 * ROWS] = own_ref[...]


def local_recurrence_kernel(*refs):
    products_ref, floor_ref, offset_ref, extra_hbm, slots_ref = refs[:5]
    message_ref, inner_ref, query_decayed_ref, gate_ref, extra_ref, arrived = refs[5:]
    copy = pltpu.make_async_copy(extra_hbm, extra_ref, arrived)
    copy.start()
    total = sum_of(products_ref)
    columns = [total[:, k * HEAD : (k + 1) * HEAD] for k in range(6)]
    query_b = columns[2].astype(F32)
    query = query_b / (1.0 + jnp.exp(-query_b))
    value = columns[4]
    gate_b = columns[5].astype(F32)
    gate_ref[...] = gate_b / (1.0 + jnp.exp(-gate_b))
    u = columns[3].astype(F32) + offset_ref[...]
    key = (1.0 - floor_ref[...]) / (1.0 + jnp.exp(u))
    copy.wait()
    log_forget = jnp.log(1.0 - key) + extra_ref[...]
    length = log_forget.shape[0]
    row = lax.broadcasted_iota(jnp.int32, (length, length), 0)
    col = lax.broadcasted_iota(jnp.int32, (length, length), 1)
    lower = (row >= col).astype(BF16)
    high = log_forget.astype(BF16)
    rest = log_forget - high.astype(F32)
    middle = rest.astype(BF16)
    low = (rest - middle.astype(F32)).astype(BF16)
    running = dot(lower, high) + (dot(lower, middle) + dot(lower, low))
    position = lax.broadcasted_iota(jnp.int32, (length, 1), 0)
    pairwise = jnp.where(row == col, dot_both(query, key, ((1,), (1,))), 0.0)
    half = 1
    while half < length:
        block = 2 * half
        if block >= 8:
            boundary = running.reshape(length // block, block, HEAD)[:, half - 1 : half]
            boundary = jnp.broadcast_to(boundary, (length // block, block, HEAD)).reshape(
                length, HEAD
            )
        else:
            tiles = running.reshape(length // 8, 8, HEAD)
            inside = lax.broadcasted_iota(jnp.int32, (1, 8, 1), 1) // block
            boundary = jnp.zeros_like(tiles)
            for k in range(8 // block):
                at = k * block + half - 1
                boundary = jnp.where(inside == k, tiles[:, at : at + 1], boundary)
            boundary = boundary.reshape(length, HEAD)
        second = (position // half) % 2 == 1
        after = jnp.where(second, query * jnp.exp(running - boundary), 0.0)
        before = jnp.where(second, 0.0, key * jnp.exp(boundary - running))
        chosen = (row // block == col // block) & (row // half != col // half) & (row > col)
        pairwise = jnp.where(chosen, dot_both(after, before, ((1,), (1,))), pairwise)
        half = block
    inner_ref[...] = dot_left(pairwise, value)
    final = running[length - 1 : length]
    query_decayed_ref[...] = query * jnp.exp(running)
    key_high, key_low = parts(key * jnp.exp(final - running))
    state = dot(value, key_high, ((0,), (0,))) + dot(value, key_low, ((0,), (0,)))
    at = 0
    vector = jnp.broadcast_to(jnp.exp(final), (TILE, HEAD)).astype(BF16)
    for piece in (columns[0], columns[1], state.astype(BF16), vector):
        message_ref[at : at + piece.shape[0]] = piece
        at += piece.shape[0]
    for k in range(slots_ref.shape[0]):
        message_ref[at : at + 2 * ROWS] = slots_ref[k, slots_ref.shape[1] - 2 * ROWS :]
        at += 2 * ROWS


def chain(message_ref, start, count):
    def step(k, carry):
        decay_all, state = carry
        decay = message_ref[k, start + HEAD : start + HEAD + TILE].astype(F32)[0:1]
        return decay * decay_all, decay * state + message_ref[k, start : start + HEAD].astype(F32)

    return lax.fori_loop(
        0, count, step, (jnp.ones((1, HEAD), F32), jnp.zeros((HEAD, HEAD), F32))
    )


def attend(query, message_ref, shift, k, ahead=None):
    length = query.shape[0]
    row = lax.broadcasted_iota(jnp.int32, (length, length), 0)
    col = lax.broadcasted_iota(jnp.int32, (length, length), 1)
    key = message_ref[k, 0:length]
    value = message_ref[k, length : 2 * length]
    scores = dot(query, key, ((1,), (1,))) * HEAD ** (-0.5) + shift
    softplus = jnp.maximum(scores, 0.0) + jnp.log(1.0 + jnp.exp(-jnp.abs(scores)))
    if ahead is not None:
        seen = row + ahead * length > col
        softplus = jnp.where(seen, softplus, 0.0)
    spent = dot_left(softplus, (row >= col).astype(BF16))
    weights = jnp.exp(scores - spent)
    if ahead is not None:
        weights = jnp.where(seen, weights, 0.0)
    return dot(weights.astype(BF16), value), spent[:, 0:1]


def attend_near(query, message_ref, shift, place=None):
    weighted, total = None, None
    for k in reversed(range(message_ref.shape[0])):
        ahead = None if place is None else place - k
        more, spent = attend(query, message_ref, shift, k, ahead)
        weighted = more if weighted is None else weighted + jnp.exp(-total) * more
        total = spent if total is None else total + spent
    return weighted, total


def as_row(total):
    return jnp.transpose(jnp.broadcast_to(total, (total.shape[0], HEAD)))[0:1]


def as_column(row):
    pieces = [
        jnp.transpose(jnp.broadcast_to(row[:, k : k + HEAD], (HEAD, HEAD)))[:, 0:1]
        for k in range(0, row.shape[1], HEAD)
    ]
    return jnp.concatenate(pieces, axis=0)


def far_kernel(group_ref, shift_ref, message_ref, query_ref, *out_refs):
    count = query_ref.shape[0]
    length = message_ref.shape[1] - count * 2 * ROWS - HEAD - TILE
    length = length // 2
    shift = shift_ref[0]
    near = message_ref.shape[0]
    index = lax.broadcasted_iota(jnp.int32, (TILE, HEAD), 0)
    for j, out_ref in enumerate(out_refs):
        wanted = group_ref[0] + j + 1 < count

        @pl.when(wanted)
        def _(j=j, out_ref=out_ref):
            query = query_ref[group_ref[0] + j + 1, 0:length]
            weighted, total = attend_near(query, message_ref, shift)
            out_ref[0:length] = weighted.astype(BF16)
            decay, state = chain(message_ref, 2 * length, near)
            high, low = parts(as_row(total))
            pieces = [
                piece[:, k * HEAD : (k + 1) * HEAD] for piece in (high, low) for k in range(2)
            ]
            vector = jnp.zeros((TILE, HEAD), F32)
            for k, piece in enumerate(pieces + [decay]):
                vector = jnp.where(index == k, piece.astype(F32), vector)
            out_ref[length : length + TILE] = vector.astype(BF16)
            out_ref[length + TILE : length + TILE + HEAD] = state.astype(BF16)

        @pl.when(jnp.logical_not(wanted))
        def _(out_ref=out_ref):
            out_ref[...] = jnp.zeros(out_ref.shape, BF16)


def near_kernel(place_ref, shift_ref, query_ref, message_ref, weighted_ref, total_ref):
    place = place_ref[0]
    length = weighted_ref.shape[0]
    weighted, total = attend_near(query_ref[0:length], message_ref, shift_ref[0], place)
    weighted_ref[...] = weighted
    total_ref[...] = jnp.broadcast_to(total, total_ref.shape)


def final_kernel(
    place_ref,
    message_ref,
    weighted_ref,
    spent_ref,
    inner_ref,
    query_decayed_ref,
    gate_ref,
    gain_a_ref,
    gain_b_ref,
    weight_ref,
    *refs,
):
    far_refs, out_ref, total_ref = refs[:-2], refs[-2], refs[-1]
    length = weighted_ref.shape[0]
    incoming = jnp.zeros((HEAD, HEAD), F32)
    outside = jnp.zeros((length, HEAD), F32)
    outside_row = jnp.zeros((1, length), F32)
    for ref in reversed(far_refs):
        vector = ref[length : length + TILE].astype(F32)
        row = jnp.concatenate(
            [vector[k : k + 1] + vector[k + 2 : k + 3] for k in range(2)], axis=1
        )
        incoming = vector[4:5] * incoming + ref[
            length + TILE : length + TILE + HEAD
        ].astype(F32)
        outside = ref[0:length].astype(F32) + jnp.exp(-as_column(row)) * outside
        outside_row = outside_row + row
    decay, state = chain(message_ref, 2 * length, place_ref[0])
    state = state + decay * incoming
    recurrent = inner_ref[...] + dot_both(query_decayed_ref[...], state, ((1,), (1,)))
    square_mean = jnp.mean(recurrent * recurrent, axis=-1, keepdims=True)
    mixed_b = (
        recurrent * lax.rsqrt(square_mean + epsilon) * gain_b_ref[...] * gate_ref[...]
    ).astype(BF16)
    total = spent_ref[...]
    weighted = weighted_ref[...] + jnp.exp(-total) * outside
    total_row = jnp.transpose(total)[0:1] + outside_row
    total_ref[...] = jnp.log(jnp.maximum(1.0 - jnp.exp(-total_row), log_floor))
    square_mean = jnp.mean(weighted * weighted, axis=-1, keepdims=True)
    mixed_a = (weighted * lax.rsqrt(square_mean + epsilon) * gain_a_ref[...]).astype(BF16)
    mixed = jnp.concatenate([mixed_a, mixed_b], axis=1)
    fs, near, groups = weight_ref.shape[:3]
    width = fs * ROWS
    for group in range(groups):
        for s in range(near):
            both = jnp.concatenate(
                [weight_ref[:, s, group, k].reshape(width, HEAD) for k in range(2)], axis=1
            )
            at = (group * near + s) * width
            out_ref[:, at : at + width] = dot(mixed, both, ((1,), (1,))).astype(BF16)


def copies(array, size):
    return jnp.broadcast_to(array[None], (size, *array.shape))


def on_device(
    input_layer_rows,
    input_norm_gain,
    query_weight_attention,
    key_weight_attention,
    value_weight_attention,
    query_weight_recurrent,
    forget_weight_recurrent,
    value_weight_recurrent,
    gate_weight_recurrent,
    output_weight_attention,
    emitted_projection_linear_scan,
    score_offset,
    attention_norm_gain,
    recurrence_norm_gain,
    forget_floor,
    forget_offset,
    extra_log_decay,
):
    x = input_layer_rows[0]
    tokens, width = x.shape
    sp, fs, tp = (lax.axis_size(name) for name in ("sp", "fs", "tp"))
    count = sp // NEAR
    rank = lax.axis_index("sp").astype(jnp.int32)
    group = (rank // NEAR).reshape(1)
    shape = jax.ShapeDtypeStruct

    slices, packed, out_own = vmem_call(
        start_kernel,
        (
            shape((fs, tokens, width // fs), BF16),
            shape((7 * ROWS, HEAD), BF16),
            shape((2 * ROWS, HEAD), BF16),
        ),
        11,
        hbm=range(11),
        scratch=(
            pltpu.VMEM((tokens, width), BF16),
            pltpu.VMEM((1, width), F32),
            pltpu.SemaphoreType.DMA((11,)),
        ),
        mib=58,
    )(
        x,
        input_norm_gain.reshape(1, width),
        query_weight_attention,
        key_weight_attention,
        value_weight_attention,
        query_weight_recurrent,
        forget_weight_recurrent,
        value_weight_recurrent,
        gate_weight_recurrent,
        output_weight_attention,
        emitted_projection_linear_scan,
    )
    rows = lax.all_to_all(slices, "fs", 0, 0, tiled=True)
    column = lax.all_gather(packed, "sp")
    first = vmem_call(
        functools.partial(partial_kernel, 0), shape((fs, tokens, HEAD), BF16), 2
    )(rows, column)
    vector = shape((1, HEAD), F32)
    second, floor, offset, gain_a, gain_b = vmem_call(
        functools.partial(partial_kernel, 1),
        (shape((fs, tokens, 6 * HEAD), BF16), vector, vector, vector, vector),
        6,
    )(
        rows,
        column,
        forget_floor.reshape(1, HEAD),
        forget_offset.reshape(1, HEAD),
        attention_norm_gain.reshape(1, HEAD),
        recurrence_norm_gain.reshape(1, HEAD),
    )
    first = lax.all_to_all(first, "fs", 0, 0, tiled=True)
    own = vmem_call(attention_inputs_kernel, shape((tokens + 2 * ROWS, HEAD), BF16), 2)(
        first, out_own
    )
    second, _ = lax.optimization_barrier((second, own))
    second = lax.all_to_all(second, "fs", 0, 0, tiled=True)
    strided = [list(range(k, sp, NEAR)) for k in range(NEAR)]
    across = lax.all_gather(own, "sp", axis_index_groups=strided)

    small = shape((tokens, HEAD), F32)
    start = 2 * tokens + HEAD + TILE
    message, inner, query_decayed, gate = vmem_call(
        local_recurrence_kernel,
        (shape((start + count * 2 * ROWS, HEAD), BF16), small, small, small),
        5,
        (),
        (3,),
        (pltpu.VMEM((tokens, HEAD), F32), pltpu.SemaphoreType.DMA(())),
    )(
        second,
        floor,
        offset,
        extra_log_decay[0],
        across,
    )
    groups = [list(range(NEAR * k, NEAR * (k + 1))) for k in range(count)]
    gathered = lax.all_gather(message, "sp", axis_index_groups=groups)
    out_weights = lax.all_to_all(
        copies(gathered[:, start:].reshape(NEAR, count, 2, ROWS, HEAD), fs),
        "fs",
        0,
        0,
        tiled=True,
    )
    far = vmem_call(
        far_kernel,
        tuple(shape((tokens + TILE + HEAD, HEAD), BF16) for _ in range(count - 1)),
        4,
        (0, 1),
    )(group, score_offset, gathered, across)
    outside = []
    for j in range(1, count):
        places = [(k, k + NEAR * j) for k in range(sp - NEAR * j)]
        outside.append(lax.ppermute(far[j - 1], "sp", places))
    place = (rank % NEAR).reshape(1)
    weighted, spent = vmem_call(near_kernel, (small, small), 4, (0, 1))(
        place, score_offset, own, gathered
    )
    projected, row_log_total = vmem_call(
        final_kernel,
        (shape((tokens, width), BF16), shape((1, tokens), F32)),
        9 + count,
        (0,),
    )(
        place,
        gathered,
        weighted,
        spent,
        inner,
        query_decayed,
        gate,
        gain_a,
        gain_b,
        out_weights,
        *outside,
    )
    tiles = lax.all_to_all(projected.reshape(tp, tokens // tp, width), "tp", 0, 0, tiled=True)
    layer_out = jnp.sum(tiles.astype(F32), axis=0).astype(BF16)
    return (layer_out[None], row_log_total[None])


def solution(mesh):
    weight = P(("sp", "fs"), "tp")
    return jax.shard_map(
        on_device,
        mesh=mesh,
        in_specs=(
            P("fs", "sp", None),
            P(),
            *(weight for _ in range(9)),
            *(P("tp") for _ in range(5)),
            P("fs", "sp", "tp"),
        ),
        out_specs=(P("fs", ("sp", "tp"), None), P("fs", "tp", "sp")),
        check_vma=False,
    )
```

```python
import functools

import jax
import jax.numpy as jnp
from jax import lax
from jax.experimental import pallas as pl
from jax.experimental.pallas import tpu as pltpu
from jax.sharding import PartitionSpec as P


HEAD = 128
ROWS = 32
TILE = 16
NEAR = 4

epsilon = 1e-06
log_floor = 0.05
F32 = jnp.float32
BF16 = jnp.bfloat16
INTERPRET = False


def vmem_call(kernel, outs, n_in, smem=(), hbm=(), scratch=(), mib=16):
    def space(k):
        return pltpu.SMEM if k in smem else pltpu.HBM if k in hbm else pltpu.VMEM

    return pl.pallas_call(
        kernel,
        out_shape=outs,
        in_specs=[pl.BlockSpec(memory_space=space(k)) for k in range(n_in)],
        out_specs=jax.tree.map(
            lambda out: pl.BlockSpec(
                memory_space=pltpu.SMEM if out.dtype == jnp.int32 else pltpu.VMEM
            ),
            outs,
        ),
        scratch_shapes=list(scratch),
        compiler_params=pltpu.CompilerParams(vmem_limit_bytes=mib << 20),
        interpret=INTERPRET,
    )


def dot(a, b, dims=((1,), (0,))):
    return lax.dot_general(a, b, (dims, ((), ())), preferred_element_type=F32)


def parts(a):
    high = a.astype(BF16)
    return high, (a - high.astype(F32)).astype(BF16)


def dot_left(a, b, dims=((1,), (0,))):
    high, low = parts(a)
    return dot(high, b, dims) + dot(low, b, dims)


def dot_both(a, b, dims):
    a_high, a_low = parts(a)
    b_high, b_low = parts(b)
    return dot(a_high, b_high, dims) + (dot(a_high, b_low, dims) + dot(a_low, b_high, dims))


def start_kernel(x_hbm, gain_hbm, *refs):
    weights = refs[:9]
    slices_ref, packed_ref, own_ref, x_ref, gain_ref, arrived = refs[9:]
    copies = [
        pltpu.make_async_copy(x_hbm, x_ref, arrived.at[0]),
        pltpu.make_async_copy(gain_hbm, gain_ref, arrived.at[1]),
    ]
    for k in range(7):
        place = packed_ref.at[k * ROWS : (k + 1) * ROWS]
        copies.append(pltpu.make_async_copy(weights[k], place, arrived.at[2 + k]))
    for k in range(2):
        place = own_ref.at[k * ROWS : (k + 1) * ROWS]
        copies.append(pltpu.make_async_copy(weights[7 + k], place, arrived.at[9 + k]))
    for copy in copies:
        copy.start()
    for copy in copies:
        copy.wait()
    values = x_ref[...].astype(F32)
    square_mean = jnp.mean(values * values, axis=-1, keepdims=True)
    normed = (values * lax.rsqrt(square_mean + epsilon) * gain_ref[...]).astype(BF16)
    count = slices_ref.shape[0]
    wide = count * HEAD
    target = lax.broadcasted_iota(jnp.int32, (wide, wide), 1)
    source = lax.broadcasted_iota(jnp.int32, (wide, wide), 0)
    inside = target % HEAD
    wanted = (inside // ROWS) * (count * ROWS) + (target // HEAD) * ROWS + inside % ROWS
    pick = (source == wanted).astype(BF16)
    for b in range(x_ref.shape[1] // wide):
        moved = dot(normed[:, b * wide : (b + 1) * wide], pick).astype(BF16)
        for k in range(count):
            slices_ref[k, :, b * HEAD : (b + 1) * HEAD] = moved[:, k * HEAD : (k + 1) * HEAD]


def partial_kernel(first, rows_ref, weight_ref, *refs):
    vectors = refs[: (len(refs) - 1) // 2]
    out_ref = refs[len(vectors)]
    for k, ref in enumerate(refs[len(vectors) + 1 :]):
        if ref.dtype == jnp.int32:
            for n in range(ref.shape[0]):
                ref[n] = vectors[k][n]
        else:
            ref[...] = vectors[k][...]
    sp = weight_ref.shape[0]
    pieces = [
        weight_ref[:, k * ROWS : (k + 1) * ROWS].reshape(sp * ROWS, HEAD)
        for k in range(first, first + out_ref.shape[2] // HEAD)
    ]
    weight = jnp.concatenate(pieces, axis=1)
    for k in range(rows_ref.shape[0]):
        out_ref[k] = dot(rows_ref[k], weight).astype(BF16)


def sum_of(products_ref):
    total = products_ref[0].astype(F32)
    for k in range(1, products_ref.shape[0]):
        total = total + products_ref[k].astype(F32)
    return total.astype(BF16)


def attention_inputs_kernel(products_ref, own_ref, far_ref):
    length = products_ref.shape[1]
    far_ref[0:length] = sum_of(products_ref)
    far_ref[length : length + 2 * ROWS] = own_ref[...]


def local_recurrence_kernel(*refs):
    products_ref, floor_ref, offset_ref, extra_hbm, slots_ref = refs[:5]
    message_ref, inner_ref, query_decayed_ref, gate_ref, extra_ref, arrived = refs[5:]
    copy = pltpu.make_async_copy(extra_hbm, extra_ref, arrived)
    copy.start()
    total = sum_of(products_ref)
    columns = [total[:, k * HEAD : (k + 1) * HEAD] for k in range(6)]
    query_b = columns[2].astype(F32)
    query = query_b / (1.0 + jnp.exp(-query_b))
    value = columns[4]
    gate_b = columns[5].astype(F32)
    gate_ref[...] = gate_b / (1.0 + jnp.exp(-gate_b))
    u = columns[3].astype(F32) + offset_ref[...]
    key = (1.0 - floor_ref[...]) / (1.0 + jnp.exp(u))
    copy.wait()
    log_forget = jnp.log(1.0 - key) + extra_ref[...]
    length = log_forget.shape[0]
    row = lax.broadcasted_iota(jnp.int32, (length, length), 0)
    col = lax.broadcasted_iota(jnp.int32, (length, length), 1)
    lower = (row >= col).astype(BF16)
    high = log_forget.astype(BF16)
    rest = log_forget - high.astype(F32)
    middle = rest.astype(BF16)
    low = (rest - middle.astype(F32)).astype(BF16)
    running = dot(lower, high) + (dot(lower, middle) + dot(lower, low))
    position = lax.broadcasted_iota(jnp.int32, (length, 1), 0)
    pairwise = jnp.where(row == col, dot_both(query, key, ((1,), (1,))), 0.0)
    half = 1
    while half < length:
        block = 2 * half
        if block >= 8:
            boundary = running.reshape(length // block, block, HEAD)[:, half - 1 : half]
            boundary = jnp.broadcast_to(boundary, (length // block, block, HEAD)).reshape(
                length, HEAD
            )
        else:
            tiles = running.reshape(length // 8, 8, HEAD)
            inside = lax.broadcasted_iota(jnp.int32, (1, 8, 1), 1) // block
            boundary = jnp.zeros_like(tiles)
            for k in range(8 // block):
                at = k * block + half - 1
                boundary = jnp.where(inside == k, tiles[:, at : at + 1], boundary)
            boundary = boundary.reshape(length, HEAD)
        second = (position // half) % 2 == 1
        after = jnp.where(second, query * jnp.exp(running - boundary), 0.0)
        before = jnp.where(second, 0.0, key * jnp.exp(boundary - running))
        chosen = (row // block == col // block) & (row // half != col // half) & (row > col)
        pairwise = jnp.where(chosen, dot_both(after, before, ((1,), (1,))), pairwise)
        half = block
    inner_ref[...] = dot_left(pairwise, value)
    final = running[length - 1 : length]
    query_decayed_ref[...] = query * jnp.exp(running)
    key_high, key_low = parts(key * jnp.exp(final - running))
    state = dot(value, key_high, ((0,), (0,))) + dot(value, key_low, ((0,), (0,)))
    at = 0
    vector = jnp.broadcast_to(jnp.exp(final), (TILE, HEAD)).astype(BF16)
    for piece in (columns[0], columns[1], state.astype(BF16), vector):
        message_ref[at : at + piece.shape[0]] = piece
        at += piece.shape[0]
    for k in range(slots_ref.shape[0]):
        message_ref[at : at + 2 * ROWS] = slots_ref[k, slots_ref.shape[1] - 2 * ROWS :]
        at += 2 * ROWS


def chain(message_ref, start, count):
    def step(k, carry):
        decay_all, state = carry
        decay = message_ref[k, start + HEAD : start + HEAD + TILE].astype(F32)[0:1]
        return decay * decay_all, decay * state + message_ref[k, start : start + HEAD].astype(F32)

    return lax.fori_loop(
        0, count, step, (jnp.ones((1, HEAD), F32), jnp.zeros((HEAD, HEAD), F32))
    )


def attend(query, message_ref, shift, k, ahead=None):
    length = query.shape[0]
    row = lax.broadcasted_iota(jnp.int32, (length, length), 0)
    col = lax.broadcasted_iota(jnp.int32, (length, length), 1)
    key = message_ref[k, 0:length]
    value = message_ref[k, length : 2 * length]
    scores = dot(query, key, ((1,), (1,))) * HEAD ** (-0.5) + shift
    softplus = jnp.maximum(scores, 0.0) + jnp.log(1.0 + jnp.exp(-jnp.abs(scores)))
    if ahead is not None:
        seen = row + ahead * length > col
        softplus = jnp.where(seen, softplus, 0.0)
    spent = dot_left(softplus, (row >= col).astype(BF16))
    weights = jnp.exp(scores - spent)
    if ahead is not None:
        weights = jnp.where(seen, weights, 0.0)
    return dot(weights.astype(BF16), value), spent[:, 0:1]


def attend_near(query, message_ref, shift, place=None):
    weighted, total = None, None
    for k in reversed(range(message_ref.shape[0])):
        ahead = None if place is None else place - k
        more, spent = attend(query, message_ref, shift, k, ahead)
        weighted = more if weighted is None else weighted + jnp.exp(-total) * more
        total = spent if total is None else total + spent
    return weighted, total


def as_row(total):
    return jnp.transpose(jnp.broadcast_to(total, (total.shape[0], HEAD)))[0:1]


def as_column(row):
    pieces = [
        jnp.transpose(jnp.broadcast_to(row[:, k : k + HEAD], (HEAD, HEAD)))[:, 0:1]
        for k in range(0, row.shape[1], HEAD)
    ]
    return jnp.concatenate(pieces, axis=0)


def far_kernel(places_ref, shift_ref, message_ref, query_ref, *out_refs):
    count = query_ref.shape[0]
    length = message_ref.shape[1] - count * 2 * ROWS - HEAD - TILE
    length = length // 2
    shift = shift_ref[0]
    near = message_ref.shape[0]
    index = lax.broadcasted_iota(jnp.int32, (TILE, HEAD), 0)
    for j, out_ref in enumerate(out_refs):
        wanted = places_ref[0] + j + 1 < count

        @pl.when(wanted)
        def _(j=j, out_ref=out_ref):
            query = query_ref[places_ref[0] + j + 1, 0:length]
            weighted, total = attend_near(query, message_ref, shift)
            out_ref[0:length] = weighted.astype(BF16)
            decay, state = chain(message_ref, 2 * length, near)
            high, low = parts(as_row(total))
            pieces = [
                piece[:, k * HEAD : (k + 1) * HEAD] for piece in (high, low) for k in range(2)
            ]
            vector = jnp.zeros((TILE, HEAD), F32)
            for k, piece in enumerate(pieces + [decay]):
                vector = jnp.where(index == k, piece.astype(F32), vector)
            out_ref[length : length + TILE] = vector.astype(BF16)
            out_ref[length + TILE : length + TILE + HEAD] = state.astype(BF16)

        @pl.when(jnp.logical_not(wanted))
        def _(out_ref=out_ref):
            out_ref[...] = jnp.zeros(out_ref.shape, BF16)


def near_kernel(
    places_ref, shift_ref, query_ref, message_ref, weighted_ref, total_ref, decay_ref, state_ref
):
    place = places_ref[1]
    length = weighted_ref.shape[0]
    weighted, total = attend_near(query_ref[0:length], message_ref, shift_ref[0], place)
    weighted_ref[...] = weighted
    total_ref[...] = jnp.broadcast_to(total, total_ref.shape)
    decay_ref[...], state_ref[...] = chain(message_ref, 2 * length, place)


def mixed_kernel(
    places_ref,
    weighted_ref,
    spent_ref,
    decay_ref,
    state_ref,
    inner_ref,
    query_decayed_ref,
    gate_ref,
    gain_a_ref,
    gain_b_ref,
    *refs,
):
    far_refs, (keep_ref, give_ref, total_ref) = refs[:-3], refs[-3:]
    length = weighted_ref.shape[0]
    incoming = jnp.zeros((HEAD, HEAD), F32)
    outside = jnp.zeros((length, HEAD), F32)
    outside_row = jnp.zeros((1, length), F32)
    for ref in reversed(far_refs):
        vector = ref[length : length + TILE].astype(F32)
        row = jnp.concatenate(
            [vector[k : k + 1] + vector[k + 2 : k + 3] for k in range(2)], axis=1
        )
        incoming = vector[4:5] * incoming + ref[
            length + TILE : length + TILE + HEAD
        ].astype(F32)
        outside = ref[0:length].astype(F32) + jnp.exp(-as_column(row)) * outside
        outside_row = outside_row + row
    state = state_ref[...] + decay_ref[...] * incoming
    recurrent = inner_ref[...] + dot_both(query_decayed_ref[...], state, ((1,), (1,)))
    square_mean = jnp.mean(recurrent * recurrent, axis=-1, keepdims=True)
    mixed_b = (
        recurrent * lax.rsqrt(square_mean + epsilon) * gain_b_ref[...] * gate_ref[...]
    ).astype(BF16)
    total = spent_ref[...]
    weighted = weighted_ref[...] + jnp.exp(-total) * outside
    total_row = jnp.transpose(total)[0:1] + outside_row
    total_ref[...] = jnp.log(jnp.maximum(1.0 - jnp.exp(-total_row), log_floor))
    square_mean = jnp.mean(weighted * weighted, axis=-1, keepdims=True)
    mixed_a = (weighted * lax.rsqrt(square_mean + epsilon) * gain_a_ref[...]).astype(BF16)
    mixed = jnp.concatenate([mixed_a, mixed_b], axis=1)
    blocks = mixed.reshape(keep_ref.shape[0], 2, *keep_ref.shape[1:])
    first = places_ref[2] == 0
    keep_ref[...] = jnp.where(first, blocks[:, 0], blocks[:, 1])
    give_ref[...] = jnp.where(first, blocks[:, 1], blocks[:, 0])


def project_out_kernel(keep_ref, other_ref, own_ref, pair_ref, out_ref):
    chips, rows, depth = keep_ref.shape
    mixed = jnp.concatenate(
        [ref[...].reshape(chips * rows, depth) for ref in (keep_ref, other_ref)], axis=1
    )
    fs, near, groups = own_ref.shape[:3]
    width = fs * ROWS
    for group in range(groups):
        for s in range(near):
            both = jnp.concatenate(
                [
                    ref[:, s, group, k].reshape(width, HEAD)
                    for ref in (own_ref, pair_ref)
                    for k in range(2)
                ],
                axis=1,
            )
            at = (group * near + s) * width
            piece = dot(mixed, both, ((1,), (1,))).astype(BF16)
            out_ref[:, :, at : at + width] = piece.reshape(chips, rows, width)


def copies(array, size):
    return jnp.broadcast_to(array[None], (size, *array.shape))


def on_device(
    input_layer_rows,
    input_norm_gain,
    query_weight_attention,
    key_weight_attention,
    value_weight_attention,
    query_weight_recurrent,
    forget_weight_recurrent,
    value_weight_recurrent,
    gate_weight_recurrent,
    output_weight_attention,
    emitted_projection_linear_scan,
    score_offset,
    attention_norm_gain,
    recurrence_norm_gain,
    forget_floor,
    forget_offset,
    extra_log_decay,
):
    x = input_layer_rows[0]
    tokens, width = x.shape
    sp, fs, tp = (lax.axis_size(name) for name in ("sp", "fs", "tp"))
    count = sp // NEAR
    rank = lax.axis_index("sp").astype(jnp.int32)
    shape = jax.ShapeDtypeStruct

    slices, packed, out_own = vmem_call(
        start_kernel,
        (
            shape((fs, tokens, width // fs), BF16),
            shape((7 * ROWS, HEAD), BF16),
            shape((2 * ROWS, HEAD), BF16),
        ),
        11,
        hbm=range(11),
        scratch=(
            pltpu.VMEM((tokens, width), BF16),
            pltpu.VMEM((1, width), F32),
            pltpu.SemaphoreType.DMA((11,)),
        ),
        mib=58,
    )(
        x,
        input_norm_gain.reshape(1, width),
        query_weight_attention,
        key_weight_attention,
        value_weight_attention,
        query_weight_recurrent,
        forget_weight_recurrent,
        value_weight_recurrent,
        gate_weight_recurrent,
        output_weight_attention,
        emitted_projection_linear_scan,
    )
    rows = lax.all_to_all(slices, "fs", 0, 0, tiled=True)
    column = lax.all_gather(packed, "sp")
    first = vmem_call(
        functools.partial(partial_kernel, 0), shape((fs, tokens, HEAD), BF16), 2
    )(rows, column)
    vector = shape((1, HEAD), F32)
    second, places, floor, offset, gain_a, gain_b = vmem_call(
        functools.partial(partial_kernel, 1),
        (
            shape((fs, tokens, 6 * HEAD), BF16),
            shape((3,), jnp.int32),
            vector,
            vector,
            vector,
            vector,
        ),
        7,
        (2,),
    )(
        rows,
        column,
        jnp.stack((rank // NEAR, rank % NEAR, lax.axis_index("tp").astype(jnp.int32) % 2)),
        forget_floor.reshape(1, HEAD),
        forget_offset.reshape(1, HEAD),
        attention_norm_gain.reshape(1, HEAD),
        recurrence_norm_gain.reshape(1, HEAD),
    )
    first = lax.all_to_all(first, "fs", 0, 0, tiled=True)
    own = vmem_call(attention_inputs_kernel, shape((tokens + 2 * ROWS, HEAD), BF16), 2)(
        first, out_own
    )
    second, _ = lax.optimization_barrier((second, own))
    second = lax.all_to_all(second, "fs", 0, 0, tiled=True)
    strided = [list(range(k, sp, NEAR)) for k in range(NEAR)]
    across = lax.all_gather(own, "sp", axis_index_groups=strided)

    small = shape((tokens, HEAD), F32)
    start = 2 * tokens + HEAD + TILE
    message, inner, query_decayed, gate = vmem_call(
        local_recurrence_kernel,
        (shape((start + count * 2 * ROWS, HEAD), BF16), small, small, small),
        5,
        (),
        (3,),
        (pltpu.VMEM((tokens, HEAD), F32), pltpu.SemaphoreType.DMA(())),
    )(
        second,
        floor,
        offset,
        extra_log_decay[0],
        across,
    )
    groups = [list(range(NEAR * k, NEAR * (k + 1))) for k in range(count)]
    gathered = lax.all_gather(message, "sp", axis_index_groups=groups)
    out_weights = lax.all_to_all(
        copies(gathered[:, start:].reshape(NEAR, count, 2, ROWS, HEAD), fs),
        "fs",
        0,
        0,
        tiled=True,
    )
    far = vmem_call(
        far_kernel,
        tuple(shape((tokens + TILE + HEAD, HEAD), BF16) for _ in range(count - 1)),
        4,
        (0, 1),
    )(places, score_offset, gathered, across)
    outside = []
    for j in range(1, count):
        moves = [(k, k + NEAR * j) for k in range(sp - NEAR * j)]
        outside.append(lax.ppermute(far[j - 1], "sp", moves))
    weighted, spent, decay, state = vmem_call(
        near_kernel, (small, small, vector, shape((HEAD, HEAD), F32)), 4, (0, 1)
    )(places, score_offset, own, gathered)
    pairs = [(k, k ^ 1) for k in range(tp)]
    out_other = lax.ppermute(out_weights, "tp", pairs)
    half_rows = (tp // 2, tokens // tp, 2 * HEAD)
    keep, give, row_log_total = vmem_call(
        mixed_kernel,
        (shape(half_rows, BF16), shape(half_rows, BF16), shape((1, tokens), F32)),
        9 + count,
        (0,),
    )(
        places,
        weighted,
        spent,
        decay,
        state,
        inner,
        query_decayed,
        gate,
        gain_a,
        gain_b,
        *outside,
    )
    other = lax.ppermute(give, "tp", pairs)
    projected = vmem_call(
        project_out_kernel, shape((tp // 2, tokens // tp, width), BF16), 4
    )(keep, other, out_weights, out_other)
    chips = [list(range(k, tp, 2)) for k in range(2)]
    tiles = lax.all_to_all(projected, "tp", 0, 0, tiled=True, axis_index_groups=chips)
    layer_out = jnp.sum(tiles.astype(F32), axis=0).astype(BF16)
    return (layer_out[None], row_log_total[None])


def solution(mesh):
    weight = P(("sp", "fs"), "tp")
    return jax.shard_map(
        on_device,
        mesh=mesh,
        in_specs=(
            P("fs", "sp", None),
            P(),
            *(weight for _ in range(9)),
            *(P("tp") for _ in range(5)),
            P("fs", "sp", "tp"),
        ),
        out_specs=(P("fs", ("sp", "tp"), None), P("fs", "tp", "sp")),
        check_vma=False,
    )
```

```python
import functools
import math

import jax
import jax.numpy as jnp
from jax import lax
from jax.experimental import pallas as pl
from jax.experimental.pallas import tpu as pltpu
from jax.sharding import PartitionSpec as P


HEAD = 128
ROWS = 32
TILE = 16
NEAR = 4

epsilon = 1e-06
log_floor = 0.05
LOG2_E = math.log2(math.e)
LN_2 = math.log(2.0)
F32 = jnp.float32
BF16 = jnp.bfloat16
INTERPRET = False


def vmem_call(kernel, outs, n_in, smem=(), hbm=(), scratch=(), mib=16):
    def space(k):
        return pltpu.SMEM if k in smem else pltpu.HBM if k in hbm else pltpu.VMEM

    return pl.pallas_call(
        kernel,
        out_shape=outs,
        in_specs=[pl.BlockSpec(memory_space=space(k)) for k in range(n_in)],
        out_specs=jax.tree.map(
            lambda out: pl.BlockSpec(
                memory_space=pltpu.SMEM if len(out.shape) == 1 else pltpu.VMEM
            ),
            outs,
        ),
        scratch_shapes=list(scratch),
        compiler_params=pltpu.CompilerParams(vmem_limit_bytes=mib << 20),
        interpret=INTERPRET,
    )


def dot(a, b, dims=((1,), (0,))):
    return lax.dot_general(a, b, (dims, ((), ())), preferred_element_type=F32)


def parts(a):
    high = a.astype(BF16)
    return high, (a - high.astype(F32)).astype(BF16)


def dot_left(a, b, dims=((1,), (0,))):
    high, low = parts(a)
    return dot(high, b, dims) + dot(low, b, dims)


def dot_both(a, b, dims):
    a_high, a_low = parts(a)
    b_high, b_low = parts(b)
    return dot(a_high, b_high, dims) + (dot(a_high, b_low, dims) + dot(a_low, b_high, dims))


def start_kernel(x_hbm, gain_hbm, *refs):
    weights = refs[:9]
    slices_ref, packed_ref, own_ref, x_ref, gain_ref, arrived = refs[9:]
    copies = [
        pltpu.make_async_copy(x_hbm, x_ref, arrived.at[0]),
        pltpu.make_async_copy(gain_hbm, gain_ref, arrived.at[1]),
    ]
    for k in range(7):
        place = packed_ref.at[k * ROWS : (k + 1) * ROWS]
        copies.append(pltpu.make_async_copy(weights[k], place, arrived.at[2 + k]))
    for k in range(2):
        place = own_ref.at[k * ROWS : (k + 1) * ROWS]
        copies.append(pltpu.make_async_copy(weights[7 + k], place, arrived.at[9 + k]))
    for copy in copies:
        copy.start()
    for copy in copies:
        copy.wait()
    values = x_ref[...].astype(F32)
    square_mean = jnp.mean(values * values, axis=-1, keepdims=True)
    normed = (values * lax.rsqrt(square_mean + epsilon) * gain_ref[...]).astype(BF16)
    count = slices_ref.shape[0]
    wide = count * HEAD
    target = lax.broadcasted_iota(jnp.int32, (wide, wide), 1)
    source = lax.broadcasted_iota(jnp.int32, (wide, wide), 0)
    inside = target % HEAD
    wanted = (inside // ROWS) * (count * ROWS) + (target // HEAD) * ROWS + inside % ROWS
    pick = (source == wanted).astype(BF16)
    for b in range(x_ref.shape[1] // wide):
        moved = dot(normed[:, b * wide : (b + 1) * wide], pick).astype(BF16)
        for k in range(count):
            slices_ref[k, :, b * HEAD : (b + 1) * HEAD] = moved[:, k * HEAD : (k + 1) * HEAD]


def partial_kernel(first, rows_ref, weight_ref, *refs):
    vectors = refs[: (len(refs) - 1) // 2]
    out_ref = refs[len(vectors)]
    for k, ref in enumerate(refs[len(vectors) + 1 :]):
        if len(ref.shape) == 1:
            for n in range(ref.shape[0]):
                ref[n] = vectors[k][n]
        else:
            ref[...] = vectors[k][...]
    sp = weight_ref.shape[0]
    pieces = [
        weight_ref[:, k * ROWS : (k + 1) * ROWS].reshape(sp * ROWS, HEAD)
        for k in range(first, first + out_ref.shape[2] // HEAD)
    ]
    weight = jnp.concatenate(pieces, axis=1)
    for k in range(rows_ref.shape[0]):
        out_ref[k] = dot(rows_ref[k], weight).astype(BF16)


def sum_of(products_ref):
    total = products_ref[0].astype(F32)
    for k in range(1, products_ref.shape[0]):
        total = total + products_ref[k].astype(F32)
    return total.astype(BF16)


def attention_inputs_kernel(products_ref, own_ref, far_ref):
    length = products_ref.shape[1]
    far_ref[0:length] = sum_of(products_ref)
    far_ref[length : length + 2 * ROWS] = own_ref[...]


def local_recurrence_kernel(*refs):
    products_ref, floor_ref, offset_ref, extra_hbm, slots_ref = refs[:5]
    message_ref, inner_ref, query_decayed_ref, gate_ref, extra_ref, arrived = refs[5:]
    copy = pltpu.make_async_copy(extra_hbm, extra_ref, arrived)
    copy.start()
    total = sum_of(products_ref)
    columns = [total[:, k * HEAD : (k + 1) * HEAD] for k in range(6)]
    query_b = columns[2].astype(F32)
    query = query_b / (1.0 + jnp.exp(-query_b))
    value = columns[4]
    gate_b = columns[5].astype(F32)
    gate_ref[...] = gate_b / (1.0 + jnp.exp(-gate_b))
    u = columns[3].astype(F32) + offset_ref[...]
    key = (1.0 - floor_ref[...]) / (1.0 + jnp.exp(u))
    copy.wait()
    log_forget = jnp.log(1.0 - key) + extra_ref[...]
    length = log_forget.shape[0]
    row = lax.broadcasted_iota(jnp.int32, (length, length), 0)
    col = lax.broadcasted_iota(jnp.int32, (length, length), 1)
    lower = (row >= col).astype(BF16)
    high = log_forget.astype(BF16)
    rest = log_forget - high.astype(F32)
    middle = rest.astype(BF16)
    low = (rest - middle.astype(F32)).astype(BF16)
    running = dot(lower, high) + (dot(lower, middle) + dot(lower, low))
    position = lax.broadcasted_iota(jnp.int32, (length, 1), 0)
    pairwise = jnp.where(row == col, dot_both(query, key, ((1,), (1,))), 0.0)
    half = 1
    while half < length:
        block = 2 * half
        if block >= 8:
            boundary = running.reshape(length // block, block, HEAD)[:, half - 1 : half]
            boundary = jnp.broadcast_to(boundary, (length // block, block, HEAD)).reshape(
                length, HEAD
            )
        else:
            tiles = running.reshape(length // 8, 8, HEAD)
            inside = lax.broadcasted_iota(jnp.int32, (1, 8, 1), 1) // block
            boundary = jnp.zeros_like(tiles)
            for k in range(8 // block):
                at = k * block + half - 1
                boundary = jnp.where(inside == k, tiles[:, at : at + 1], boundary)
            boundary = boundary.reshape(length, HEAD)
        second = (position // half) % 2 == 1
        after = jnp.where(second, query * jnp.exp(running - boundary), 0.0)
        before = jnp.where(second, 0.0, key * jnp.exp(boundary - running))
        chosen = (row // block == col // block) & (row // half != col // half) & (row > col)
        pairwise = jnp.where(chosen, dot_both(after, before, ((1,), (1,))), pairwise)
        half = block
    inner_ref[...] = dot_left(pairwise, value)
    final = running[length - 1 : length]
    query_decayed_ref[...] = query * jnp.exp(running)
    key_high, key_low = parts(key * jnp.exp(final - running))
    state = dot(value, key_high, ((0,), (0,))) + dot(value, key_low, ((0,), (0,)))
    at = 0
    vector = jnp.broadcast_to(jnp.exp(final), (TILE, HEAD)).astype(BF16)
    for piece in (columns[0], columns[1], state.astype(BF16), vector):
        message_ref[at : at + piece.shape[0]] = piece
        at += piece.shape[0]
    for k in range(slots_ref.shape[0]):
        message_ref[at : at + 2 * ROWS] = slots_ref[k, slots_ref.shape[1] - 2 * ROWS :]
        at += 2 * ROWS


def chain(message_ref, start, count=None):
    decay_all, state = None, None
    for k in range(message_ref.shape[0]):
        decay = message_ref[k, start + HEAD : start + HEAD + TILE].astype(F32)[0:1]
        added = message_ref[k, start : start + HEAD].astype(F32)
        if count is not None:
            decay = jnp.where(k < count, decay, 1.0)
            added = jnp.where(k < count, added, 0.0)
        state = added if state is None else decay * state + added
        decay_all = decay if decay_all is None else decay * decay_all
    return decay_all, state


def attend(query, message_ref, shift, k, ahead=None):
    length = query.shape[0]
    row = lax.broadcasted_iota(jnp.int32, (length, length), 0)
    col = lax.broadcasted_iota(jnp.int32, (length, length), 1)
    key = message_ref[k, 0:length]
    value = message_ref[k, length : 2 * length]
    scores = dot(query, key, ((1,), (1,))) * (HEAD ** (-0.5) * LOG2_E) + shift * LOG2_E
    tail = jnp.log(1.0 + jnp.exp2(-jnp.abs(scores))) * LOG2_E
    softplus = jnp.maximum(scores, 0.0) + tail
    if ahead is not None:
        seen = row + ahead * length > col
        softplus = jnp.where(seen, softplus, 0.0)
    after = dot(softplus.astype(BF16), (row > col).astype(BF16))
    weights = jnp.exp2(scores - softplus - after)
    if ahead is not None:
        weights = jnp.where(seen, weights, 0.0)
    return dot(weights.astype(BF16), value), after[:, 0:1] + softplus[:, 0:1]


def attend_near(query, message_ref, shift, place=None):
    weighted, total = None, None
    for k in reversed(range(message_ref.shape[0])):
        ahead = None if place is None else place - k
        more, spent = attend(query, message_ref, shift, k, ahead)
        weighted = more if weighted is None else weighted + jnp.exp2(-total) * more
        total = spent if total is None else total + spent
    return weighted, total * LN_2


def as_row(total):
    return jnp.transpose(jnp.broadcast_to(total, (total.shape[0], HEAD)))[0:1]


def as_column(row):
    pieces = [
        jnp.transpose(jnp.broadcast_to(row[:, k : k + HEAD], (HEAD, HEAD)))[:, 0:1]
        for k in range(0, row.shape[1], HEAD)
    ]
    return jnp.concatenate(pieces, axis=0)


def far_kernel(places_ref, shift_ref, message_ref, query_ref, *out_refs):
    count = query_ref.shape[0]
    length = message_ref.shape[1] - count * 2 * ROWS - HEAD - TILE
    length = length // 2
    shift = shift_ref[0]
    index = lax.broadcasted_iota(jnp.int32, (TILE, HEAD), 0)
    decay, state = chain(message_ref, 2 * length)
    for j, out_ref in enumerate(out_refs):
        wanted = places_ref[0] + j + 1 < count

        @pl.when(wanted)
        def _(j=j, out_ref=out_ref):
            query = query_ref[places_ref[0] + j + 1, 0:length]
            weighted, total = attend_near(query, message_ref, shift)
            out_ref[0:length] = weighted.astype(BF16)
            high, low = parts(as_row(total))
            pieces = [
                piece[:, k * HEAD : (k + 1) * HEAD] for piece in (high, low) for k in range(2)
            ]
            vector = jnp.zeros((TILE, HEAD), F32)
            for k, piece in enumerate(pieces + [decay]):
                vector = jnp.where(index == k, piece.astype(F32), vector)
            out_ref[length : length + TILE] = vector.astype(BF16)
            out_ref[length + TILE : length + TILE + HEAD] = state.astype(BF16)

        @pl.when(jnp.logical_not(wanted))
        def _(out_ref=out_ref):
            out_ref[...] = jnp.zeros(out_ref.shape, BF16)


def near_kernel(
    places_ref, shift_ref, query_ref, message_ref, weighted_ref, total_ref, decay_ref, state_ref
):
    place = places_ref[1]
    length = weighted_ref.shape[0]
    weighted, total = attend_near(query_ref[0:length], message_ref, shift_ref[0], place)
    weighted_ref[...] = weighted
    total_ref[...] = jnp.broadcast_to(total, total_ref.shape)
    decay_ref[...], state_ref[...] = chain(message_ref, 2 * length, place)


def mixed_kernel(
    places_ref,
    weighted_ref,
    spent_ref,
    decay_ref,
    state_ref,
    inner_ref,
    query_decayed_ref,
    gate_ref,
    gain_a_ref,
    gain_b_ref,
    *refs,
):
    far_refs, (keep_ref, give_ref, total_ref) = refs[:-3], refs[-3:]
    length = weighted_ref.shape[0]
    incoming = jnp.zeros((HEAD, HEAD), F32)
    outside = jnp.zeros((length, HEAD), F32)
    outside_row = jnp.zeros((1, length), F32)
    for ref in reversed(far_refs):
        vector = ref[length : length + TILE].astype(F32)
        row = jnp.concatenate(
            [vector[k : k + 1] + vector[k + 2 : k + 3] for k in range(2)], axis=1
        )
        incoming = vector[4:5] * incoming + ref[
            length + TILE : length + TILE + HEAD
        ].astype(F32)
        outside = ref[0:length].astype(F32) + jnp.exp(-as_column(row)) * outside
        outside_row = outside_row + row
    state = state_ref[...] + decay_ref[...] * incoming
    recurrent = inner_ref[...] + dot_both(query_decayed_ref[...], state, ((1,), (1,)))
    square_mean = jnp.mean(recurrent * recurrent, axis=-1, keepdims=True)
    mixed_b = (
        recurrent * lax.rsqrt(square_mean + epsilon) * gain_b_ref[...] * gate_ref[...]
    ).astype(BF16)
    total = spent_ref[...]
    weighted = weighted_ref[...] + jnp.exp(-total) * outside
    total_row = jnp.transpose(total)[0:1] + outside_row
    total_ref[...] = jnp.log(jnp.maximum(1.0 - jnp.exp(-total_row), log_floor))
    square_mean = jnp.mean(weighted * weighted, axis=-1, keepdims=True)
    mixed_a = (weighted * lax.rsqrt(square_mean + epsilon) * gain_a_ref[...]).astype(BF16)
    mixed = jnp.concatenate([mixed_a, mixed_b], axis=1)
    blocks = mixed.reshape(keep_ref.shape[0], 2, *keep_ref.shape[1:])
    first = places_ref[2] == 0
    keep_ref[...] = jnp.where(first, blocks[:, 0], blocks[:, 1])
    give_ref[...] = jnp.where(first, blocks[:, 1], blocks[:, 0])


def project_out_kernel(keep_ref, other_ref, own_ref, pair_ref, out_ref):
    chips, rows, depth = keep_ref.shape
    mixed = jnp.concatenate(
        [ref[...].reshape(chips * rows, depth) for ref in (keep_ref, other_ref)], axis=1
    )
    fs, near, groups = own_ref.shape[:3]
    width = fs * ROWS
    for group in range(groups):
        for s in range(near):
            both = jnp.concatenate(
                [
                    ref[:, s, group, k].reshape(width, HEAD)
                    for ref in (own_ref, pair_ref)
                    for k in range(2)
                ],
                axis=1,
            )
            at = (group * near + s) * width
            piece = dot(mixed, both, ((1,), (1,))).astype(BF16)
            out_ref[:, :, at : at + width] = piece.reshape(chips, rows, width)


def copies(array, size):
    return jnp.broadcast_to(array[None], (size, *array.shape))


def on_device(
    input_layer_rows,
    input_norm_gain,
    query_weight_attention,
    key_weight_attention,
    value_weight_attention,
    query_weight_recurrent,
    forget_weight_recurrent,
    value_weight_recurrent,
    gate_weight_recurrent,
    output_weight_attention,
    emitted_projection_linear_scan,
    score_offset,
    attention_norm_gain,
    recurrence_norm_gain,
    forget_floor,
    forget_offset,
    extra_log_decay,
):
    x = input_layer_rows[0]
    tokens, width = x.shape
    sp, fs, tp = (lax.axis_size(name) for name in ("sp", "fs", "tp"))
    count = sp // NEAR
    rank = lax.axis_index("sp").astype(jnp.int32)
    shape = jax.ShapeDtypeStruct

    slices, packed, out_own = vmem_call(
        start_kernel,
        (
            shape((fs, tokens, width // fs), BF16),
            shape((7 * ROWS, HEAD), BF16),
            shape((2 * ROWS, HEAD), BF16),
        ),
        11,
        hbm=range(11),
        scratch=(
            pltpu.VMEM((tokens, width), BF16),
            pltpu.VMEM((1, width), F32),
            pltpu.SemaphoreType.DMA((11,)),
        ),
        mib=58,
    )(
        x,
        input_norm_gain.reshape(1, width),
        query_weight_attention,
        key_weight_attention,
        value_weight_attention,
        query_weight_recurrent,
        forget_weight_recurrent,
        value_weight_recurrent,
        gate_weight_recurrent,
        output_weight_attention,
        emitted_projection_linear_scan,
    )
    rows = lax.all_to_all(slices, "fs", 0, 0, tiled=True)
    column = lax.all_gather(packed, "sp")
    first = vmem_call(
        functools.partial(partial_kernel, 0), shape((fs, tokens, HEAD), BF16), 2
    )(rows, column)
    vector = shape((1, HEAD), F32)
    second, places, shift, floor, offset, gain_a, gain_b = vmem_call(
        functools.partial(partial_kernel, 1),
        (
            shape((fs, tokens, 6 * HEAD), BF16),
            shape((3,), jnp.int32),
            shape((1,), F32),
            vector,
            vector,
            vector,
            vector,
        ),
        8,
        (2, 3),
    )(
        rows,
        column,
        jnp.stack((rank // NEAR, rank % NEAR, lax.axis_index("tp").astype(jnp.int32) % 2)),
        score_offset,
        forget_floor.reshape(1, HEAD),
        forget_offset.reshape(1, HEAD),
        attention_norm_gain.reshape(1, HEAD),
        recurrence_norm_gain.reshape(1, HEAD),
    )
    first = lax.all_to_all(first, "fs", 0, 0, tiled=True)
    own = vmem_call(attention_inputs_kernel, shape((tokens + 2 * ROWS, HEAD), BF16), 2)(
        first, out_own
    )
    second, _ = lax.optimization_barrier((second, own))
    second = lax.all_to_all(second, "fs", 0, 0, tiled=True)
    strided = [list(range(k, sp, NEAR)) for k in range(NEAR)]
    across = lax.all_gather(own, "sp", axis_index_groups=strided)

    small = shape((tokens, HEAD), F32)
    start = 2 * tokens + HEAD + TILE
    message, inner, query_decayed, gate = vmem_call(
        local_recurrence_kernel,
        (shape((start + count * 2 * ROWS, HEAD), BF16), small, small, small),
        5,
        (),
        (3,),
        (pltpu.VMEM((tokens, HEAD), F32), pltpu.SemaphoreType.DMA(())),
    )(
        second,
        floor,
        offset,
        extra_log_decay[0],
        across,
    )
    groups = [list(range(NEAR * k, NEAR * (k + 1))) for k in range(count)]
    gathered = lax.all_gather(message, "sp", axis_index_groups=groups)
    out_weights = lax.all_to_all(
        copies(gathered[:, start:].reshape(NEAR, count, 2, ROWS, HEAD), fs),
        "fs",
        0,
        0,
        tiled=True,
    )
    far = vmem_call(
        far_kernel,
        tuple(shape((tokens + TILE + HEAD, HEAD), BF16) for _ in range(count - 1)),
        4,
        (0, 1),
    )(places, shift, gathered, across)
    outside = []
    for j in range(1, count):
        moves = [(k, k + NEAR * j) for k in range(sp - NEAR * j)]
        outside.append(lax.ppermute(far[j - 1], "sp", moves))
    weighted, spent, decay, state = vmem_call(
        near_kernel, (small, small, vector, shape((HEAD, HEAD), F32)), 4, (0, 1)
    )(places, shift, own, gathered)
    pairs = [(k, k ^ 1) for k in range(tp)]
    out_other = lax.ppermute(out_weights, "tp", pairs)
    half_rows = (tp // 2, tokens // tp, 2 * HEAD)
    keep, give, row_log_total = vmem_call(
        mixed_kernel,
        (shape(half_rows, BF16), shape(half_rows, BF16), shape((1, tokens), F32)),
        9 + count,
        (0,),
    )(
        places,
        weighted,
        spent,
        decay,
        state,
        inner,
        query_decayed,
        gate,
        gain_a,
        gain_b,
        *outside,
    )
    other = lax.ppermute(give, "tp", pairs)
    projected = vmem_call(
        project_out_kernel, shape((tp // 2, tokens // tp, width), BF16), 4
    )(keep, other, out_weights, out_other)
    chips = [list(range(k, tp, 2)) for k in range(2)]
    tiles = lax.all_to_all(projected, "tp", 0, 0, tiled=True, axis_index_groups=chips)
    layer_out = jnp.sum(tiles.astype(F32), axis=0).astype(BF16)
    return (layer_out[None], row_log_total[None])


def solution(mesh):
    weight = P(("sp", "fs"), "tp")
    return jax.shard_map(
        on_device,
        mesh=mesh,
        in_specs=(
            P("fs", "sp", None),
            P(),
            *(weight for _ in range(9)),
            *(P("tp") for _ in range(5)),
            P("fs", "sp", "tp"),
        ),
        out_specs=(P("fs", ("sp", "tp"), None), P("fs", "tp", "sp")),
        check_vma=False,
    )
```

```python
import math

import jax
import jax.numpy as jnp
from jax import lax
from jax.experimental import pallas as pl
from jax.experimental.pallas import tpu as pltpu
from jax.sharding import PartitionSpec as P


HEAD = 128
ROWS = 32
TILE = 16
NEAR = 4

epsilon = 1e-06
log_floor = 0.05
LOG2_E = math.log2(math.e)
LN_2 = math.log(2.0)
F32 = jnp.float32
BF16 = jnp.bfloat16
INTERPRET = False


def vmem_call(kernel, outs, n_in, smem=(), hbm=(), scratch=(), mib=16):
    def space(k):
        return pltpu.SMEM if k in smem else pltpu.HBM if k in hbm else pltpu.VMEM

    return pl.pallas_call(
        kernel,
        out_shape=outs,
        in_specs=[pl.BlockSpec(memory_space=space(k)) for k in range(n_in)],
        out_specs=jax.tree.map(
            lambda out: pl.BlockSpec(
                memory_space=pltpu.SMEM if len(out.shape) == 1 else pltpu.VMEM
            ),
            outs,
        ),
        scratch_shapes=list(scratch),
        compiler_params=pltpu.CompilerParams(vmem_limit_bytes=mib << 20),
        interpret=INTERPRET,
    )


def dot(a, b, dims=((1,), (0,))):
    return lax.dot_general(a, b, (dims, ((), ())), preferred_element_type=F32)


def parts(a):
    high = a.astype(BF16)
    return high, (a - high.astype(F32)).astype(BF16)


def dot_left(a, b, dims=((1,), (0,))):
    high, low = parts(a)
    return dot(high, b, dims) + dot(low, b, dims)


def dot_both(a, b, dims):
    a_high, a_low = parts(a)
    b_high, b_low = parts(b)
    return dot(a_high, b_high, dims) + (dot(a_high, b_low, dims) + dot(a_low, b_high, dims))


def start_kernel(x_hbm, gain_hbm, *refs):
    weights = refs[:9]
    slices_ref, packed_ref, own_ref, x_ref, gain_ref, arrived = refs[9:]
    copies = [
        pltpu.make_async_copy(x_hbm, x_ref, arrived.at[0]),
        pltpu.make_async_copy(gain_hbm, gain_ref, arrived.at[1]),
    ]
    for k in range(7):
        place = packed_ref.at[k * ROWS : (k + 1) * ROWS]
        copies.append(pltpu.make_async_copy(weights[k], place, arrived.at[2 + k]))
    for k in range(2):
        place = own_ref.at[k * ROWS : (k + 1) * ROWS]
        copies.append(pltpu.make_async_copy(weights[7 + k], place, arrived.at[9 + k]))
    for copy in copies:
        copy.start()
    for copy in copies:
        copy.wait()
    values = x_ref[...].astype(F32)
    square_mean = jnp.mean(values * values, axis=-1, keepdims=True)
    normed = (values * lax.rsqrt(square_mean + epsilon) * gain_ref[...]).astype(BF16)
    count = slices_ref.shape[0]
    wide = count * HEAD
    target = lax.broadcasted_iota(jnp.int32, (wide, wide), 1)
    source = lax.broadcasted_iota(jnp.int32, (wide, wide), 0)
    inside = target % HEAD
    wanted = (inside // ROWS) * (count * ROWS) + (target // HEAD) * ROWS + inside % ROWS
    pick = (source == wanted).astype(BF16)
    for b in range(x_ref.shape[1] // wide):
        moved = dot(normed[:, b * wide : (b + 1) * wide], pick).astype(BF16)
        for k in range(count):
            slices_ref[k, :, b * HEAD : (b + 1) * HEAD] = moved[:, k * HEAD : (k + 1) * HEAD]


def partial_kernel(rows_ref, weight_ref, out_ref):
    sp, depth = weight_ref.shape[:2]
    weight = jnp.concatenate(
        [
            weight_ref[:, at : at + ROWS].reshape(sp * ROWS, HEAD)
            for at in range(0, depth, ROWS)
        ],
        axis=1,
    )
    for k in range(rows_ref.shape[0]):
        out_ref[k] = dot(rows_ref[k], weight).astype(BF16)


def forward_kernel(*refs):
    half = len(refs) // 2
    for taken, given in zip(refs[:half], refs[half:]):
        if len(taken.shape) == 1:
            for n in range(taken.shape[0]):
                given[n] = taken[n]
        else:
            given[...] = taken[...]


def sum_of(products_ref):
    total = products_ref[0].astype(F32)
    for k in range(1, products_ref.shape[0]):
        total = total + products_ref[k].astype(F32)
    return total.astype(BF16)


def local_recurrence_kernel(*refs):
    products_ref, floor_ref, offset_ref, extra_hbm, slots_ref = refs[:5]
    message_ref, query_ref, inner_ref, query_decayed_ref, gate_ref, extra_ref, arrived = refs[5:]
    copy = pltpu.make_async_copy(extra_hbm, extra_ref, arrived)
    copy.start()
    total = sum_of(products_ref)
    columns = [total[:, k * HEAD : (k + 1) * HEAD] for k in range(7)]
    query_ref[...] = columns[0]
    query_b = columns[3].astype(F32)
    query = query_b / (1.0 + jnp.exp(-query_b))
    value = columns[5]
    gate_b = columns[6].astype(F32)
    gate_ref[...] = gate_b / (1.0 + jnp.exp(-gate_b))
    u = columns[4].astype(F32) + offset_ref[...]
    key = (1.0 - floor_ref[...]) / (1.0 + jnp.exp(u))
    copy.wait()
    log_forget = jnp.log(1.0 - key) + extra_ref[...]
    length = log_forget.shape[0]
    row = lax.broadcasted_iota(jnp.int32, (length, length), 0)
    col = lax.broadcasted_iota(jnp.int32, (length, length), 1)
    lower = (row >= col).astype(BF16)
    high = log_forget.astype(BF16)
    rest = log_forget - high.astype(F32)
    middle = rest.astype(BF16)
    low = (rest - middle.astype(F32)).astype(BF16)
    running = dot(lower, high) + (dot(lower, middle) + dot(lower, low))
    position = lax.broadcasted_iota(jnp.int32, (length, 1), 0)
    pairwise = jnp.where(row == col, dot_both(query, key, ((1,), (1,))), 0.0)
    half = 1
    while half < length:
        block = 2 * half
        if block >= 8:
            boundary = running.reshape(length // block, block, HEAD)[:, half - 1 : half]
            boundary = jnp.broadcast_to(boundary, (length // block, block, HEAD)).reshape(
                length, HEAD
            )
        else:
            tiles = running.reshape(length // 8, 8, HEAD)
            inside = lax.broadcasted_iota(jnp.int32, (1, 8, 1), 1) // block
            boundary = jnp.zeros_like(tiles)
            for k in range(8 // block):
                at = k * block + half - 1
                boundary = jnp.where(inside == k, tiles[:, at : at + 1], boundary)
            boundary = boundary.reshape(length, HEAD)
        second = (position // half) % 2 == 1
        after = jnp.where(second, query * jnp.exp(running - boundary), 0.0)
        before = jnp.where(second, 0.0, key * jnp.exp(boundary - running))
        chosen = (row // block == col // block) & (row // half != col // half) & (row > col)
        pairwise = jnp.where(chosen, dot_both(after, before, ((1,), (1,))), pairwise)
        half = block
    inner_ref[...] = dot_left(pairwise, value)
    final = running[length - 1 : length]
    query_decayed_ref[...] = query * jnp.exp(running)
    key_high, key_low = parts(key * jnp.exp(final - running))
    state = dot(value, key_high, ((0,), (0,))) + dot(value, key_low, ((0,), (0,)))
    at = 0
    vector = jnp.broadcast_to(jnp.exp(final), (TILE, HEAD)).astype(BF16)
    for piece in (columns[1], columns[2], state.astype(BF16), vector):
        message_ref[at : at + piece.shape[0]] = piece
        at += piece.shape[0]
    for k in range(slots_ref.shape[0]):
        message_ref[at : at + 2 * ROWS] = slots_ref[k]
        at += 2 * ROWS


def chain(message_ref, start, count=None):
    decay_all, state = None, None
    for k in range(message_ref.shape[0]):
        decay = message_ref[k, start + HEAD : start + HEAD + TILE].astype(F32)[0:1]
        added = message_ref[k, start : start + HEAD].astype(F32)
        if count is not None:
            decay = jnp.where(k < count, decay, 1.0)
            added = jnp.where(k < count, added, 0.0)
        state = added if state is None else decay * state + added
        decay_all = decay if decay_all is None else decay * decay_all
    return decay_all, state


def attend(query, message_ref, shift, k, ahead=None):
    length = query.shape[0]
    row = lax.broadcasted_iota(jnp.int32, (length, length), 0)
    col = lax.broadcasted_iota(jnp.int32, (length, length), 1)
    key = message_ref[k, 0:length]
    value = message_ref[k, length : 2 * length]
    scores = dot(query, key, ((1,), (1,))) * (HEAD ** (-0.5) * LOG2_E) + shift * LOG2_E
    tail = jnp.log(1.0 + jnp.exp2(-jnp.abs(scores))) * LOG2_E
    softplus = jnp.maximum(scores, 0.0) + tail
    if ahead is not None:
        seen = row + ahead * length > col
        softplus = jnp.where(seen, softplus, 0.0)
    after = dot(softplus.astype(BF16), (row > col).astype(BF16))
    weights = jnp.exp2(scores - softplus - after)
    if ahead is not None:
        weights = jnp.where(seen, weights, 0.0)
    return dot(weights.astype(BF16), value), after[:, 0:1] + softplus[:, 0:1]


def attend_near(query, message_ref, shift, place=None):
    weighted, total = None, None
    for k in reversed(range(message_ref.shape[0])):
        ahead = None if place is None else place - k
        more, spent = attend(query, message_ref, shift, k, ahead)
        weighted = more if weighted is None else weighted + jnp.exp2(-total) * more
        total = spent if total is None else total + spent
    return weighted, total * LN_2


def as_row(total):
    return jnp.transpose(jnp.broadcast_to(total, (total.shape[0], HEAD)))[0:1]


def as_column(row):
    pieces = [
        jnp.transpose(jnp.broadcast_to(row[:, k : k + HEAD], (HEAD, HEAD)))[:, 0:1]
        for k in range(0, row.shape[1], HEAD)
    ]
    return jnp.concatenate(pieces, axis=0)


def far_kernel(places_ref, shift_ref, message_ref, *refs):
    count = len(refs) // 2
    shift = shift_ref[0]
    length = refs[0].shape[0]
    index = lax.broadcasted_iota(jnp.int32, (TILE, HEAD), 0)
    for j, query_ref, out_ref in zip(range(count), refs[:count], refs[count:]):
        wanted = places_ref[0] + j < count

        @pl.when(wanted)
        def _(query_ref=query_ref, out_ref=out_ref):
            weighted, total = attend_near(query_ref[...], message_ref, shift)
            out_ref[0:length] = weighted.astype(BF16)
            decay, state = chain(message_ref, 2 * length)
            high, low = parts(as_row(total))
            pieces = [
                piece[:, k * HEAD : (k + 1) * HEAD] for piece in (high, low) for k in range(2)
            ]
            vector = jnp.zeros((TILE, HEAD), F32)
            for k, piece in enumerate(pieces + [decay]):
                vector = jnp.where(index == k, piece.astype(F32), vector)
            out_ref[length : length + TILE] = vector.astype(BF16)
            out_ref[length + TILE : length + TILE + HEAD] = state.astype(BF16)

        @pl.when(jnp.logical_not(wanted))
        def _(out_ref=out_ref):
            out_ref[...] = jnp.zeros(out_ref.shape, BF16)


def near_kernel(
    places_ref, shift_ref, query_ref, message_ref, weighted_ref, total_ref, decay_ref, state_ref
):
    place = places_ref[1]
    length = weighted_ref.shape[0]
    weighted, total = attend_near(query_ref[...], message_ref, shift_ref[0], place)
    weighted_ref[...] = weighted
    total_ref[...] = jnp.broadcast_to(total, total_ref.shape)
    decay_ref[...], state_ref[...] = chain(message_ref, 2 * length, place)


def mixed_kernel(
    places_ref,
    weighted_ref,
    spent_ref,
    decay_ref,
    state_ref,
    inner_ref,
    query_decayed_ref,
    gate_ref,
    gain_a_ref,
    gain_b_ref,
    *refs,
):
    far_refs, (keep_ref, give_ref, total_ref) = refs[:-3], refs[-3:]
    length = weighted_ref.shape[0]
    incoming = jnp.zeros((HEAD, HEAD), F32)
    outside = jnp.zeros((length, HEAD), F32)
    outside_row = jnp.zeros((1, length), F32)
    for ref in reversed(far_refs):
        vector = ref[length : length + TILE].astype(F32)
        row = jnp.concatenate(
            [vector[k : k + 1] + vector[k + 2 : k + 3] for k in range(2)], axis=1
        )
        incoming = vector[4:5] * incoming + ref[
            length + TILE : length + TILE + HEAD
        ].astype(F32)
        outside = ref[0:length].astype(F32) + jnp.exp(-as_column(row)) * outside
        outside_row = outside_row + row
    state = state_ref[...] + decay_ref[...] * incoming
    recurrent = inner_ref[...] + dot_both(query_decayed_ref[...], state, ((1,), (1,)))
    square_mean = jnp.mean(recurrent * recurrent, axis=-1, keepdims=True)
    mixed_b = (
        recurrent * lax.rsqrt(square_mean + epsilon) * gain_b_ref[...] * gate_ref[...]
    ).astype(BF16)
    total = spent_ref[...]
    weighted = weighted_ref[...] + jnp.exp(-total) * outside
    total_row = jnp.transpose(total)[0:1] + outside_row
    total_ref[...] = jnp.log(jnp.maximum(1.0 - jnp.exp(-total_row), log_floor))
    square_mean = jnp.mean(weighted * weighted, axis=-1, keepdims=True)
    mixed_a = (weighted * lax.rsqrt(square_mean + epsilon) * gain_a_ref[...]).astype(BF16)
    mixed = jnp.concatenate([mixed_a, mixed_b], axis=1)
    blocks = mixed.reshape(keep_ref.shape[0], 2, *keep_ref.shape[1:])
    first = places_ref[2] == 0
    keep_ref[...] = jnp.where(first, blocks[:, 0], blocks[:, 1])
    give_ref[...] = jnp.where(first, blocks[:, 1], blocks[:, 0])


def project_out_kernel(keep_ref, other_ref, own_ref, pair_ref, out_ref):
    chips, rows, depth = keep_ref.shape
    mixed = jnp.concatenate(
        [ref[...].reshape(chips * rows, depth) for ref in (keep_ref, other_ref)], axis=1
    )
    fs, near, groups = own_ref.shape[:3]
    width = fs * ROWS
    for group in range(groups):
        for s in range(near):
            both = jnp.concatenate(
                [
                    ref[:, s, group, k].reshape(width, HEAD)
                    for ref in (own_ref, pair_ref)
                    for k in range(2)
                ],
                axis=1,
            )
            at = (group * near + s) * width
            piece = dot(mixed, both, ((1,), (1,))).astype(BF16)
            out_ref[:, :, at : at + width] = piece.reshape(chips, rows, width)


def copies(array, size):
    return jnp.broadcast_to(array[None], (size, *array.shape))


def on_device(
    input_layer_rows,
    input_norm_gain,
    query_weight_attention,
    key_weight_attention,
    value_weight_attention,
    query_weight_recurrent,
    forget_weight_recurrent,
    value_weight_recurrent,
    gate_weight_recurrent,
    output_weight_attention,
    emitted_projection_linear_scan,
    score_offset,
    attention_norm_gain,
    recurrence_norm_gain,
    forget_floor,
    forget_offset,
    extra_log_decay,
):
    x = input_layer_rows[0]
    tokens, width = x.shape
    sp, fs, tp = (lax.axis_size(name) for name in ("sp", "fs", "tp"))
    count = sp // NEAR
    rank = lax.axis_index("sp").astype(jnp.int32)
    shape = jax.ShapeDtypeStruct

    slices, packed, out_own = vmem_call(
        start_kernel,
        (
            shape((fs, tokens, width // fs), BF16),
            shape((7 * ROWS, HEAD), BF16),
            shape((2 * ROWS, HEAD), BF16),
        ),
        11,
        hbm=range(11),
        scratch=(
            pltpu.VMEM((tokens, width), BF16),
            pltpu.VMEM((1, width), F32),
            pltpu.SemaphoreType.DMA((11,)),
        ),
        mib=58,
    )(
        x,
        input_norm_gain.reshape(1, width),
        query_weight_attention,
        key_weight_attention,
        value_weight_attention,
        query_weight_recurrent,
        forget_weight_recurrent,
        value_weight_recurrent,
        gate_weight_recurrent,
        output_weight_attention,
        emitted_projection_linear_scan,
    )
    rows = lax.all_to_all(slices, "fs", 0, 0, tiled=True)
    column = lax.all_gather(packed, "sp")
    products = vmem_call(partial_kernel, shape((fs, tokens, 7 * HEAD), BF16), 2)(rows, column)
    products = lax.all_to_all(products, "fs", 0, 0, tiled=True)
    vector = shape((1, HEAD), F32)
    places, shift, floor, offset, gain_a, gain_b = vmem_call(
        forward_kernel,
        (shape((3,), jnp.int32), shape((1,), F32), vector, vector, vector, vector),
        6,
        (0, 1),
    )(
        jnp.stack((rank // NEAR, rank % NEAR, lax.axis_index("tp").astype(jnp.int32) % 2)),
        score_offset,
        forget_floor.reshape(1, HEAD),
        forget_offset.reshape(1, HEAD),
        attention_norm_gain.reshape(1, HEAD),
        recurrence_norm_gain.reshape(1, HEAD),
    )
    strided = [list(range(k, sp, NEAR)) for k in range(NEAR)]
    across = lax.all_gather(out_own, "sp", axis_index_groups=strided)

    small = shape((tokens, HEAD), F32)
    start = 2 * tokens + HEAD + TILE
    message, query, inner, query_decayed, gate = vmem_call(
        local_recurrence_kernel,
        (
            shape((start + count * 2 * ROWS, HEAD), BF16),
            shape((tokens, HEAD), BF16),
            small,
            small,
            small,
        ),
        5,
        (),
        (3,),
        (pltpu.VMEM((tokens, HEAD), F32), pltpu.SemaphoreType.DMA(())),
    )(
        products,
        floor,
        offset,
        extra_log_decay[0],
        across,
    )
    queries = []
    for j in (2, 1, 3):
        moves = [(k, k - NEAR * j) for k in range(NEAR * j, sp)]
        queries.append((j, lax.ppermute(query, "sp", moves)))
    queries = [array for _, array in sorted(queries, key=lambda pair: pair[0])]
    groups = [list(range(NEAR * k, NEAR * (k + 1))) for k in range(count)]
    gathered = lax.all_gather(message, "sp", axis_index_groups=groups)
    out_weights = lax.all_to_all(
        copies(gathered[:, start:].reshape(NEAR, count, 2, ROWS, HEAD), fs),
        "fs",
        0,
        0,
        tiled=True,
    )
    far = vmem_call(
        far_kernel,
        tuple(shape((tokens + TILE + HEAD, HEAD), BF16) for _ in range(count - 1)),
        3 + len(queries),
        (0, 1),
    )(places, shift, gathered, *queries)
    outside = []
    for j in range(1, count):
        moves = [(k, k + NEAR * j) for k in range(sp - NEAR * j)]
        outside.append(lax.ppermute(far[j - 1], "sp", moves))
    weighted, spent, decay, state = vmem_call(
        near_kernel, (small, small, vector, shape((HEAD, HEAD), F32)), 4, (0, 1)
    )(places, shift, query, gathered)
    pairs = [(k, k ^ 1) for k in range(tp)]
    out_other = lax.ppermute(out_weights, "tp", pairs)
    half_rows = (tp // 2, tokens // tp, 2 * HEAD)
    keep, give, row_log_total = vmem_call(
        mixed_kernel,
        (shape(half_rows, BF16), shape(half_rows, BF16), shape((1, tokens), F32)),
        9 + count,
        (0,),
    )(
        places,
        weighted,
        spent,
        decay,
        state,
        inner,
        query_decayed,
        gate,
        gain_a,
        gain_b,
        *outside,
    )
    other = lax.ppermute(give, "tp", pairs)
    projected = vmem_call(
        project_out_kernel, shape((tp // 2, tokens // tp, width), BF16), 4
    )(keep, other, out_weights, out_other)
    chips = [list(range(k, tp, 2)) for k in range(2)]
    tiles = lax.all_to_all(projected, "tp", 0, 0, tiled=True, axis_index_groups=chips)
    layer_out = jnp.sum(tiles.astype(F32), axis=0).astype(BF16)
    return (layer_out[None], row_log_total[None])


def solution(mesh):
    weight = P(("sp", "fs"), "tp")
    return jax.shard_map(
        on_device,
        mesh=mesh,
        in_specs=(
            P("fs", "sp", None),
            P(),
            *(weight for _ in range(9)),
            *(P("tp") for _ in range(5)),
            P("fs", "sp", "tp"),
        ),
        out_specs=(P("fs", ("sp", "tp"), None), P("fs", "tp", "sp")),
        check_vma=False,
    )
```

```python
import functools
import math

import jax
import jax.numpy as jnp
from jax import lax
from jax.experimental import pallas as pl
from jax.experimental.pallas import tpu as pltpu
from jax.sharding import PartitionSpec as P


HEAD = 128
ROWS = 32
TILE = 16
NEAR = 4

epsilon = 1e-06
log_floor = 0.05
LOG2_E = math.log2(math.e)
LN_2 = math.log(2.0)
F32 = jnp.float32
BF16 = jnp.bfloat16
INTERPRET = False


def vmem_call(kernel, outs, n_in, smem=(), hbm=(), scratch=(), mib=16):
    def space(k):
        return pltpu.SMEM if k in smem else pltpu.HBM if k in hbm else pltpu.VMEM

    return pl.pallas_call(
        kernel,
        out_shape=outs,
        in_specs=[pl.BlockSpec(memory_space=space(k)) for k in range(n_in)],
        out_specs=jax.tree.map(lambda _: pl.BlockSpec(memory_space=pltpu.VMEM), outs),
        scratch_shapes=list(scratch),
        compiler_params=pltpu.CompilerParams(vmem_limit_bytes=mib << 20),
        interpret=INTERPRET,
    )


def dot(a, b, dims=((1,), (0,))):
    return lax.dot_general(a, b, (dims, ((), ())), preferred_element_type=F32)


def parts(a):
    high = a.astype(BF16)
    return high, (a - high.astype(F32)).astype(BF16)


def dot_left(a, b, dims=((1,), (0,))):
    high, low = parts(a)
    return dot(high, b, dims) + dot(low, b, dims)


def dot_both(a, b, dims):
    a_high, a_low = parts(a)
    b_high, b_low = parts(b)
    return dot(a_high, b_high, dims) + (dot(a_high, b_low, dims) + dot(a_low, b_high, dims))


def start_kernel(x_hbm, gain_hbm, *refs):
    weights = refs[:9]
    slices_ref, packed_ref, own_ref, x_ref, gain_ref, arrived = refs[9:]
    copies = [
        pltpu.make_async_copy(x_hbm, x_ref, arrived.at[0]),
        pltpu.make_async_copy(gain_hbm, gain_ref, arrived.at[1]),
    ]
    for k in range(7):
        place = packed_ref.at[k * ROWS : (k + 1) * ROWS]
        copies.append(pltpu.make_async_copy(weights[k], place, arrived.at[2 + k]))
    for k in range(2):
        place = own_ref.at[k * ROWS : (k + 1) * ROWS]
        copies.append(pltpu.make_async_copy(weights[7 + k], place, arrived.at[9 + k]))
    for copy in copies:
        copy.start()
    for copy in copies:
        copy.wait()
    values = x_ref[...].astype(F32)
    square_mean = jnp.mean(values * values, axis=-1, keepdims=True)
    normed = (values * lax.rsqrt(square_mean + epsilon) * gain_ref[...]).astype(BF16)
    count = slices_ref.shape[0]
    wide = count * HEAD
    target = lax.broadcasted_iota(jnp.int32, (wide, wide), 1)
    source = lax.broadcasted_iota(jnp.int32, (wide, wide), 0)
    inside = target % HEAD
    wanted = (inside // ROWS) * (count * ROWS) + (target // HEAD) * ROWS + inside % ROWS
    pick = (source == wanted).astype(BF16)
    for b in range(x_ref.shape[1] // wide):
        moved = dot(normed[:, b * wide : (b + 1) * wide], pick).astype(BF16)
        for k in range(count):
            slices_ref[k, :, b * HEAD : (b + 1) * HEAD] = moved[:, k * HEAD : (k + 1) * HEAD]


def partial_kernel(first, rows_ref, weight_ref, *refs):
    vectors = refs[: (len(refs) - 1) // 2]
    out_ref = refs[len(vectors)]
    for k, ref in enumerate(refs[len(vectors) + 1 :]):
        if len(vectors[k].shape) == 1:
            ref[...] = jnp.full(ref.shape, vectors[k][0])
        else:
            ref[...] = vectors[k][...]
    sp = weight_ref.shape[0]
    pieces = [
        weight_ref[:, k * ROWS : (k + 1) * ROWS].reshape(sp * ROWS, HEAD)
        for k in range(first, first + out_ref.shape[2] // HEAD)
    ]
    weight = jnp.concatenate(pieces, axis=1)
    for k in range(rows_ref.shape[0]):
        out_ref[k] = dot(rows_ref[k], weight).astype(BF16)


def sum_of(products_ref):
    total = products_ref[0].astype(F32)
    for k in range(1, products_ref.shape[0]):
        total = total + products_ref[k].astype(F32)
    return total.astype(BF16)


def attention_inputs_kernel(products_ref, own_ref, far_ref):
    length = products_ref.shape[1]
    far_ref[0:length] = sum_of(products_ref)
    far_ref[length : length + 2 * ROWS] = own_ref[...]


def local_recurrence_kernel(*refs):
    products_ref, floor_ref, offset_ref, extra_hbm, slots_ref = refs[:5]
    message_ref, inner_ref, query_decayed_ref, gate_ref, extra_ref, arrived = refs[5:]
    copy = pltpu.make_async_copy(extra_hbm, extra_ref, arrived)
    copy.start()
    total = sum_of(products_ref)
    columns = [total[:, k * HEAD : (k + 1) * HEAD] for k in range(6)]
    query_b = columns[2].astype(F32)
    query = query_b / (1.0 + jnp.exp(-query_b))
    value = columns[4]
    gate_b = columns[5].astype(F32)
    gate_ref[...] = gate_b / (1.0 + jnp.exp(-gate_b))
    u = columns[3].astype(F32) + offset_ref[...]
    key = (1.0 - floor_ref[...]) / (1.0 + jnp.exp(u))
    copy.wait()
    log_forget = jnp.log(1.0 - key) + extra_ref[...]
    length = log_forget.shape[0]
    row = lax.broadcasted_iota(jnp.int32, (length, length), 0)
    col = lax.broadcasted_iota(jnp.int32, (length, length), 1)
    lower = (row >= col).astype(BF16)
    high = log_forget.astype(BF16)
    rest = log_forget - high.astype(F32)
    middle = rest.astype(BF16)
    low = (rest - middle.astype(F32)).astype(BF16)
    running = dot(lower, high) + (dot(lower, middle) + dot(lower, low))
    position = lax.broadcasted_iota(jnp.int32, (length, 1), 0)
    pairwise = jnp.where(row == col, dot_both(query, key, ((1,), (1,))), 0.0)
    half = 1
    while half < length:
        block = 2 * half
        if block >= 8:
            boundary = running.reshape(length // block, block, HEAD)[:, half - 1 : half]
            boundary = jnp.broadcast_to(boundary, (length // block, block, HEAD)).reshape(
                length, HEAD
            )
        else:
            tiles = running.reshape(length // 8, 8, HEAD)
            inside = lax.broadcasted_iota(jnp.int32, (1, 8, 1), 1) // block
            boundary = jnp.zeros_like(tiles)
            for k in range(8 // block):
                at = k * block + half - 1
                boundary = jnp.where(inside == k, tiles[:, at : at + 1], boundary)
            boundary = boundary.reshape(length, HEAD)
        second = (position // half) % 2 == 1
        after = jnp.where(second, query * jnp.exp(running - boundary), 0.0)
        before = jnp.where(second, 0.0, key * jnp.exp(boundary - running))
        chosen = (row // block == col // block) & (row // half != col // half) & (row > col)
        pairwise = jnp.where(chosen, dot_both(after, before, ((1,), (1,))), pairwise)
        half = block
    inner_ref[...] = dot_left(pairwise, value)
    final = running[length - 1 : length]
    query_decayed_ref[...] = query * jnp.exp(running)
    key_high, key_low = parts(key * jnp.exp(final - running))
    state = dot(value, key_high, ((0,), (0,))) + dot(value, key_low, ((0,), (0,)))
    at = 0
    vector = jnp.broadcast_to(jnp.exp(final), (TILE, HEAD)).astype(BF16)
    for piece in (columns[0], columns[1], state.astype(BF16), vector):
        message_ref[at : at + piece.shape[0]] = piece
        at += piece.shape[0]
    for k in range(slots_ref.shape[0]):
        message_ref[at : at + 2 * ROWS] = slots_ref[k, slots_ref.shape[1] - 2 * ROWS :]
        at += 2 * ROWS


def chain(message_ref, start, count=None):
    decay_all, state = None, None
    for k in range(message_ref.shape[0]):
        decay = message_ref[k, start + HEAD : start + HEAD + TILE].astype(F32)[0:1]
        added = message_ref[k, start : start + HEAD].astype(F32)
        if count is not None:
            decay = jnp.where(k < count, decay, 1.0)
            added = jnp.where(k < count, added, 0.0)
        state = added if state is None else decay * state + added
        decay_all = decay if decay_all is None else decay * decay_all
    return decay_all, state


def attend(query, message_ref, shift, k, ahead=None):
    length = query.shape[0]
    row = lax.broadcasted_iota(jnp.int32, (length, length), 0)
    col = lax.broadcasted_iota(jnp.int32, (length, length), 1)
    key = message_ref[k, 0:length]
    value = message_ref[k, length : 2 * length]
    scores = dot(query, key, ((1,), (1,))) * (HEAD ** (-0.5) * LOG2_E) + shift * LOG2_E
    tail = jnp.log(1.0 + jnp.exp2(-jnp.abs(scores))) * LOG2_E
    softplus = jnp.maximum(scores, 0.0) + tail
    if ahead is not None:
        seen = row + ahead * length > col
        softplus = jnp.where(seen, softplus, 0.0)
    after = dot(softplus.astype(BF16), (row > col).astype(BF16))
    weights = jnp.exp2(scores - softplus - after)
    if ahead is not None:
        weights = jnp.where(seen, weights, 0.0)
    return dot(weights.astype(BF16), value), after[:, 0:1] + softplus[:, 0:1]


def attend_near(query, message_ref, shift, place=None):
    weighted, total = None, None
    for k in reversed(range(message_ref.shape[0])):
        ahead = None if place is None else place - k
        more, spent = attend(query, message_ref, shift, k, ahead)
        weighted = more if weighted is None else weighted + jnp.exp2(-total) * more
        total = spent if total is None else total + spent
    return weighted, total * LN_2


def as_row(total):
    return jnp.transpose(jnp.broadcast_to(total, (total.shape[0], HEAD)))[0:1]


def as_column(row):
    pieces = [
        jnp.transpose(jnp.broadcast_to(row[:, k : k + HEAD], (HEAD, HEAD)))[:, 0:1]
        for k in range(0, row.shape[1], HEAD)
    ]
    return jnp.concatenate(pieces, axis=0)


def far_kernel(position_ref, shift_ref, message_ref, query_ref, *out_refs):
    count = query_ref.shape[0]
    length = message_ref.shape[1] - count * 2 * ROWS - HEAD - TILE
    length = length // 2
    shift = shift_ref[...]
    group = position_ref[0] // message_ref.shape[0] % count
    index = lax.broadcasted_iota(jnp.int32, (TILE, HEAD), 0)
    for j, out_ref in enumerate(out_refs):
        wanted = group + j + 1 < count

        @pl.when(wanted)
        def _(j=j, out_ref=out_ref):
            query = query_ref[group + j + 1, 0:length]
            weighted, total = attend_near(query, message_ref, shift)
            out_ref[0:length] = weighted.astype(BF16)
            decay, state = chain(message_ref, 2 * length)
            high, low = parts(as_row(total))
            pieces = [
                piece[:, k * HEAD : (k + 1) * HEAD] for piece in (high, low) for k in range(2)
            ]
            vector = jnp.zeros((TILE, HEAD), F32)
            for k, piece in enumerate(pieces + [decay]):
                vector = jnp.where(index == k, piece.astype(F32), vector)
            out_ref[length : length + TILE] = vector.astype(BF16)
            out_ref[length + TILE : length + TILE + HEAD] = state.astype(BF16)

        @pl.when(jnp.logical_not(wanted))
        def _(out_ref=out_ref):
            out_ref[...] = jnp.zeros(out_ref.shape, BF16)


def near_kernel(
    position_ref, shift_ref, query_ref, message_ref, weighted_ref, total_ref, decay_ref, state_ref
):
    place = position_ref[0] % message_ref.shape[0]
    length = weighted_ref.shape[0]
    weighted, total = attend_near(query_ref[0:length], message_ref, shift_ref[...], place)
    weighted_ref[...] = weighted
    total_ref[...] = jnp.broadcast_to(total, total_ref.shape)
    decay_ref[...], state_ref[...] = chain(message_ref, 2 * length, place)


def mixed_kernel(
    sp,
    position_ref,
    weighted_ref,
    spent_ref,
    decay_ref,
    state_ref,
    inner_ref,
    query_decayed_ref,
    gate_ref,
    gain_a_ref,
    gain_b_ref,
    *refs,
):
    far_refs, (keep_ref, give_ref, total_ref) = refs[:-3], refs[-3:]
    length = weighted_ref.shape[0]
    incoming = jnp.zeros((HEAD, HEAD), F32)
    outside = jnp.zeros((length, HEAD), F32)
    outside_row = jnp.zeros((1, length), F32)
    for ref in reversed(far_refs):
        vector = ref[length : length + TILE].astype(F32)
        row = jnp.concatenate(
            [vector[k : k + 1] + vector[k + 2 : k + 3] for k in range(2)], axis=1
        )
        incoming = vector[4:5] * incoming + ref[
            length + TILE : length + TILE + HEAD
        ].astype(F32)
        outside = ref[0:length].astype(F32) + jnp.exp(-as_column(row)) * outside
        outside_row = outside_row + row
    state = state_ref[...] + decay_ref[...] * incoming
    recurrent = inner_ref[...] + dot_both(query_decayed_ref[...], state, ((1,), (1,)))
    square_mean = jnp.mean(recurrent * recurrent, axis=-1, keepdims=True)
    mixed_b = (
        recurrent * lax.rsqrt(square_mean + epsilon) * gain_b_ref[...] * gate_ref[...]
    ).astype(BF16)
    total = spent_ref[...]
    weighted = weighted_ref[...] + jnp.exp(-total) * outside
    total_row = jnp.transpose(total)[0:1] + outside_row
    total_ref[...] = jnp.log(jnp.maximum(1.0 - jnp.exp(-total_row), log_floor))
    square_mean = jnp.mean(weighted * weighted, axis=-1, keepdims=True)
    mixed_a = (weighted * lax.rsqrt(square_mean + epsilon) * gain_a_ref[...]).astype(BF16)
    mixed = jnp.concatenate([mixed_a, mixed_b], axis=1)
    blocks = mixed.reshape(keep_ref.shape[0], 2, *keep_ref.shape[1:])
    first = position_ref[0] < sp
    keep_ref[...] = jnp.where(first, blocks[:, 0], blocks[:, 1])
    give_ref[...] = jnp.where(first, blocks[:, 1], blocks[:, 0])


def project_out_kernel(keep_ref, other_ref, own_ref, pair_ref, out_ref):
    chips, rows, depth = keep_ref.shape
    mixed = jnp.concatenate(
        [ref[...].reshape(chips * rows, depth) for ref in (keep_ref, other_ref)], axis=1
    )
    fs, near, groups = own_ref.shape[:3]
    width = fs * ROWS
    for group in range(groups):
        for s in range(near):
            both = jnp.concatenate(
                [
                    ref[:, s, group, k].reshape(width, HEAD)
                    for ref in (own_ref, pair_ref)
                    for k in range(2)
                ],
                axis=1,
            )
            at = (group * near + s) * width
            piece = dot(mixed, both, ((1,), (1,))).astype(BF16)
            out_ref[:, :, at : at + width] = piece.reshape(chips, rows, width)


def copies(array, size):
    return jnp.broadcast_to(array[None], (size, *array.shape))


def on_device(
    input_layer_rows,
    input_norm_gain,
    query_weight_attention,
    key_weight_attention,
    value_weight_attention,
    query_weight_recurrent,
    forget_weight_recurrent,
    value_weight_recurrent,
    gate_weight_recurrent,
    output_weight_attention,
    emitted_projection_linear_scan,
    score_offset,
    attention_norm_gain,
    recurrence_norm_gain,
    forget_floor,
    forget_offset,
    extra_log_decay,
):
    x = input_layer_rows[0]
    tokens, width = x.shape
    sp, fs, tp = (lax.axis_size(name) for name in ("sp", "fs", "tp"))
    count = sp // NEAR
    rank = lax.axis_index("sp").astype(jnp.int32)
    core = lax.axis_index("tp").astype(jnp.int32) & 1
    position = (rank + sp * core).reshape(1)
    shape = jax.ShapeDtypeStruct

    slices, packed, out_own = vmem_call(
        start_kernel,
        (
            shape((fs, tokens, width // fs), BF16),
            shape((7 * ROWS, HEAD), BF16),
            shape((2 * ROWS, HEAD), BF16),
        ),
        11,
        hbm=range(11),
        scratch=(
            pltpu.VMEM((tokens, width), BF16),
            pltpu.VMEM((1, width), F32),
            pltpu.SemaphoreType.DMA((11,)),
        ),
        mib=58,
    )(
        x,
        input_norm_gain.reshape(1, width),
        query_weight_attention,
        key_weight_attention,
        value_weight_attention,
        query_weight_recurrent,
        forget_weight_recurrent,
        value_weight_recurrent,
        gate_weight_recurrent,
        output_weight_attention,
        emitted_projection_linear_scan,
    )
    rows = lax.all_to_all(slices, "fs", 0, 0, tiled=True)
    column = lax.all_gather(packed, "sp")
    first = vmem_call(
        functools.partial(partial_kernel, 0), shape((fs, tokens, HEAD), BF16), 2
    )(rows, column)
    vector = shape((1, HEAD), F32)
    second, shift, floor, offset, gain_a, gain_b = vmem_call(
        functools.partial(partial_kernel, 1),
        (
            shape((fs, tokens, 6 * HEAD), BF16),
            shape((1, tokens), F32),
            vector,
            vector,
            vector,
            vector,
        ),
        7,
        (2,),
    )(
        rows,
        column,
        score_offset,
        forget_floor.reshape(1, HEAD),
        forget_offset.reshape(1, HEAD),
        attention_norm_gain.reshape(1, HEAD),
        recurrence_norm_gain.reshape(1, HEAD),
    )
    first = lax.all_to_all(first, "fs", 0, 0, tiled=True)
    own = vmem_call(attention_inputs_kernel, shape((tokens + 2 * ROWS, HEAD), BF16), 2)(
        first, out_own
    )
    second, _ = lax.optimization_barrier((second, own))
    second = lax.all_to_all(second, "fs", 0, 0, tiled=True)
    strided = [list(range(k, sp, NEAR)) for k in range(NEAR)]
    across = lax.all_gather(own, "sp", axis_index_groups=strided)

    small = shape((tokens, HEAD), F32)
    start = 2 * tokens + HEAD + TILE
    message, inner, query_decayed, gate = vmem_call(
        local_recurrence_kernel,
        (shape((start + count * 2 * ROWS, HEAD), BF16), small, small, small),
        5,
        (),
        (3,),
        (pltpu.VMEM((tokens, HEAD), F32), pltpu.SemaphoreType.DMA(())),
    )(
        second,
        floor,
        offset,
        extra_log_decay[0],
        across,
    )
    groups = [list(range(NEAR * k, NEAR * (k + 1))) for k in range(count)]
    gathered = lax.all_gather(message, "sp", axis_index_groups=groups)
    out_weights = lax.all_to_all(
        copies(gathered[:, start:].reshape(NEAR, count, 2, ROWS, HEAD), fs),
        "fs",
        0,
        0,
        tiled=True,
    )
    far = vmem_call(
        far_kernel,
        tuple(shape((tokens + TILE + HEAD, HEAD), BF16) for _ in range(count - 1)),
        4,
        (0,),
    )(position, shift, gathered, across)
    outside = []
    for j in range(1, count):
        moves = [(k, k + NEAR * j) for k in range(sp - NEAR * j)]
        outside.append(lax.ppermute(far[j - 1], "sp", moves))
    weighted, spent, decay, state = vmem_call(
        near_kernel, (small, small, vector, shape((HEAD, HEAD), F32)), 4, (0,)
    )(position, shift, own, gathered)
    pairs = [(k, k ^ 1) for k in range(tp)]
    out_other = lax.ppermute(out_weights, "tp", pairs)
    half_rows = (tp // 2, tokens // tp, 2 * HEAD)
    keep, give, row_log_total = vmem_call(
        functools.partial(mixed_kernel, sp),
        (shape(half_rows, BF16), shape(half_rows, BF16), shape((1, tokens), F32)),
        9 + count,
        (0,),
    )(
        position,
        weighted,
        spent,
        decay,
        state,
        inner,
        query_decayed,
        gate,
        gain_a,
        gain_b,
        *outside,
    )
    other = lax.ppermute(give, "tp", pairs)
    projected = vmem_call(
        project_out_kernel, shape((tp // 2, tokens // tp, width), BF16), 4
    )(keep, other, out_weights, out_other)
    chips = [list(range(k, tp, 2)) for k in range(2)]
    tiles = lax.all_to_all(projected, "tp", 0, 0, tiled=True, axis_index_groups=chips)
    layer_out = jnp.sum(tiles.astype(F32), axis=0).astype(BF16)
    return (layer_out[None], row_log_total[None])


def solution(mesh):
    weight = P(("sp", "fs"), "tp")
    return jax.shard_map(
        on_device,
        mesh=mesh,
        in_specs=(
            P("fs", "sp", None),
            P(),
            *(weight for _ in range(9)),
            *(P("tp") for _ in range(5)),
            P("fs", "sp", "tp"),
        ),
        out_specs=(P("fs", ("sp", "tp"), None), P("fs", "tp", "sp")),
        check_vma=False,
    )
```

```python
import functools
import math

import jax
import jax.numpy as jnp
from jax import lax
from jax.experimental import pallas as pl
from jax.experimental.pallas import tpu as pltpu
from jax.sharding import PartitionSpec as P


HEAD = 128
ROWS = 32
TILE = 16
NEAR = 4

epsilon = 1e-06
log_floor = 0.05
LOG2_E = math.log2(math.e)
LN_2 = math.log(2.0)
F32 = jnp.float32
BF16 = jnp.bfloat16
INTERPRET = False


def vmem_call(kernel, outs, n_in, smem=(), hbm=(), scratch=(), mib=16):
    def space(k):
        return pltpu.SMEM if k in smem else pltpu.HBM if k in hbm else pltpu.VMEM

    return pl.pallas_call(
        kernel,
        out_shape=outs,
        in_specs=[pl.BlockSpec(memory_space=space(k)) for k in range(n_in)],
        out_specs=jax.tree.map(lambda _: pl.BlockSpec(memory_space=pltpu.VMEM), outs),
        scratch_shapes=list(scratch),
        compiler_params=pltpu.CompilerParams(vmem_limit_bytes=mib << 20),
        interpret=INTERPRET,
    )


def dot(a, b, dims=((1,), (0,))):
    return lax.dot_general(a, b, (dims, ((), ())), preferred_element_type=F32)


def parts(a):
    high = a.astype(BF16)
    return high, (a - high.astype(F32)).astype(BF16)


def dot_left(a, b, dims=((1,), (0,))):
    high, low = parts(a)
    return dot(high, b, dims) + dot(low, b, dims)


def dot_both(a, b, dims):
    a_high, a_low = parts(a)
    b_high, b_low = parts(b)
    return dot(a_high, b_high, dims) + (dot(a_high, b_low, dims) + dot(a_low, b_high, dims))


def start_kernel(x_hbm, gain_hbm, *refs):
    weights = refs[:9]
    slices_ref, packed_ref, own_ref, x_ref, gain_ref, arrived = refs[9:]
    copies = [
        pltpu.make_async_copy(x_hbm, x_ref, arrived.at[0]),
        pltpu.make_async_copy(gain_hbm, gain_ref, arrived.at[1]),
    ]
    for k in range(7):
        place = packed_ref.at[k * ROWS : (k + 1) * ROWS]
        copies.append(pltpu.make_async_copy(weights[k], place, arrived.at[2 + k]))
    for k in range(2):
        place = own_ref.at[k * ROWS : (k + 1) * ROWS]
        copies.append(pltpu.make_async_copy(weights[7 + k], place, arrived.at[9 + k]))
    for copy in copies:
        copy.start()
    for copy in copies:
        copy.wait()
    values = x_ref[...].astype(F32)
    square_mean = jnp.mean(values * values, axis=-1, keepdims=True)
    normed = (values * lax.rsqrt(square_mean + epsilon) * gain_ref[...]).astype(BF16)
    count = slices_ref.shape[0]
    wide = count * HEAD
    target = lax.broadcasted_iota(jnp.int32, (wide, wide), 1)
    source = lax.broadcasted_iota(jnp.int32, (wide, wide), 0)
    inside = target % HEAD
    wanted = (inside // ROWS) * (count * ROWS) + (target // HEAD) * ROWS + inside % ROWS
    pick = (source == wanted).astype(BF16)
    for b in range(x_ref.shape[1] // wide):
        moved = dot(normed[:, b * wide : (b + 1) * wide], pick).astype(BF16)
        for k in range(count):
            slices_ref[k, :, b * HEAD : (b + 1) * HEAD] = moved[:, k * HEAD : (k + 1) * HEAD]


def partial_kernel(first, rows_ref, weight_ref, *refs):
    vectors = refs[: (len(refs) - 1) // 2]
    out_ref = refs[len(vectors)]
    for k, ref in enumerate(refs[len(vectors) + 1 :]):
        if len(vectors[k].shape) == 1:
            ref[...] = jnp.full(ref.shape, vectors[k][0])
        else:
            ref[...] = vectors[k][...]
    sp = weight_ref.shape[0]
    pieces = [
        weight_ref[:, k * ROWS : (k + 1) * ROWS].reshape(sp * ROWS, HEAD)
        for k in range(first, first + out_ref.shape[2] // HEAD)
    ]
    weight = jnp.concatenate(pieces, axis=1)
    for k in range(rows_ref.shape[0]):
        out_ref[k] = dot(rows_ref[k], weight).astype(BF16)


def sum_of(products_ref):
    total = products_ref[0].astype(F32)
    for k in range(1, products_ref.shape[0]):
        total = total + products_ref[k].astype(F32)
    return total.astype(BF16)


def attention_inputs_kernel(products_ref, own_ref, far_ref):
    length = products_ref.shape[1]
    far_ref[0:length] = sum_of(products_ref)
    far_ref[length : length + 2 * ROWS] = own_ref[...]


def local_recurrence_kernel(*refs):
    products_ref, floor_ref, offset_ref, extra_hbm, slots_ref = refs[:5]
    message_ref, inner_ref, query_decayed_ref, gate_ref, extra_ref, arrived = refs[5:]
    copy = pltpu.make_async_copy(extra_hbm, extra_ref, arrived)
    copy.start()
    total = sum_of(products_ref)
    columns = [total[:, k * HEAD : (k + 1) * HEAD] for k in range(6)]
    query_b = columns[2].astype(F32)
    query = query_b / (1.0 + jnp.exp(-query_b))
    value = columns[4]
    gate_b = columns[5].astype(F32)
    gate_ref[...] = gate_b / (1.0 + jnp.exp(-gate_b))
    u = columns[3].astype(F32) + offset_ref[...]
    key = (1.0 - floor_ref[...]) / (1.0 + jnp.exp(u))
    copy.wait()
    log_forget = jnp.log(1.0 - key) + extra_ref[...]
    length = log_forget.shape[0]
    row = lax.broadcasted_iota(jnp.int32, (length, length), 0)
    col = lax.broadcasted_iota(jnp.int32, (length, length), 1)
    lower = (row >= col).astype(BF16)
    high = log_forget.astype(BF16)
    rest = log_forget - high.astype(F32)
    middle = rest.astype(BF16)
    low = (rest - middle.astype(F32)).astype(BF16)
    running = dot(lower, high) + (dot(lower, middle) + dot(lower, low))
    position = lax.broadcasted_iota(jnp.int32, (length, 1), 0)
    products = dot(query.astype(BF16), key.astype(BF16), ((1,), (1,)))
    pairwise = jnp.where(row == col, products, 0.0)
    half = 1
    while half < length:
        block = 2 * half
        if block >= 8:
            boundary = running.reshape(length // block, block, HEAD)[:, half - 1 : half]
            boundary = jnp.broadcast_to(boundary, (length // block, block, HEAD)).reshape(
                length, HEAD
            )
        else:
            tiles = running.reshape(length // 8, 8, HEAD)
            inside = lax.broadcasted_iota(jnp.int32, (1, 8, 1), 1) // block
            boundary = jnp.zeros_like(tiles)
            for k in range(8 // block):
                at = k * block + half - 1
                boundary = jnp.where(inside == k, tiles[:, at : at + 1], boundary)
            boundary = boundary.reshape(length, HEAD)
        second = (position // half) % 2 == 1
        after = jnp.where(second, query * jnp.exp(running - boundary), 0.0)
        before = jnp.where(second, 0.0, key * jnp.exp(boundary - running))
        chosen = (row // block == col // block) & (row // half != col // half) & (row > col)
        products = dot(after.astype(BF16), before.astype(BF16), ((1,), (1,)))
        pairwise = jnp.where(chosen, products, pairwise)
        half = block
    inner_ref[...] = dot_left(pairwise, value)
    final = running[length - 1 : length]
    query_decayed_ref[...] = query * jnp.exp(running)
    key_high, key_low = parts(key * jnp.exp(final - running))
    state = dot(value, key_high, ((0,), (0,))) + dot(value, key_low, ((0,), (0,)))
    at = 0
    vector = jnp.broadcast_to(jnp.exp(final), (TILE, HEAD)).astype(BF16)
    for piece in (columns[0], columns[1], state.astype(BF16), vector):
        message_ref[at : at + piece.shape[0]] = piece
        at += piece.shape[0]
    for k in range(slots_ref.shape[0]):
        message_ref[at : at + 2 * ROWS] = slots_ref[k, slots_ref.shape[1] - 2 * ROWS :]
        at += 2 * ROWS


def chain(message_ref, start, count=None):
    decay_all, state = None, None
    for k in range(message_ref.shape[0]):
        decay = message_ref[k, start + HEAD : start + HEAD + TILE].astype(F32)[0:1]
        added = message_ref[k, start : start + HEAD].astype(F32)
        if count is not None:
            decay = jnp.where(k < count, decay, 1.0)
            added = jnp.where(k < count, added, 0.0)
        state = added if state is None else decay * state + added
        decay_all = decay if decay_all is None else decay * decay_all
    return decay_all, state


def attend(query, message_ref, shift, k, ahead=None):
    length = query.shape[0]
    row = lax.broadcasted_iota(jnp.int32, (length, length), 0)
    col = lax.broadcasted_iota(jnp.int32, (length, length), 1)
    key = message_ref[k, 0:length]
    value = message_ref[k, length : 2 * length]
    scores = dot(query, key, ((1,), (1,))) * (HEAD ** (-0.5) * LOG2_E) + shift * LOG2_E
    tail = jnp.log(1.0 + jnp.exp2(-jnp.abs(scores))) * LOG2_E
    softplus = jnp.maximum(scores, 0.0) + tail
    if ahead is not None:
        seen = row + ahead * length > col
        softplus = jnp.where(seen, softplus, 0.0)
    after = dot(softplus.astype(BF16), (row > col).astype(BF16))
    weights = jnp.exp2(scores - softplus - after)
    if ahead is not None:
        weights = jnp.where(seen, weights, 0.0)
    return dot(weights.astype(BF16), value), after[:, 0:1] + softplus[:, 0:1]


def attend_near(query, message_ref, shift, place=None):
    weighted, total = None, None
    for k in reversed(range(message_ref.shape[0])):
        ahead = None if place is None else place - k
        more, spent = attend(query, message_ref, shift, k, ahead)
        weighted = more if weighted is None else weighted + jnp.exp2(-total) * more
        total = spent if total is None else total + spent
    return weighted, total * LN_2


def as_row(total):
    return jnp.transpose(jnp.broadcast_to(total, (total.shape[0], HEAD)))[0:1]


def as_column(row):
    pieces = [
        jnp.transpose(jnp.broadcast_to(row[:, k : k + HEAD], (HEAD, HEAD)))[:, 0:1]
        for k in range(0, row.shape[1], HEAD)
    ]
    return jnp.concatenate(pieces, axis=0)


def far_kernel(position_ref, shift_ref, message_ref, query_ref, *out_refs):
    count = query_ref.shape[0]
    length = message_ref.shape[1] - count * 2 * ROWS - HEAD - TILE
    length = length // 2
    shift = shift_ref[...]
    group = position_ref[0] // message_ref.shape[0] % count
    index = lax.broadcasted_iota(jnp.int32, (TILE, HEAD), 0)
    for j, out_ref in enumerate(out_refs):
        wanted = group + j + 1 < count

        @pl.when(wanted)
        def _(j=j, out_ref=out_ref):
            query = query_ref[group + j + 1, 0:length]
            weighted, total = attend_near(query, message_ref, shift)
            out_ref[0:length] = weighted.astype(BF16)
            decay, state = chain(message_ref, 2 * length)
            high, low = parts(as_row(total))
            pieces = [
                piece[:, k * HEAD : (k + 1) * HEAD] for piece in (high, low) for k in range(2)
            ]
            vector = jnp.zeros((TILE, HEAD), F32)
            for k, piece in enumerate(pieces + [decay]):
                vector = jnp.where(index == k, piece.astype(F32), vector)
            out_ref[length : length + TILE] = vector.astype(BF16)
            out_ref[length + TILE : length + TILE + HEAD] = state.astype(BF16)

        @pl.when(jnp.logical_not(wanted))
        def _(out_ref=out_ref):
            out_ref[...] = jnp.zeros(out_ref.shape, BF16)


def near_kernel(
    position_ref, shift_ref, query_ref, message_ref, weighted_ref, total_ref, decay_ref, state_ref
):
    place = position_ref[0] % message_ref.shape[0]
    length = weighted_ref.shape[0]
    weighted, total = attend_near(query_ref[0:length], message_ref, shift_ref[...], place)
    weighted_ref[...] = weighted
    total_ref[...] = jnp.broadcast_to(total, total_ref.shape)
    decay_ref[...], state_ref[...] = chain(message_ref, 2 * length, place)


def mixed_kernel(
    sp,
    position_ref,
    weighted_ref,
    spent_ref,
    decay_ref,
    state_ref,
    inner_ref,
    query_decayed_ref,
    gate_ref,
    gain_a_ref,
    gain_b_ref,
    *refs,
):
    far_refs, (keep_ref, give_ref, total_ref) = refs[:-3], refs[-3:]
    length = weighted_ref.shape[0]
    incoming = jnp.zeros((HEAD, HEAD), F32)
    outside = jnp.zeros((length, HEAD), F32)
    outside_row = jnp.zeros((1, length), F32)
    for ref in reversed(far_refs):
        vector = ref[length : length + TILE].astype(F32)
        row = jnp.concatenate(
            [vector[k : k + 1] + vector[k + 2 : k + 3] for k in range(2)], axis=1
        )
        incoming = vector[4:5] * incoming + ref[
            length + TILE : length + TILE + HEAD
        ].astype(F32)
        outside = ref[0:length].astype(F32) + jnp.exp(-as_column(row)) * outside
        outside_row = outside_row + row
    state = state_ref[...] + decay_ref[...] * incoming
    recurrent = inner_ref[...] + dot_both(query_decayed_ref[...], state, ((1,), (1,)))
    square_mean = jnp.mean(recurrent * recurrent, axis=-1, keepdims=True)
    mixed_b = (
        recurrent * lax.rsqrt(square_mean + epsilon) * gain_b_ref[...] * gate_ref[...]
    ).astype(BF16)
    total = spent_ref[...]
    weighted = weighted_ref[...] + jnp.exp(-total) * outside
    total_row = jnp.transpose(total)[0:1] + outside_row
    total_ref[...] = jnp.log(jnp.maximum(1.0 - jnp.exp(-total_row), log_floor))
    square_mean = jnp.mean(weighted * weighted, axis=-1, keepdims=True)
    mixed_a = (weighted * lax.rsqrt(square_mean + epsilon) * gain_a_ref[...]).astype(BF16)
    mixed = jnp.concatenate([mixed_a, mixed_b], axis=1)
    blocks = mixed.reshape(keep_ref.shape[0], 2, *keep_ref.shape[1:])
    first = position_ref[0] < sp
    keep_ref[...] = jnp.where(first, blocks[:, 0], blocks[:, 1])
    give_ref[...] = jnp.where(first, blocks[:, 1], blocks[:, 0])


def project_out_kernel(keep_ref, other_ref, own_ref, pair_ref, out_ref):
    chips, rows, depth = keep_ref.shape
    mixed = jnp.concatenate(
        [ref[...].reshape(chips * rows, depth) for ref in (keep_ref, other_ref)], axis=1
    )
    fs, near, groups = own_ref.shape[:3]
    width = fs * ROWS
    for group in range(groups):
        for s in range(near):
            both = jnp.concatenate(
                [
                    ref[:, s, group, k].reshape(width, HEAD)
                    for ref in (own_ref, pair_ref)
                    for k in range(2)
                ],
                axis=1,
            )
            at = (group * near + s) * width
            piece = dot(mixed, both, ((1,), (1,))).astype(BF16)
            out_ref[:, :, at : at + width] = piece.reshape(chips, rows, width)


def copies(array, size):
    return jnp.broadcast_to(array[None], (size, *array.shape))


def on_device(
    input_layer_rows,
    input_norm_gain,
    query_weight_attention,
    key_weight_attention,
    value_weight_attention,
    query_weight_recurrent,
    forget_weight_recurrent,
    value_weight_recurrent,
    gate_weight_recurrent,
    output_weight_attention,
    emitted_projection_linear_scan,
    score_offset,
    attention_norm_gain,
    recurrence_norm_gain,
    forget_floor,
    forget_offset,
    extra_log_decay,
):
    x = input_layer_rows[0]
    tokens, width = x.shape
    sp, fs, tp = (lax.axis_size(name) for name in ("sp", "fs", "tp"))
    count = sp // NEAR
    rank = lax.axis_index("sp").astype(jnp.int32)
    core = lax.axis_index("tp").astype(jnp.int32) & 1
    position = (rank + sp * core).reshape(1)
    shape = jax.ShapeDtypeStruct

    slices, packed, out_own = vmem_call(
        start_kernel,
        (
            shape((fs, tokens, width // fs), BF16),
            shape((7 * ROWS, HEAD), BF16),
            shape((2 * ROWS, HEAD), BF16),
        ),
        11,
        hbm=range(11),
        scratch=(
            pltpu.VMEM((tokens, width), BF16),
            pltpu.VMEM((1, width), F32),
            pltpu.SemaphoreType.DMA((11,)),
        ),
        mib=58,
    )(
        x,
        input_norm_gain.reshape(1, width),
        query_weight_attention,
        key_weight_attention,
        value_weight_attention,
        query_weight_recurrent,
        forget_weight_recurrent,
        value_weight_recurrent,
        gate_weight_recurrent,
        output_weight_attention,
        emitted_projection_linear_scan,
    )
    rows = lax.all_to_all(slices, "fs", 0, 0, tiled=True)
    column = lax.all_gather(packed, "sp")
    first = vmem_call(
        functools.partial(partial_kernel, 0), shape((fs, tokens, HEAD), BF16), 2
    )(rows, column)
    vector = shape((1, HEAD), F32)
    second, shift, floor, offset, gain_a, gain_b = vmem_call(
        functools.partial(partial_kernel, 1),
        (
            shape((fs, tokens, 6 * HEAD), BF16),
            shape((1, tokens), F32),
            vector,
            vector,
            vector,
            vector,
        ),
        7,
        (2,),
    )(
        rows,
        column,
        score_offset,
        forget_floor.reshape(1, HEAD),
        forget_offset.reshape(1, HEAD),
        attention_norm_gain.reshape(1, HEAD),
        recurrence_norm_gain.reshape(1, HEAD),
    )
    first = lax.all_to_all(first, "fs", 0, 0, tiled=True)
    own = vmem_call(attention_inputs_kernel, shape((tokens + 2 * ROWS, HEAD), BF16), 2)(
        first, out_own
    )
    second, _ = lax.optimization_barrier((second, own))
    second = lax.all_to_all(second, "fs", 0, 0, tiled=True)
    strided = [list(range(k, sp, NEAR)) for k in range(NEAR)]
    across = lax.all_gather(own, "sp", axis_index_groups=strided)

    small = shape((tokens, HEAD), F32)
    start = 2 * tokens + HEAD + TILE
    message, inner, query_decayed, gate = vmem_call(
        local_recurrence_kernel,
        (shape((start + count * 2 * ROWS, HEAD), BF16), small, small, small),
        5,
        (),
        (3,),
        (pltpu.VMEM((tokens, HEAD), F32), pltpu.SemaphoreType.DMA(())),
    )(
        second,
        floor,
        offset,
        extra_log_decay[0],
        across,
    )
    groups = [list(range(NEAR * k, NEAR * (k + 1))) for k in range(count)]
    gathered = lax.all_gather(message, "sp", axis_index_groups=groups)
    out_weights = lax.all_to_all(
        copies(gathered[:, start:].reshape(NEAR, count, 2, ROWS, HEAD), fs),
        "fs",
        0,
        0,
        tiled=True,
    )
    far = vmem_call(
        far_kernel,
        tuple(shape((tokens + TILE + HEAD, HEAD), BF16) for _ in range(count - 1)),
        4,
        (0,),
    )(position, shift, gathered, across)
    outside = []
    for j in range(1, count):
        moves = [(k, k + NEAR * j) for k in range(sp - NEAR * j)]
        outside.append(lax.ppermute(far[j - 1], "sp", moves))
    weighted, spent, decay, state = vmem_call(
        near_kernel, (small, small, vector, shape((HEAD, HEAD), F32)), 4, (0,)
    )(position, shift, own, gathered)
    pairs = [(k, k ^ 1) for k in range(tp)]
    out_other = lax.ppermute(out_weights, "tp", pairs)
    half_rows = (tp // 2, tokens // tp, 2 * HEAD)
    keep, give, row_log_total = vmem_call(
        functools.partial(mixed_kernel, sp),
        (shape(half_rows, BF16), shape(half_rows, BF16), shape((1, tokens), F32)),
        9 + count,
        (0,),
    )(
        position,
        weighted,
        spent,
        decay,
        state,
        inner,
        query_decayed,
        gate,
        gain_a,
        gain_b,
        *outside,
    )
    other = lax.ppermute(give, "tp", pairs)
    projected = vmem_call(
        project_out_kernel, shape((tp // 2, tokens // tp, width), BF16), 4
    )(keep, other, out_weights, out_other)
    chips = [list(range(k, tp, 2)) for k in range(2)]
    tiles = lax.all_to_all(projected, "tp", 0, 0, tiled=True, axis_index_groups=chips)
    layer_out = jnp.sum(tiles.astype(F32), axis=0).astype(BF16)
    return (layer_out[None], row_log_total[None])


def solution(mesh):
    weight = P(("sp", "fs"), "tp")
    return jax.shard_map(
        on_device,
        mesh=mesh,
        in_specs=(
            P("fs", "sp", None),
            P(),
            *(weight for _ in range(9)),
            *(P("tp") for _ in range(5)),
            P("fs", "sp", "tp"),
        ),
        out_specs=(P("fs", ("sp", "tp"), None), P("fs", "tp", "sp")),
        check_vma=False,
    )
```

```python
import functools
import math

import jax
import jax.numpy as jnp
from jax import lax
from jax.experimental import pallas as pl
from jax.experimental.pallas import tpu as pltpu
from jax.sharding import PartitionSpec as P


HEAD = 128
ROWS = 32
TILE = 16
NEAR = 4

epsilon = 1e-06
log_floor = 0.05
LOG2_E = math.log2(math.e)
LN_2 = math.log(2.0)
F32 = jnp.float32
BF16 = jnp.bfloat16
INTERPRET = False


def vmem_call(kernel, outs, n_in, smem=(), hbm=(), scratch=(), mib=16):
    def space(k):
        return pltpu.SMEM if k in smem else pltpu.HBM if k in hbm else pltpu.VMEM

    return pl.pallas_call(
        kernel,
        out_shape=outs,
        in_specs=[pl.BlockSpec(memory_space=space(k)) for k in range(n_in)],
        out_specs=jax.tree.map(lambda _: pl.BlockSpec(memory_space=pltpu.VMEM), outs),
        scratch_shapes=list(scratch),
        compiler_params=pltpu.CompilerParams(vmem_limit_bytes=mib << 20),
        interpret=INTERPRET,
    )


def dot(a, b, dims=((1,), (0,))):
    return lax.dot_general(a, b, (dims, ((), ())), preferred_element_type=F32)


def parts(a):
    high = a.astype(BF16)
    return high, (a - high.astype(F32)).astype(BF16)


def dot_left(a, b, dims=((1,), (0,))):
    high, low = parts(a)
    return dot(high, b, dims) + dot(low, b, dims)


def dot_both(a, b, dims):
    a_high, a_low = parts(a)
    b_high, b_low = parts(b)
    return dot(a_high, b_high, dims) + (dot(a_high, b_low, dims) + dot(a_low, b_high, dims))


def start_kernel(x_hbm, gain_hbm, *refs):
    weights = refs[:9]
    slices_ref, packed_ref, own_ref, x_ref, gain_ref, arrived = refs[9:]
    copies = [
        pltpu.make_async_copy(x_hbm, x_ref, arrived.at[0]),
        pltpu.make_async_copy(gain_hbm, gain_ref, arrived.at[1]),
    ]
    for k in range(7):
        place = packed_ref.at[k * ROWS : (k + 1) * ROWS]
        copies.append(pltpu.make_async_copy(weights[k], place, arrived.at[2 + k]))
    for k in range(2):
        place = own_ref.at[k * ROWS : (k + 1) * ROWS]
        copies.append(pltpu.make_async_copy(weights[7 + k], place, arrived.at[9 + k]))
    for copy in copies:
        copy.start()
    packed_ref[7 * ROWS :] = jnp.zeros((1, HEAD), BF16)
    for copy in copies[:2]:
        copy.wait()
    values = x_ref[...].astype(F32)
    square_mean = jnp.mean(values * values, axis=-1, keepdims=True)
    normed = (values * lax.rsqrt(square_mean + epsilon) * gain_ref[...]).astype(BF16)
    count = slices_ref.shape[0]
    wide = count * HEAD
    target = lax.broadcasted_iota(jnp.int32, (wide, wide), 1)
    source = lax.broadcasted_iota(jnp.int32, (wide, wide), 0)
    inside = target % HEAD
    wanted = (inside // ROWS) * (count * ROWS) + (target // HEAD) * ROWS + inside % ROWS
    pick = (source == wanted).astype(BF16)
    for b in range(x_ref.shape[1] // wide):
        moved = dot(normed[:, b * wide : (b + 1) * wide], pick).astype(BF16)
        for k in range(count):
            slices_ref[k, :, b * HEAD : (b + 1) * HEAD] = moved[:, k * HEAD : (k + 1) * HEAD]
    for copy in copies[2:]:
        copy.wait()


def partial_kernel(first, rows_ref, weight_ref, *refs):
    vectors = refs[: (len(refs) - 1) // 2]
    out_ref = refs[len(vectors)]
    for k, ref in enumerate(refs[len(vectors) + 1 :]):
        if len(vectors[k].shape) == 1:
            ref[...] = jnp.full(ref.shape, vectors[k][0])
        else:
            ref[...] = vectors[k][...]
    sp = weight_ref.shape[0]
    pieces = [
        weight_ref[:, k * ROWS : (k + 1) * ROWS].reshape(sp * ROWS, HEAD)
        for k in range(first, first + out_ref.shape[2] // HEAD)
    ]
    weight = jnp.concatenate(pieces, axis=1)
    for k in range(rows_ref.shape[0]):
        out_ref[k] = dot(rows_ref[k], weight).astype(BF16)


def sum_of(products_ref):
    total = products_ref[0].astype(F32)
    for k in range(1, products_ref.shape[0]):
        total = total + products_ref[k].astype(F32)
    return total.astype(BF16)


def attention_inputs_kernel(products_ref, own_ref, far_ref):
    length = products_ref.shape[1]
    far_ref[0:length] = sum_of(products_ref)
    far_ref[length : length + 2 * ROWS] = own_ref[...]


def local_recurrence_kernel(*refs):
    products_ref, floor_ref, offset_ref, extra_hbm, slots_ref = refs[:5]
    message_ref, inner_ref, query_decayed_ref, gate_ref, extra_ref, arrived = refs[5:]
    copy = pltpu.make_async_copy(extra_hbm, extra_ref, arrived)
    copy.start()
    total = sum_of(products_ref)
    columns = [total[:, k * HEAD : (k + 1) * HEAD] for k in range(6)]
    query_b = columns[2].astype(F32)
    query = query_b / (1.0 + jnp.exp(-query_b))
    value = columns[4]
    gate_b = columns[5].astype(F32)
    gate_ref[...] = gate_b / (1.0 + jnp.exp(-gate_b))
    u = columns[3].astype(F32) + offset_ref[...]
    key = (1.0 - floor_ref[...]) / (1.0 + jnp.exp(u))
    copy.wait()
    log_forget = jnp.log(1.0 - key) + extra_ref[...]
    length = log_forget.shape[0]
    row = lax.broadcasted_iota(jnp.int32, (length, length), 0)
    col = lax.broadcasted_iota(jnp.int32, (length, length), 1)
    lower = (row >= col).astype(BF16)
    high = log_forget.astype(BF16)
    rest = log_forget - high.astype(F32)
    middle = rest.astype(BF16)
    low = (rest - middle.astype(F32)).astype(BF16)
    running = dot(lower, high) + (dot(lower, middle) + dot(lower, low))
    position = lax.broadcasted_iota(jnp.int32, (length, 1), 0)
    products = dot(query.astype(BF16), key.astype(BF16), ((1,), (1,)))
    pairwise = jnp.where(row == col, products, 0.0)
    half = 1
    while half < length:
        block = 2 * half
        if block >= 8:
            boundary = running.reshape(length // block, block, HEAD)[:, half - 1 : half]
            boundary = jnp.broadcast_to(boundary, (length // block, block, HEAD)).reshape(
                length, HEAD
            )
        else:
            tiles = running.reshape(length // 8, 8, HEAD)
            inside = lax.broadcasted_iota(jnp.int32, (1, 8, 1), 1) // block
            boundary = jnp.zeros_like(tiles)
            for k in range(8 // block):
                at = k * block + half - 1
                boundary = jnp.where(inside == k, tiles[:, at : at + 1], boundary)
            boundary = boundary.reshape(length, HEAD)
        second = (position // half) % 2 == 1
        after = jnp.where(second, query * jnp.exp(running - boundary), 0.0)
        before = jnp.where(second, 0.0, key * jnp.exp(boundary - running))
        chosen = (row // block == col // block) & (row // half != col // half) & (row > col)
        products = dot(after.astype(BF16), before.astype(BF16), ((1,), (1,)))
        pairwise = jnp.where(chosen, products, pairwise)
        half = block
    inner_ref[...] = dot_left(pairwise, value)
    final = running[length - 1 : length]
    query_decayed_ref[...] = query * jnp.exp(running)
    key_high, key_low = parts(key * jnp.exp(final - running))
    state = dot(value, key_high, ((0,), (0,))) + dot(value, key_low, ((0,), (0,)))
    at = 0
    vector = jnp.broadcast_to(jnp.exp(final), (TILE, HEAD)).astype(BF16)
    for piece in (columns[0], columns[1], state.astype(BF16), vector):
        message_ref[at : at + piece.shape[0]] = piece
        at += piece.shape[0]
    for k in range(slots_ref.shape[0]):
        message_ref[at : at + 2 * ROWS] = slots_ref[k, slots_ref.shape[1] - 2 * ROWS :]
        at += 2 * ROWS


def chain(message_ref, start, count=None):
    decay_all, state = None, None
    for k in range(message_ref.shape[0]):
        decay = message_ref[k, start + HEAD : start + HEAD + TILE].astype(F32)[0:1]
        added = message_ref[k, start : start + HEAD].astype(F32)
        if count is not None:
            decay = jnp.where(k < count, decay, 1.0)
            added = jnp.where(k < count, added, 0.0)
        state = added if state is None else decay * state + added
        decay_all = decay if decay_all is None else decay * decay_all
    return decay_all, state


def attend(query, message_ref, shift, k, ahead=None):
    length = query.shape[0]
    row = lax.broadcasted_iota(jnp.int32, (length, length), 0)
    col = lax.broadcasted_iota(jnp.int32, (length, length), 1)
    key = message_ref[k, 0:length]
    value = message_ref[k, length : 2 * length]
    scores = dot(query, key, ((1,), (1,))) * (HEAD ** (-0.5) * LOG2_E) + shift * LOG2_E
    tail = jnp.log(1.0 + jnp.exp2(-jnp.abs(scores))) * LOG2_E
    softplus = jnp.maximum(scores, 0.0) + tail
    if ahead is not None:
        seen = row + ahead * length > col
        softplus = jnp.where(seen, softplus, 0.0)
    after = dot(softplus.astype(BF16), (row > col).astype(BF16))
    weights = jnp.exp2(scores - softplus - after)
    if ahead is not None:
        weights = jnp.where(seen, weights, 0.0)
    return dot(weights.astype(BF16), value), after[:, 0:1] + softplus[:, 0:1]


def attend_near(query, message_ref, shift, place=None):
    weighted, total = None, None
    for k in reversed(range(message_ref.shape[0])):
        ahead = None if place is None else place - k
        more, spent = attend(query, message_ref, shift, k, ahead)
        weighted = more if weighted is None else weighted + jnp.exp2(-total) * more
        total = spent if total is None else total + spent
    return weighted, total * LN_2


def as_row(total):
    return jnp.transpose(jnp.broadcast_to(total, (total.shape[0], HEAD)))[0:1]


def as_column(row):
    pieces = [
        jnp.transpose(jnp.broadcast_to(row[:, k : k + HEAD], (HEAD, HEAD)))[:, 0:1]
        for k in range(0, row.shape[1], HEAD)
    ]
    return jnp.concatenate(pieces, axis=0)


def far_kernel(position_ref, shift_ref, message_ref, query_ref, *out_refs):
    count = query_ref.shape[0]
    length = message_ref.shape[1] - count * 2 * ROWS - HEAD - TILE
    length = length // 2
    shift = shift_ref[...]
    group = position_ref[0] // message_ref.shape[0] % count
    index = lax.broadcasted_iota(jnp.int32, (TILE, HEAD), 0)
    for j, out_ref in enumerate(out_refs):
        wanted = group + j + 1 < count

        @pl.when(wanted)
        def _(j=j, out_ref=out_ref):
            query = query_ref[group + j + 1, 0:length]
            weighted, total = attend_near(query, message_ref, shift)
            out_ref[0:length] = weighted.astype(BF16)
            decay, state = chain(message_ref, 2 * length)
            high, low = parts(as_row(total))
            pieces = [
                piece[:, k * HEAD : (k + 1) * HEAD] for piece in (high, low) for k in range(2)
            ]
            vector = jnp.zeros((TILE, HEAD), F32)
            for k, piece in enumerate(pieces + [decay]):
                vector = jnp.where(index == k, piece.astype(F32), vector)
            out_ref[length : length + TILE] = vector.astype(BF16)
            out_ref[length + TILE : length + TILE + HEAD] = state.astype(BF16)

        @pl.when(jnp.logical_not(wanted))
        def _(out_ref=out_ref):
            out_ref[...] = jnp.zeros(out_ref.shape, BF16)


def near_kernel(
    position_ref, shift_ref, query_ref, message_ref, weighted_ref, total_ref, decay_ref, state_ref
):
    place = position_ref[0] % message_ref.shape[0]
    length = weighted_ref.shape[0]
    weighted, total = attend_near(query_ref[0:length], message_ref, shift_ref[...], place)
    weighted_ref[...] = weighted
    total_ref[...] = jnp.broadcast_to(total, total_ref.shape)
    decay_ref[...], state_ref[...] = chain(message_ref, 2 * length, place)


def mixed_kernel(
    sp,
    position_ref,
    weighted_ref,
    spent_ref,
    decay_ref,
    state_ref,
    inner_ref,
    query_decayed_ref,
    gate_ref,
    gain_a_ref,
    gain_b_ref,
    *refs,
):
    far_refs, (keep_ref, give_ref, total_ref) = refs[:-3], refs[-3:]
    length = weighted_ref.shape[0]
    incoming = jnp.zeros((HEAD, HEAD), F32)
    outside = jnp.zeros((length, HEAD), F32)
    outside_row = jnp.zeros((1, length), F32)
    for ref in reversed(far_refs):
        vector = ref[length : length + TILE].astype(F32)
        row = jnp.concatenate(
            [vector[k : k + 1] + vector[k + 2 : k + 3] for k in range(2)], axis=1
        )
        incoming = vector[4:5] * incoming + ref[
            length + TILE : length + TILE + HEAD
        ].astype(F32)
        outside = ref[0:length].astype(F32) + jnp.exp(-as_column(row)) * outside
        outside_row = outside_row + row
    state = state_ref[...] + decay_ref[...] * incoming
    recurrent = inner_ref[...] + dot_both(query_decayed_ref[...], state, ((1,), (1,)))
    square_mean = jnp.mean(recurrent * recurrent, axis=-1, keepdims=True)
    mixed_b = (
        recurrent * lax.rsqrt(square_mean + epsilon) * gain_b_ref[...] * gate_ref[...]
    ).astype(BF16)
    total = spent_ref[...]
    weighted = weighted_ref[...] + jnp.exp(-total) * outside
    total_row = jnp.transpose(total)[0:1] + outside_row
    total_ref[...] = jnp.log(jnp.maximum(1.0 - jnp.exp(-total_row), log_floor))
    square_mean = jnp.mean(weighted * weighted, axis=-1, keepdims=True)
    mixed_a = (weighted * lax.rsqrt(square_mean + epsilon) * gain_a_ref[...]).astype(BF16)
    mixed = jnp.concatenate([mixed_a, mixed_b], axis=1)
    blocks = mixed.reshape(keep_ref.shape[0], 2, *keep_ref.shape[1:])
    first = position_ref[0] < sp
    keep_ref[...] = jnp.where(first, blocks[:, 0], blocks[:, 1])
    give_ref[...] = jnp.where(first, blocks[:, 1], blocks[:, 0])


def project_out_kernel(keep_ref, other_ref, own_ref, pair_ref, out_ref):
    chips, rows, depth = keep_ref.shape
    mixed = jnp.concatenate(
        [ref[...].reshape(chips * rows, depth) for ref in (keep_ref, other_ref)], axis=1
    )
    fs, near, groups = own_ref.shape[:3]
    width = fs * ROWS
    for group in range(groups):
        for s in range(near):
            both = jnp.concatenate(
                [
                    ref[:, s, group, k].reshape(width, HEAD)
                    for ref in (own_ref, pair_ref)
                    for k in range(2)
                ],
                axis=1,
            )
            at = (group * near + s) * width
            piece = dot(mixed, both, ((1,), (1,))).astype(BF16)
            out_ref[:, :, at : at + width] = piece.reshape(chips, rows, width)


def copies(array, size):
    return jnp.broadcast_to(array[None], (size, *array.shape))


def on_device(
    input_layer_rows,
    input_norm_gain,
    query_weight_attention,
    key_weight_attention,
    value_weight_attention,
    query_weight_recurrent,
    forget_weight_recurrent,
    value_weight_recurrent,
    gate_weight_recurrent,
    output_weight_attention,
    emitted_projection_linear_scan,
    score_offset,
    attention_norm_gain,
    recurrence_norm_gain,
    forget_floor,
    forget_offset,
    extra_log_decay,
):
    x = input_layer_rows[0]
    tokens, width = x.shape
    sp, fs, tp = (lax.axis_size(name) for name in ("sp", "fs", "tp"))
    count = sp // NEAR
    rank = lax.axis_index("sp").astype(jnp.int32)
    core = lax.axis_index("tp").astype(jnp.int32) & 1
    position = (rank + sp * core).reshape(1)
    shape = jax.ShapeDtypeStruct

    slices, packed, out_own = vmem_call(
        start_kernel,
        (
            shape((fs, tokens, width // fs), BF16),
            shape((7 * ROWS + 1, HEAD), BF16),
            shape((2 * ROWS, HEAD), BF16),
        ),
        11,
        hbm=range(11),
        scratch=(
            pltpu.VMEM((tokens, width), BF16),
            pltpu.VMEM((1, width), F32),
            pltpu.SemaphoreType.DMA((11,)),
        ),
        mib=58,
    )(
        x,
        input_norm_gain.reshape(1, width),
        query_weight_attention,
        key_weight_attention,
        value_weight_attention,
        query_weight_recurrent,
        forget_weight_recurrent,
        value_weight_recurrent,
        gate_weight_recurrent,
        output_weight_attention,
        emitted_projection_linear_scan,
    )
    rows = lax.all_to_all(slices, "fs", 0, 0, tiled=True)
    column = lax.all_gather(packed, "sp")
    first = vmem_call(
        functools.partial(partial_kernel, 0), shape((fs, tokens, HEAD), BF16), 2
    )(rows, column)
    vector = shape((1, HEAD), F32)
    second, shift, floor, offset, gain_a, gain_b = vmem_call(
        functools.partial(partial_kernel, 1),
        (
            shape((fs, tokens, 6 * HEAD), BF16),
            shape((1, tokens), F32),
            vector,
            vector,
            vector,
            vector,
        ),
        7,
        (2,),
    )(
        rows,
        column,
        score_offset,
        forget_floor.reshape(1, HEAD),
        forget_offset.reshape(1, HEAD),
        attention_norm_gain.reshape(1, HEAD),
        recurrence_norm_gain.reshape(1, HEAD),
    )
    first = lax.all_to_all(first, "fs", 0, 0, tiled=True)
    own = vmem_call(attention_inputs_kernel, shape((tokens + 2 * ROWS, HEAD), BF16), 2)(
        first, out_own
    )
    second, _ = lax.optimization_barrier((second, own))
    second = lax.all_to_all(second, "fs", 0, 0, tiled=True)
    strided = [list(range(k, sp, NEAR)) for k in range(NEAR)]
    across = lax.all_gather(own, "sp", axis_index_groups=strided)

    small = shape((tokens, HEAD), F32)
    start = 2 * tokens + HEAD + TILE
    message, inner, query_decayed, gate = vmem_call(
        local_recurrence_kernel,
        (shape((start + count * 2 * ROWS, HEAD), BF16), small, small, small),
        5,
        (),
        (3,),
        (pltpu.VMEM((tokens, HEAD), F32), pltpu.SemaphoreType.DMA(())),
    )(
        second,
        floor,
        offset,
        extra_log_decay[0],
        across,
    )
    groups = [list(range(NEAR * k, NEAR * (k + 1))) for k in range(count)]
    gathered = lax.all_gather(message, "sp", axis_index_groups=groups)
    out_weights = lax.all_to_all(
        copies(gathered[:, start:].reshape(NEAR, count, 2, ROWS, HEAD), fs),
        "fs",
        0,
        0,
        tiled=True,
    )
    far = vmem_call(
        far_kernel,
        tuple(shape((tokens + TILE + HEAD, HEAD), BF16) for _ in range(count - 1)),
        4,
        (0,),
    )(position, shift, gathered, across)
    outside = []
    for j in range(1, count):
        moves = [(k, k + NEAR * j) for k in range(sp - NEAR * j)]
        outside.append(lax.ppermute(far[j - 1], "sp", moves))
    weighted, spent, decay, state = vmem_call(
        near_kernel, (small, small, vector, shape((HEAD, HEAD), F32)), 4, (0,)
    )(position, shift, own, gathered)
    pairs = [(k, k ^ 1) for k in range(tp)]
    out_other = lax.ppermute(out_weights, "tp", pairs)
    half_rows = (tp // 2, tokens // tp, 2 * HEAD)
    keep, give, row_log_total = vmem_call(
        functools.partial(mixed_kernel, sp),
        (shape(half_rows, BF16), shape(half_rows, BF16), shape((1, tokens), F32)),
        9 + count,
        (0,),
    )(
        position,
        weighted,
        spent,
        decay,
        state,
        inner,
        query_decayed,
        gate,
        gain_a,
        gain_b,
        *outside,
    )
    other = lax.ppermute(give, "tp", pairs)
    projected = vmem_call(
        project_out_kernel, shape((tp // 2, tokens // tp, width), BF16), 4
    )(keep, other, out_weights, out_other)
    chips = [list(range(k, tp, 2)) for k in range(2)]
    tiles = lax.all_to_all(projected, "tp", 0, 0, tiled=True, axis_index_groups=chips)
    layer_out = jnp.sum(tiles.astype(F32), axis=0).astype(BF16)
    return (layer_out[None], row_log_total[None])


def solution(mesh):
    weight = P(("sp", "fs"), "tp")
    return jax.shard_map(
        on_device,
        mesh=mesh,
        in_specs=(
            P("fs", "sp", None),
            P(),
            *(weight for _ in range(9)),
            *(P("tp") for _ in range(5)),
            P("fs", "sp", "tp"),
        ),
        out_specs=(P("fs", ("sp", "tp"), None), P("fs", "tp", "sp")),
        check_vma=False,
    )
```
